32 devices in a mesh: sp: 8 (over z, y), tp: 4 (over x, core).
Axes of the slice: x: 2, y: 2, z: 4, core: 2. Of those that a mesh axis runs over, the one named last changes fastest.
Arguments:
- conv_outer: bfloat16 [6144, 2048], P('sp', 'tp'), may hold values from -6 to 6
- conv_inner: bfloat16 [6144, 2048], P('sp', 'tp'), may hold values from -6 to 6
- conv_input: bfloat16 [6144, 2048], P('sp', 'tp'), may hold values from -6 to 6
- conv_taps: float32 [3, 2048], P(None, 'tp'), may hold values from -3.5 to 3.5
- out_weight: bfloat16 [2048, 2048], P('tp'), may hold values from -0.125 to 0.125
- mix_gate: bfloat16 [6144, 2048], P(('sp', 'tp')), may hold values from -8 to 8
- residual: bfloat16 [6144, 2048], P(('sp', 'tp')), may hold values from -6 to 6
- mix_gain: float32 [2048], replicated, may hold values from 0.1 to 1.9
- expert_gain: float32 [2048], replicated, may hold values from 0.1 to 1.9
- expert_ids: int32 [6144, 2], P(('sp', 'tp')), may hold values from 0 to 7, all different within a row; in each aligned block of 192 rows (0 to 191, 192 to 383, ...) at most 96 rows name the same one
- group_share: float32 [6144], P(('sp', 'tp')), may hold values from 0.25 to 1
- pair_scores: float32 [6144, 2], P(('sp', 'tp')), may hold values from -8 to 8
- gate_experts: bfloat16 [8, 2048, 512], P('sp'), may hold values from -0.125 to 0.125
- up_experts: bfloat16 [8, 2048, 512], P('sp'), may hold values from -0.125 to 0.125
- down_experts: bfloat16 [8, 512, 2048], P('sp'), may hold values from -0.25 to 0.25
Outputs:
- layer_out: bfloat16 [6144, 2048], P(('sp', 'tp'))
The draws below stay inside these ranges and needn't reach their ends.
Inputs may be any that keep to these rules, and one draw needn't show every extreme that they name: `expert_ids`: within the rows of one device (aligned blocks of 192 rows), no expert is named by more than 96 rows, a bound that some block reaches; the 2 experts of a row differ.
All inputs are finite; a program needn't handle non-finite values.
Results may differ from the reference program's by a relative error of at most 0.0069.
Values may be sent and summed in bfloat16 or wider, within the bound.
A program may use at most 128 MiB of HBM per device.

```python
import math
import jax
import jax.numpy as jnp
import numpy as np
from jax import lax

D = 2048
CW = 2048
FF = 512
KSIZE = 3
TOP = 2
TOK_DEV = 192
EXPERTS = 8
CAP = 96
TOKENS = 6144


def block_scale(stream_key, dims, cuts, smallest, largest):
    loudness, own = 1.0, jax.random.fold_in(stream_key, 6)
    for axis_at, blocks in cuts:
        steps = jnp.exp(jax.random.uniform(jax.random.fold_in(own, axis_at), (blocks,), jnp.float32, smallest / len(cuts), largest / len(cuts)))
        loudness = loudness * jnp.repeat(steps, dims[axis_at] // blocks).reshape([-1 if axis == axis_at else 1 for axis in range(len(dims))])
    return loudness


def routed_block(own_key, own, number, rows, amount, top, limit, skew):
    order = jax.random.permutation(own_key, amount)
    packed, ordinary = load_shares(amount, rows * top, limit, skew, True), load_shares(amount, rows * top, limit, skew, False)
    places = jnp.arange(amount)

    def named(sizes, rotation):
        used = int((sizes > 0).sum())
        fixed = max(1, used // 4)
        moved = fixed + (places - fixed + rotation * (used - fixed)) % max(1, amount - fixed)
        return jnp.zeros((amount,), jnp.int32).at[order[jnp.where(places < fixed, places, moved)]].set(jnp.asarray(sizes, jnp.int32))

    sizes = jnp.where(number % 4 == 0, named(packed, number // 4), named(ordinary, number - number // 4 - 1))
    mixed = jax.random.permutation(jax.random.fold_in(own, 3), amount)
    donor, sink = mixed[0:amount // 2 * 2:2], mixed[1:amount // 2 * 2:2]
    margin = jnp.minimum(sizes[donor] - 1, limit - sizes[sink]) // 2
    margin = jnp.where((donor == order[0]) | (sink == order[0]) | (sizes[sink] == 0), 0, jnp.maximum(margin, 0))
    moved = jax.random.randint(jax.random.fold_in(own, 4), (amount // 2,), 0, 1 << 20) % (margin + 1)
    sizes = sizes.at[donor].add(-moved).at[sink].add(moved)
    members = jnp.searchsorted(jnp.cumsum(sizes), jnp.arange(rows * top), side="right").astype(jnp.int32)
    table = members.reshape(top, rows).T
    table = table[jax.random.permutation(jax.random.fold_in(own, 1), rows)]
    rotation = jax.random.randint(jax.random.fold_in(own, 2), (rows, 1), 0, top)
    return jnp.take_along_axis(table, (jnp.arange(top)[None, :] + rotation) % top, axis=1)


def load_shares(number_of, total, reach, slope, full):
    portions = [(1 << 20) // math.isqrt(standing ** slope) + 1 for standing in range(1, number_of + 1)]
    largest = reach if full else min(reach, max(-(-total // number_of), total * portions[0] // sum(portions)))
    least = 1 if total - largest >= number_of - 1 else 0
    given, spare = [largest] + [least] * (number_of - 1), total - largest - least * (number_of - 1)
    while spare > 0:
        candidates = [i for i in range(1, number_of) if given[i] < largest] or [i for i in range(1, number_of) if given[i] < reach]
        mass, budget = sum([portions[i] for i in candidates]), spare
        for i in candidates:
            extra = min(reach - given[i], max(1, budget * portions[i] // mass), spare)
            given[i] = given[i] + extra
            spare = spare - extra
    return np.array(given)


def bell_draw(rng, extent, spread, limit, pieces=(), kind=jnp.bfloat16):
    level = block_scale(rng, extent, pieces, -0.22, 0.18) if pieces else 1.0
    values = jax.random.normal(rng, extent, jnp.float32) * spread * level
    return jnp.minimum(jnp.maximum(values, -limit), limit).astype(kind)


def setup_inputs(seed: int = 0) -> dict:
    key_list = jax.random.split(jax.random.key(seed), 16)
    conv_outer = bell_draw(key_list[0], (TOKENS, CW), 1.0, 6.0, ((0, 8), (1, 4)))
    conv_inner = bell_draw(key_list[1], (TOKENS, CW), 1.0, 6.0, ((0, 8), (1, 4)))
    conv_input = bell_draw(key_list[2], (TOKENS, CW), 1.0, 6.0, ((0, 8), (1, 4)))
    conv_taps = bell_draw(key_list[3], (KSIZE, CW), KSIZE ** -0.5, 3.5, ((1, 4),), jnp.float32)
    out_weight = bell_draw(key_list[4], (CW, D), CW ** -0.5, 0.125, ((0, 4),))
    mix_gate = bell_draw(key_list[5], (TOKENS, D), 1.5, 8.0, ((0, 32),))
    residual = bell_draw(key_list[6], (TOKENS, D), 1.0, 6.0, ((0, 32),))
    mix_gain = jnp.clip(1.0 + 0.18 * jax.random.normal(key_list[7], (D,), jnp.float32), 0.1, 1.9)
    expert_gain = jnp.clip(1.0 + 0.18 * jax.random.normal(key_list[8], (D,), jnp.float32), 0.1, 1.9)
    expert_ids_keys = jax.random.split(jax.random.fold_in(key_list[9], 1), TOKENS // TOK_DEV)
    expert_ids_turns = jax.random.permutation(jax.random.fold_in(key_list[9], 3), TOKENS // TOK_DEV)
    expert_ids = jax.vmap(lambda own, number: routed_block(jax.random.fold_in(key_list[9], 2), own, number, TOK_DEV, EXPERTS, TOP, CAP, 1))(expert_ids_keys, expert_ids_turns).reshape((TOKENS, TOP))
    group_share = jnp.clip(0.25 + 0.75 * jax.random.uniform(key_list[10], (TOKENS,), jnp.float32) ** block_scale(key_list[10], (TOKENS,), ((0, 32),), -0.2, 0.2), 0.25, 1.0)
    pair_scores = bell_draw(key_list[11], (TOKENS, TOP), 1.5, 8.0, ((0, 32),), jnp.float32)
    gate_experts = bell_draw(key_list[12], (EXPERTS, D, FF), D ** -0.5, 0.125, ((0, 8),))
    up_experts = bell_draw(key_list[13], (EXPERTS, D, FF), D ** -0.5, 0.125, ((0, 8),))
    down_experts = bell_draw(key_list[14], (EXPERTS, FF, D), FF ** -0.5, 0.25, ((0, 8),))
    return {"conv_outer": conv_outer, "conv_inner": conv_inner, "conv_input": conv_input, "conv_taps": conv_taps, "out_weight": out_weight, "mix_gate": mix_gate, "residual": residual, "mix_gain": mix_gain, "expert_gain": expert_gain, "expert_ids": expert_ids, "group_share": group_share, "pair_scores": pair_scores, "gate_experts": gate_experts, "up_experts": up_experts, "down_experts": down_experts}


epsilon = 1e-06

def rms_scale(values, gain):
    return values * lax.rsqrt(lax.optimization_barrier(jnp.mean(values * values, axis=-1, keepdims=True)) + epsilon) * gain

def reference(conv_outer, conv_inner, conv_input, conv_taps, out_weight, mix_gate, residual, mix_gain, expert_gain, expert_ids, group_share, pair_scores, gate_experts, up_experts, down_experts):
    inner = conv_inner.astype(jnp.float32) * conv_input.astype(jnp.float32)
    length = inner.shape[0]
    padded = jnp.pad(inner, ((KSIZE - 1, 0), (0, 0)))
    conv = conv_taps[0] * padded[0:length]
    for offset in range(1, KSIZE):
        conv = conv + conv_taps[offset] * padded[offset:offset + length]
    mixed_rows = (conv_outer.astype(jnp.float32) * conv).astype(jnp.bfloat16)
    projected = jnp.dot(mixed_rows, out_weight, preferred_element_type=jnp.float32)
    mixed = jax.nn.sigmoid(mix_gate.astype(jnp.float32)) * projected
    hidden_state = (residual.astype(jnp.float32) + rms_scale(mixed, mix_gain)).astype(jnp.bfloat16)
    normed = rms_scale(hidden_state.astype(jnp.float32), expert_gain).astype(jnp.bfloat16)
    flat_ids = expert_ids.reshape(-1).astype(jnp.int32)
    total = flat_ids.shape[0]
    bound = TOKENS // TOK_DEV * CAP

    def one_expert(carried, expert):
        chosen = jnp.nonzero(flat_ids == expert, size=bound, fill_value=total)[0].astype(jnp.int32)
        rows = normed[jnp.minimum(chosen, total - 1) // TOP]
        first = jnp.dot(rows, gate_experts[expert], preferred_element_type=jnp.float32)
        second = jnp.dot(rows, up_experts[expert], preferred_element_type=jnp.float32)
        inner_hidden = (jax.nn.silu(first) * second).astype(jnp.bfloat16)
        result = jnp.dot(inner_hidden, down_experts[expert], preferred_element_type=jnp.float32).astype(jnp.bfloat16)
        return (carried.at[chosen].set(result, mode='drop'), None)
    start = jnp.zeros((total, D), jnp.bfloat16)
    assigned, unused = lax.scan(one_expert, start, jnp.arange(EXPERTS, dtype=jnp.int32))
    assigned = assigned.reshape(TOKENS, TOP, D)
    weights = group_share[:, None] * jax.nn.softmax(pair_scores, axis=-1)
    result = hidden_state.astype(jnp.float32)
    for slot in range(TOP):
        result = result + weights[:, slot:slot + 1] * assigned[:, slot].astype(jnp.float32)
    return result.astype(jnp.bfloat16)
```

```python
import jax
import jax.numpy as jnp
from jax import lax
from jax.experimental import pallas as pl
from jax.experimental.pallas import tpu as pltpu
from jax.sharding import PartitionSpec as P

epsilon = 1e-06


def f32(value):
    return value.astype(jnp.float32)


def bf16(value):
    return value.astype(jnp.bfloat16)


def rms_scale(values, gain):
    return values * lax.rsqrt(jnp.mean(values * values, axis=-1, keepdims=True) + epsilon) * gain


def shifted(value, steps, senders):
    return lax.ppermute(value, "sp", [(s, s + steps) for s in senders])


def swapped(value, axis, bit):
    return lax.ppermute(value, axis, [(s, s ^ bit) for s in range(lax.axis_size(axis))])


def mixer_rows(conv_outer, conv_inner, conv_input, conv_taps):
    kept = conv_taps.shape[0] - 1
    inner = f32(conv_inner) * f32(conv_input)
    tail = f32(conv_inner[-kept:]) * f32(conv_input[-kept:])
    earlier = shifted(tail, 1, range(lax.axis_size("sp") - 1))
    length = conv_inner.shape[0]
    inner = jnp.concatenate([earlier, inner], 0)
    conv = conv_taps[0] * inner[0:length]
    for offset in range(1, kept + 1):
        conv = conv + conv_taps[offset] * inner[offset : offset + length]
    return bf16(f32(conv_outer) * conv)


def project(mixed_rows, out_weight, own_rows):
    parts = lax.axis_size("tp")
    me = lax.axis_index("tp")
    blocks = mixed_rows.reshape(parts, own_rows, -1)

    def partial(owner):
        rows = lax.dynamic_index_in_dim(blocks, owner, 0, keepdims=False)
        return jnp.dot(rows, out_weight, preferred_element_type=jnp.float32)

    def total(owner_bits, bit):
        if bit == 1:
            return partial(me ^ owner_bits)
        half = bit // 2
        sent = bf16(total(owner_bits | half, half))
        given = swapped(sent, "tp", half)
        return total(owner_bits, half) + f32(given)

    return total(0, parts)


def routing_table(expert_ids, group_share, pair_scores, own_rows, count):
    weights = group_share[:, None] * jax.nn.softmax(pair_scores, axis=-1)
    lanes = -(-2 * count // 128) * 128
    column = jnp.arange(lanes, dtype=jnp.int32)[None, :]
    coarse = lax.reduce_precision(weights, 8, 7)
    fine = weights - coarse
    table = jnp.zeros((own_rows, lanes), jnp.float32)
    for slot in range(expert_ids.shape[1]):
        at = expert_ids[:, slot : slot + 1]
        table = table + jnp.where(column == at, coarse[:, slot : slot + 1], 0.0)
        table = table + jnp.where(column == at + count, fine[:, slot : slot + 1], 0.0)
    return bf16(table)


def per_device(
    conv_outer,
    conv_inner,
    conv_input,
    conv_taps,
    out_weight,
    mix_gate,
    residual,
    mix_gain,
    expert_gain,
    expert_ids,
    group_share,
    pair_scores,
    gate_experts,
    up_experts,
    down_experts,
):
    count = lax.axis_size("sp")
    me = lax.axis_index("sp")
    own_rows = residual.shape[0]
    groups = count // 2
    place = me // 2
    side = lax.axis_index("tp") % 2
    half = gate_experts.shape[2] // 2

    def fetched(weight, axis):
        piece = lax.dynamic_slice_in_dim(weight[0], side * half, half, axis)
        first = swapped(piece, "sp", 1)
        second = swapped(first, "tp", 1)
        return jnp.concatenate([weight[0], first, second], axis)

    gate_both = fetched(gate_experts, 1)
    up_both = fetched(up_experts, 1)
    down_both = fetched(down_experts, 0)

    lanes = -(-2 * count // 128) * 128
    table = routing_table(expert_ids, group_share, pair_scores, own_rows, count)

    def spread(own):
        below, above = {0: own}, {0: own}
        for step in range(1, groups):
            below[step] = shifted(below[step - 1], 2, range(2 * (step - 1), count - 2))
            above[step] = shifted(above[step - 1], -2, range(2, count - 2 * (step - 1)))
        order = {0: own}
        for near in range(1, (groups - 1) // 2 + 1):
            far = groups - near
            early = jnp.where(place < near, above[near], below[near])
            _, over, under, away = lax.optimization_barrier(
                (early, above[near], below[far], above[far])
            )
            order[near] = early
            late = jnp.where(place < far, over, under)
            order[far] = jnp.where(place < near, away, late)
        if groups % 2 == 0:
            mid = groups // 2
            order[mid] = jnp.where(place < mid, above[mid], below[mid])
        return order

    mixed_rows = mixer_rows(conv_outer, conv_inner, conv_input, conv_taps)
    projected = project(mixed_rows, out_weight, own_rows)
    mixed = jax.nn.sigmoid(f32(mix_gate)) * projected
    hidden_state = bf16(f32(residual) + rms_scale(mixed, mix_gain))
    normed = bf16(rms_scale(f32(hidden_state), expert_gain))

    blocks = spread(jnp.concatenate([normed, table], 1))
    depth = normed.shape[1]

    def served(block):
        rows = block[:, :depth]
        chosen = jnp.arange(lanes, dtype=jnp.int32)[:, None] % count
        picks = bf16(chosen == jnp.stack([me, me ^ 1])[None, :])
        picks = jnp.where(jnp.arange(lanes)[:, None] < 2 * count, picks, 0)
        shares = jnp.dot(block[:, depth:], picks, preferred_element_type=jnp.float32)
        wide = 2 * half
        first = jnp.dot(rows, gate_both, preferred_element_type=jnp.float32)
        second = jnp.dot(rows, up_both, preferred_element_type=jnp.float32)
        mine = jnp.arange(2 * wide)[None, :] < wide
        share = jnp.where(mine, shares[:, :1], shares[:, 1:])
        hidden = lax.optimization_barrier(bf16(jax.nn.silu(first) * second * share))
        return lax.optimization_barrier(
            jnp.dot(hidden, down_both, preferred_element_type=jnp.float32)
        )

    results = {number: served(block) for number, block in blocks.items()}

    def for_upper(step):
        gone = groups - step
        if step == gone or step < gone:
            return results[gone]
        return jnp.where(place < gone, results[gone], results[step])

    down = up = None
    for step in range(1, groups):
        gone = groups - step
        lower, upper = results[gone], for_upper(step)
        if down is not None:
            lower, upper = lower + f32(down), upper + f32(up)
        down = shifted(bf16(lower), -2, range(2 * gone, count))
        up = shifted(bf16(upper), 2, range(0, count - 2 * gone))
    result = f32(hidden_state) + results[0]
    if down is not None:
        result = result + f32(down) + f32(up)
    return bf16(result)


MESH_ID = pl.DeviceIdType.MESH
OWN, OTHER, OUT, ARRIVE, FORWARD = 8, 16, 32, 64, 128

OUTER_STEPS = (
    0 | OWN,
    1 | OWN,
    2 | OWN | ARRIVE,
    4 | OWN | ARRIVE,
    0,
    0,
    4 | OTHER | OUT,
    2 | OTHER,
    6 | OWN | OTHER | OUT | ARRIVE,
    0 | OTHER,
    7 | OWN | OTHER | OUT | ARRIVE,
    1 | OTHER,
    5 | OWN | OTHER | OUT | ARRIVE,
    2 | OUT,
    3 | OWN | OTHER | OUT | ARRIVE,
    0 | OUT,
    1 | OUT,
    0,
    0,
    0,
    0,
    0,
)
INNER_STEPS = (
    2 | OWN,
    3 | OWN,
    0 | OWN | ARRIVE | FORWARD,
    4 | OWN | ARRIVE | FORWARD,
    1 | OWN | ARRIVE | FORWARD,
    6 | OWN | ARRIVE | FORWARD,
    4 | OTHER,
    6 | OTHER,
    7 | OWN | OTHER | ARRIVE | FORWARD,
    4 | OUT,
    5 | OWN | OTHER | ARRIVE | FORWARD,
    6 | OUT,
    1 | OTHER,
    0 | OTHER,
    7 | OUT,
    0 | OUT,
    2 | OTHER,
    5 | OUT,
    1 | OUT,
    3 | OTHER,
    2 | OUT,
    3 | OUT,
)
WEIGHTS_STEP = 6
LATE_ACROSS = 4
LATE_OUTWARD = 10


def mega_kernel(
    co_hbm, ci_hbm, cx_hbm, taps, ow_hbm, mg_hbm, res_hbm, mgain, egain, table_hbm,
    g_hbm, u_hbm, d_hbm, out_hbm,
    ci, cx, co, ow, mg, res, mix, acc, part_out, part_in, x_out, x_in,
    X, T, P, S, H, g1, u1, g2, u2, wd, picks,
    load_sem, halo_s, halo_r, tab_s, tab_r, core_s, core_r, xsw_s, xsw_r,
    w_s, w_r, rows_s, rows_r, sum_s, sum_r, out_sem,
):
    sp = lax.axis_index("sp")
    tp = lax.axis_index("tp")
    z = sp // 2
    y = sp % 2
    half = z // 2
    outer = z * (3 - z) == 0
    inner = jnp.logical_not(outer)
    own = jnp.where(outer, 0, 1)
    core_peer = tp + 1 - 2 * (tp % 2)
    x_peer = (tp + 2) % 4
    y_peer = sp + 1 - 2 * y
    rows, depth = res.shape
    piece = rows // 2
    width = g1.shape[1]
    count = 8
    channels = ow.shape[0]
    halo = ci.shape[0] - co.shape[0]

    def line(slot):
        where = jnp.where(slot == 0, 3 * half, jnp.where(slot == 1, 1 + half, jnp.where(slot == 2, 2 - half, 3 - 3 * half)))
        return 2 * where + y

    def remote(src, dst, s, r, device):
        return pltpu.make_async_remote_copy(
            src_ref=src, dst_ref=dst, send_sem=s, recv_sem=r, device_id=device, device_id_type=MESH_ID
        )

    tokens = co.shape[0]
    loads = [
        pltpu.make_async_copy(ci_hbm, ci.at[pl.ds(halo, tokens)], load_sem.at[0]),
        pltpu.make_async_copy(cx_hbm, cx.at[pl.ds(halo, tokens)], load_sem.at[1]),
        pltpu.make_async_copy(co_hbm, co, load_sem.at[2]),
        pltpu.make_async_copy(ow_hbm, ow, load_sem.at[3]),
        pltpu.make_async_copy(mg_hbm, mg, load_sem.at[4]),
        pltpu.make_async_copy(res_hbm, res, load_sem.at[5]),
        pltpu.make_async_copy(g_hbm.at[0], g1, load_sem.at[6]),
        pltpu.make_async_copy(u_hbm.at[0], u1, load_sem.at[7]),
        pltpu.make_async_copy(d_hbm.at[0], wd.at[pl.ds(0, width)], load_sem.at[8]),
        pltpu.make_async_copy(table_hbm, T.at[pl.ds(2 * own, 2)], load_sem.at[9]),
    ]
    for copy in loads:
        copy.start()

    barrier = pltpu.get_barrier_semaphore()

    def greet(device):
        pl.semaphore_signal(barrier, inc=1, device_id=device, device_id_type=MESH_ID)

    greet((sp, core_peer))
    greet((sp, x_peer))
    greet((y_peer, tp))
    for away in range(1, 4):
        greet(((sp + 2 * away) % count, tp))
    has_next = jnp.logical_and(y == 1, sp < count - 1)
    has_last = jnp.logical_and(y == 0, sp > 0)

    @pl.when(has_next)
    def _():
        greet((sp + 1, tp))

    @pl.when(has_last)
    def _():
        greet((sp - 1, tp))

    pl.semaphore_wait(barrier, 6 + jnp.where(has_next, 1, 0) + jnp.where(has_last, 1, 0))

    def halo_copy(k, device):
        src = (ci_hbm, cx_hbm)[k].at[pl.ds(tokens - halo, halo)]
        return remote(src, (ci, cx)[k].at[pl.ds(0, halo)], halo_s.at[k], halo_r.at[k], device)

    @pl.when(sp < count - 1)
    def _():
        for k in range(2):
            halo_copy(k, (sp + 1, tp)).start()

    quarter = depth // 4
    wide = width // 2
    mine = pl.multiple_of(tp * quarter, quarter)
    theirs = pl.multiple_of(x_peer * quarter, quarter)
    side = tp % 2

    def weight_copy(k, leg):
        at = 4 * k + leg
        if k < 2:
            buf = (g2, u2)[k]
            rows_at = pl.ds(theirs if leg == 3 else mine, quarter)
            src = (g_hbm, u_hbm)[k].at[0, rows_at] if leg == 0 else buf.at[rows_at]
            dst = buf.at[rows_at]
        else:
            rows_at = pl.ds(pl.multiple_of(width + side * wide, wide), wide)
            src = d_hbm.at[0, pl.ds(pl.multiple_of(side * wide, wide), wide)] if leg == 0 else wd.at[rows_at]
            dst = wd.at[rows_at]
        device = ((y_peer, tp), (sp, core_peer), (sp, x_peer), (sp, core_peer))[leg]
        return remote(src, dst, w_s.at[at], w_r.at[at], device)

    for k in range(3):
        weight_copy(k, 0).start()

    def table_copy(away):
        zz = (z + away) % 4
        same = zz // 2 == half
        slot = jnp.where(same, own, 3 - own)
        return remote(
            table_hbm, T.at[pl.ds(2 * slot, 2)], tab_s.at[away], tab_r.at[slot], ((sp + 2 * away) % count, tp)
        )

    for away in range(1, 4):
        table_copy(away).start()

    P[0] = jnp.zeros(P.shape[1:], P.dtype)
    lane = lax.broadcasted_iota(jnp.int32, (T.shape[2], width), 0)
    for k in range(2):
        expert = (sp, y_peer)[k]
        picks[k] = jnp.where(jnp.logical_and(lane % count == expert, lane < 2 * count), 1.0, 0.0).astype(picks.dtype)

    for k in range(3):
        loads[k].wait()

    @pl.when(sp == 0)
    def _():
        ci[pl.ds(0, halo)] = jnp.zeros((halo, channels), ci.dtype)
        cx[pl.ds(0, halo)] = jnp.zeros((halo, channels), cx.dtype)

    @pl.when(sp > 0)
    def _():
        for k in range(2):
            halo_copy(k, (sp, core_peer)).wait_recv()

    kept = taps.shape[0] - 1
    run = 32

    def conv(block):
        def some(i, c):
            at = pl.multiple_of(block * rows + i * run, run)
            near = f32(ci[pl.ds(at, halo + run)]) * f32(cx[pl.ds(at, halo + run)])
            total = taps[0:1] * near[halo - kept : halo - kept + run]
            for j in range(1, kept + 1):
                total = total + taps[j : j + 1] * near[halo - kept + j : halo - kept + j + run]
            mix[pl.ds(at, run)] = bf16(f32(co[pl.ds(at, run)]) * total)
            return c

        lax.fori_loop(0, rows // run, some, 0)

    tile = min(512, depth)
    loads[3].wait()

    def core_copy(k):
        return remote(part_out.at[k], part_in.at[k], core_s.at[k], core_r.at[k], (sp, core_peer))

    def x_copy(c):
        return remote(x_out.at[c], x_in.at[c], xsw_s.at[c], xsw_r.at[c], (sp, x_peer))

    def projected(i, carry):
        owner = jnp.where(i == 0, 3 - tp, jnp.where(i == 1, x_peer, jnp.where(i == 2, core_peer, tp)))
        conv(owner)

        def some(n, c):
            cols = pl.ds(pl.multiple_of(n * tile, tile), tile)
            got = jnp.dot(
                mix[pl.ds(pl.multiple_of(owner * rows, rows), rows)], ow[:, cols], preferred_element_type=jnp.float32
            )

            @pl.when(i % 2 == 0)
            def _():
                part_out[i // 2, :, cols] = bf16(got)

            @pl.when(i % 2 == 1)
            def _():
                acc[:, cols] = got

            return c

        lax.fori_loop(0, depth // tile, some, 0)

        @pl.when(i == 0)
        def _():
            core_copy(0).start()

        @pl.when(i == 1)
        def _():
            core_copy(0).wait_recv()

            def add(r, c):
                at = pl.ds(pl.multiple_of(r * 16, 16), 16)
                for k in range(2):
                    src = pl.ds(pl.multiple_of(k * piece + r * 16, 16), 16)
                    x_out[k, at] = bf16(acc[src] + f32(part_in[0, src]))
                return c

            lax.fori_loop(0, piece // 16, add, 0)
            x_copy(0).start()
            x_copy(1).start()

        @pl.when(i == 2)
        def _():
            core_copy(1).start()

        return carry

    lax.fori_loop(0, 4, projected, 0)
    core_copy(1).wait_recv()
    loads[4].wait()
    loads[5].wait()

    def rows_copy(item, device, dst, at):
        return remote(X.at[item], X.at[dst], rows_s.at[at], rows_r.at[dst], device)

    def normalize(c):
        def some(r, carry):
            at = pl.ds(pl.multiple_of(r * 16, 16), 16)
            src = pl.ds(pl.multiple_of(c * piece + r * 16, 16), 16)
            total = acc[src] + f32(part_in[1, src]) + f32(x_in[c, at])
            mixed = jax.nn.sigmoid(f32(mg[src])) * total
            state = bf16(f32(res[src]) + rms_scale(mixed, mgain[...]))
            P[1 + c, at] = state
            X[2 * own + c, at] = bf16(rms_scale(f32(state), egain[...]))
            return carry

        lax.fori_loop(0, piece // 16, some, 0)

    def send_own(c, across):
        item = 2 * own + c
        if across:
            rows_copy(item, (line(2), tp), 4 + c, 8 + c).start()
        else:
            rows_copy(item, (line(1 - own), tp), item, item).start()

    def relay(k, leg):
        weight_copy(k, leg).wait_recv()

    relay(0, 0)
    weight_copy(0, 1).start()
    weight_copy(0, 2).start()
    x_copy(0).wait_recv()
    normalize(0)
    send_own(0, False)

    @pl.when(inner)
    def _():
        send_own(0, True)

    x_copy(1).wait_recv()
    normalize(1)

    @pl.when(outer)
    def _():
        send_own(1, False)

    relay(1, 0)
    weight_copy(1, 1).start()
    weight_copy(1, 2).start()
    for k in range(6, 10):
        loads[k].wait()
    for away in range(1, 4):
        slot = (own + away) % 4
        remote(table_hbm, T.at[pl.ds(2 * slot, 2)], tab_s.at[away], tab_r.at[slot], (sp, core_peer)).wait_recv()

    def hidden(item, k):
        gate, up = ((g1, u1), (g2, u2))[k]
        x = X[item]
        first = jnp.dot(x, gate[...], preferred_element_type=jnp.float32)
        second = jnp.dot(x, up[...], preferred_element_type=jnp.float32)
        share = jnp.dot(T[item], picks[k], preferred_element_type=jnp.float32)
        H[item, :, k * width : (k + 1) * width] = bf16(jax.nn.silu(first) * second * share)

    def sum_copy(item):
        slot = item // 2
        c = item % 2
        to = jnp.where(outer, 1, jnp.where(slot == 0, 0, 2))
        dst = jnp.where(
            outer, 1 + item, jnp.where(slot == 0, 9 + c, jnp.where(slot == 2, 11 + c, 9 + c))
        )
        return remote(S.at[item], P.at[dst], sum_s.at[item], sum_r.at[dst], (line(to), tp))

    def out_copy(c):
        return pltpu.make_async_copy(
            S.at[2 * own + c], out_hbm.at[pl.ds(pl.multiple_of(c * piece, piece), piece)], out_sem.at[c]
        )

    def came(at):
        remote(S.at[0], P.at[at], sum_s.at[0], sum_r.at[at], (sp, core_peer)).wait_recv()

    def step(n, carry):
        code = 0
        for i, (a, b) in enumerate(zip(OUTER_STEPS, INNER_STEPS)):
            code = jnp.where(n == i, jnp.where(outer, a, b), code)
        item = code % 8

        def has(flag):
            return code // flag % 2 == 1

        slot = item // 2
        c = item % 2

        @pl.when(has(ARRIVE))
        def _():
            rows_copy(item, (sp, core_peer), item, item).wait_recv()

        @pl.when(has(FORWARD))
        def _():
            across = slot == 0
            rows_copy(
                item,
                (line(jnp.where(across, 2, 0)), tp),
                jnp.where(across, 6 + c, item),
                jnp.where(across, 10 + c, item),
            ).start()

        @pl.when(jnp.logical_and(inner, n == LATE_ACROSS))
        def _():
            send_own(1, True)

        @pl.when(jnp.logical_and(inner, n == LATE_OUTWARD))
        def _():
            send_own(1, False)

        @pl.when(n == WEIGHTS_STEP)
        def _():
            relay(0, 2)
            weight_copy(0, 3).start()
            relay(1, 2)
            weight_copy(1, 3).start()
            relay(2, 0)
            weight_copy(2, 1).start()
            for k, leg in ((0, 1), (1, 1), (0, 3), (1, 3), (2, 1)):
                got = pl.multiple_of((core_peer if leg == 1 else 3 - tp) * quarter, quarter)
                if k < 2:
                    at = (g2, u2)[k].at[pl.ds(got, quarter)]
                else:
                    at = wd.at[pl.ds(pl.multiple_of(width + (1 - side) * wide, wide), wide)]
                remote(at, at, w_s.at[4 * k + leg], w_r.at[4 * k + leg], (sp, core_peer)).wait_recv()

        @pl.when(has(OWN))
        def _():
            hidden(item, 0)

        @pl.when(has(OTHER))
        def _():
            hidden(item, 1)

        @pl.when(has(OUT))
        def _():
            a = jnp.where(slot == 0, 9 + c, jnp.where(outer, 0, 1 + item))
            b = jnp.where(outer, 0, jnp.where(slot == 1, 11 + c, 0))
            d = jnp.where(slot == own, 1 + c, 0)

            @pl.when(a > 0)
            def _():
                came(a)

            @pl.when(b > 0)
            def _():
                came(b)

            def some(m, carry):
                cols = pl.ds(pl.multiple_of(m * tile, tile), tile)
                got = jnp.dot(H[item], wd[:, cols], preferred_element_type=jnp.float32)
                got = got + f32(P[d, :, cols]) + f32(P[a, :, cols]) + f32(P[b, :, cols])
                S[item, :, cols] = bf16(got)
                return carry

            lax.fori_loop(0, depth // tile, some, 0)

            @pl.when(slot == own)
            def _():
                out_copy(c).start()

            @pl.when(slot != own)
            def _():
                sum_copy(item).start()

        return carry

    lax.fori_loop(0, len(OUTER_STEPS), step, 0)

    for c in range(2):
        out_copy(c).wait()
        core_copy(c).wait_send()
        x_copy(c).wait_send()

    @pl.when(sp < count - 1)
    def _():
        for k in range(2):
            halo_copy(k, (sp + 1, tp)).wait_send()

    for k in range(3):
        for leg in range(4 if k < 2 else 2):
            weight_copy(k, leg).wait_send()
    for away in range(1, 4):
        table_copy(away).wait_send()

    def gone(item, at):
        rows_copy(item, (sp, core_peer), item, at).wait_send()

    for c in range(2):
        gone(2 * own + c, 2 * own + c)
    for i in range(3):
        for c in range(2):
            item = 2 * ((own + 1 + i) % 4) + c
            remote(S.at[item], P.at[0], sum_s.at[item], sum_r.at[0], (sp, core_peer)).wait_send()

    @pl.when(inner)
    def _():
        for c in range(2):
            for at in (4 + c, 6 + c, 8 + c, 10 + c):
                gone(at % 8, at)


def mega(
    conv_outer, conv_inner, conv_input, conv_taps, out_weight, mix_gate, residual, mix_gain, expert_gain,
    expert_ids, group_share, pair_scores, gate_experts, up_experts, down_experts,
):
    count = lax.axis_size("sp")
    rows, depth = residual.shape
    tokens, channels = conv_inner.shape
    width = gate_experts.shape[2]
    piece = rows // 2
    table = routing_table(expert_ids, group_share, pair_scores, rows, count)
    lanes = table.shape[1]
    table = table.reshape(2, piece, lanes)
    halo = 16
    half_type, full = jnp.bfloat16, jnp.float32
    hbm = pl.BlockSpec(memory_space=pl.ANY)
    vmem = pl.BlockSpec(memory_space=pltpu.VMEM)
    dma = pltpu.SemaphoreType.DMA
    return pl.pallas_call(
        mega_kernel,
        out_shape=jax.ShapeDtypeStruct((rows, depth), half_type),
        in_specs=[hbm, hbm, hbm, vmem, hbm, hbm, hbm, vmem, vmem, hbm, hbm, hbm, hbm],
        out_specs=hbm,
        scratch_shapes=[
            pltpu.VMEM((halo + tokens, channels), half_type),
            pltpu.VMEM((halo + tokens, channels), half_type),
            pltpu.VMEM((tokens, channels), half_type),
            pltpu.VMEM((channels, depth), half_type),
            pltpu.VMEM((rows, depth), half_type),
            pltpu.VMEM((rows, depth), half_type),
            pltpu.VMEM((tokens, channels), half_type),
            pltpu.VMEM((rows, depth), full),
            pltpu.VMEM((2, rows, depth), half_type),
            pltpu.VMEM((2, rows, depth), half_type),
            pltpu.VMEM((2, piece, depth), half_type),
            pltpu.VMEM((2, piece, depth), half_type),
            pltpu.VMEM((8, piece, depth), half_type),
            pltpu.VMEM((8, piece, lanes), half_type),
            pltpu.VMEM((13, piece, depth), half_type),
            pltpu.VMEM((8, piece, depth), half_type),
            pltpu.VMEM((8, piece, 2 * width), half_type),
            pltpu.VMEM((depth, width), half_type),
            pltpu.VMEM((depth, width), half_type),
            pltpu.VMEM((depth, width), half_type),
            pltpu.VMEM((depth, width), half_type),
            pltpu.VMEM((2 * width, depth), half_type),
            pltpu.VMEM((2, lanes, width), half_type),
            dma((10,)),
            dma((2,)),
            dma((2,)),
            dma((4,)),
            dma((4,)),
            dma((2,)),
            dma((2,)),
            dma((2,)),
            dma((2,)),
            dma((12,)),
            dma((12,)),
            dma((16,)),
            dma((8,)),
            dma((8,)),
            dma((13,)),
            dma((2,)),
        ],
        compiler_params=pltpu.CompilerParams(
            collective_id=0, has_side_effects=True, vmem_limit_bytes=60 * 1024 * 1024
        ),
        name="layer",
    )(
        conv_outer, conv_inner, conv_input, conv_taps, out_weight, mix_gate, residual,
        mix_gain[None, :], expert_gain[None, :], table, gate_experts, up_experts, down_experts,
    )


def solution(mesh):
    placed = (
        P("sp", "tp"),
        P("sp", "tp"),
        P("sp", "tp"),
        P(None, "tp"),
        P("tp", None),
        P(("sp", "tp"), None),
        P(("sp", "tp"), None),
        P(),
        P(),
        P(("sp", "tp"), None),
        P(("sp", "tp")),
        P(("sp", "tp"), None),
        P("sp", None, None),
        P("sp", None, None),
        P("sp", None, None),
    )

    square = mesh.shape["tp"] == 4 and mesh.shape["sp"] == 8

    def layer(*arrays):
        return (mega if square else per_device)(*arrays)

    return jax.shard_map(
        layer, mesh=mesh, in_specs=placed, out_specs=P(("sp", "tp"), None), check_vma=False
    )
```

```python
import jax
import jax.numpy as jnp
from jax import lax
from jax.experimental import pallas as pl
from jax.experimental.pallas import tpu as pltpu
from jax.sharding import PartitionSpec as P

epsilon = 1e-06


def f32(value):
    return value.astype(jnp.float32)


def bf16(value):
    return value.astype(jnp.bfloat16)


def rms_scale(values, gain):
    return values * lax.rsqrt(jnp.mean(values * values, axis=-1, keepdims=True) + epsilon) * gain


def shifted(value, steps, senders):
    return lax.ppermute(value, "sp", [(s, s + steps) for s in senders])


def swapped(value, axis, bit):
    return lax.ppermute(value, axis, [(s, s ^ bit) for s in range(lax.axis_size(axis))])


def mixer_rows(conv_outer, conv_inner, conv_input, conv_taps):
    kept = conv_taps.shape[0] - 1
    inner = f32(conv_inner) * f32(conv_input)
    tail = f32(conv_inner[-kept:]) * f32(conv_input[-kept:])
    earlier = shifted(tail, 1, range(lax.axis_size("sp") - 1))
    length = conv_inner.shape[0]
    inner = jnp.concatenate([earlier, inner], 0)
    conv = conv_taps[0] * inner[0:length]
    for offset in range(1, kept + 1):
        conv = conv + conv_taps[offset] * inner[offset : offset + length]
    return bf16(f32(conv_outer) * conv)


def project(mixed_rows, out_weight, own_rows):
    parts = lax.axis_size("tp")
    me = lax.axis_index("tp")
    blocks = mixed_rows.reshape(parts, own_rows, -1)

    def partial(owner):
        rows = lax.dynamic_index_in_dim(blocks, owner, 0, keepdims=False)
        return jnp.dot(rows, out_weight, preferred_element_type=jnp.float32)

    def total(owner_bits, bit):
        if bit == 1:
            return partial(me ^ owner_bits)
        half = bit // 2
        sent = bf16(total(owner_bits | half, half))
        given = swapped(sent, "tp", half)
        return total(owner_bits, half) + f32(given)

    return total(0, parts)


def routing_table(expert_ids, group_share, pair_scores, own_rows, count):
    weights = group_share[:, None] * jax.nn.softmax(pair_scores, axis=-1)
    lanes = -(-2 * count // 128) * 128
    column = jnp.arange(lanes, dtype=jnp.int32)[None, :]
    coarse = lax.reduce_precision(weights, 8, 7)
    fine = weights - coarse
    table = jnp.zeros((own_rows, lanes), jnp.float32)
    for slot in range(expert_ids.shape[1]):
        at = expert_ids[:, slot : slot + 1]
        table = table + jnp.where(column == at, coarse[:, slot : slot + 1], 0.0)
        table = table + jnp.where(column == at + count, fine[:, slot : slot + 1], 0.0)
    return bf16(table)


def per_device(
    conv_outer,
    conv_inner,
    conv_input,
    conv_taps,
    out_weight,
    mix_gate,
    residual,
    mix_gain,
    expert_gain,
    expert_ids,
    group_share,
    pair_scores,
    gate_experts,
    up_experts,
    down_experts,
):
    count = lax.axis_size("sp")
    me = lax.axis_index("sp")
    own_rows = residual.shape[0]
    groups = count // 2
    place = me // 2
    side = lax.axis_index("tp") % 2
    half = gate_experts.shape[2] // 2

    def fetched(weight, axis):
        piece = lax.dynamic_slice_in_dim(weight[0], side * half, half, axis)
        first = swapped(piece, "sp", 1)
        second = swapped(first, "tp", 1)
        return jnp.concatenate([weight[0], first, second], axis)

    gate_both = fetched(gate_experts, 1)
    up_both = fetched(up_experts, 1)
    down_both = fetched(down_experts, 0)

    lanes = -(-2 * count // 128) * 128
    table = routing_table(expert_ids, group_share, pair_scores, own_rows, count)

    def spread(own):
        below, above = {0: own}, {0: own}
        for step in range(1, groups):
            below[step] = shifted(below[step - 1], 2, range(2 * (step - 1), count - 2))
            above[step] = shifted(above[step - 1], -2, range(2, count - 2 * (step - 1)))
        order = {0: own}
        for near in range(1, (groups - 1) // 2 + 1):
            far = groups - near
            early = jnp.where(place < near, above[near], below[near])
            _, over, under, away = lax.optimization_barrier(
                (early, above[near], below[far], above[far])
            )
            order[near] = early
            late = jnp.where(place < far, over, under)
            order[far] = jnp.where(place < near, away, late)
        if groups % 2 == 0:
            mid = groups // 2
            order[mid] = jnp.where(place < mid, above[mid], below[mid])
        return order

    mixed_rows = mixer_rows(conv_outer, conv_inner, conv_input, conv_taps)
    projected = project(mixed_rows, out_weight, own_rows)
    mixed = jax.nn.sigmoid(f32(mix_gate)) * projected
    hidden_state = bf16(f32(residual) + rms_scale(mixed, mix_gain))
    normed = bf16(rms_scale(f32(hidden_state), expert_gain))

    blocks = spread(jnp.concatenate([normed, table], 1))
    depth = normed.shape[1]

    def served(block):
        rows = block[:, :depth]
        chosen = jnp.arange(lanes, dtype=jnp.int32)[:, None] % count
        picks = bf16(chosen == jnp.stack([me, me ^ 1])[None, :])
        picks = jnp.where(jnp.arange(lanes)[:, None] < 2 * count, picks, 0)
        shares = jnp.dot(block[:, depth:], picks, preferred_element_type=jnp.float32)
        wide = 2 * half
        first = jnp.dot(rows, gate_both, preferred_element_type=jnp.float32)
        second = jnp.dot(rows, up_both, preferred_element_type=jnp.float32)
        mine = jnp.arange(2 * wide)[None, :] < wide
        share = jnp.where(mine, shares[:, :1], shares[:, 1:])
        hidden = lax.optimization_barrier(bf16(jax.nn.silu(first) * second * share))
        return lax.optimization_barrier(
            jnp.dot(hidden, down_both, preferred_element_type=jnp.float32)
        )

    results = {number: served(block) for number, block in blocks.items()}

    def for_upper(step):
        gone = groups - step
        if step == gone or step < gone:
            return results[gone]
        return jnp.where(place < gone, results[gone], results[step])

    down = up = None
    for step in range(1, groups):
        gone = groups - step
        lower, upper = results[gone], for_upper(step)
        if down is not None:
            lower, upper = lower + f32(down), upper + f32(up)
        down = shifted(bf16(lower), -2, range(2 * gone, count))
        up = shifted(bf16(upper), 2, range(0, count - 2 * gone))
    result = f32(hidden_state) + results[0]
    if down is not None:
        result = result + f32(down) + f32(up)
    return bf16(result)


MESH_ID = pl.DeviceIdType.MESH
OWN, OTHER, OUT, ARRIVE, FORWARD = 8, 16, 32, 64, 128

OUTER_STEPS = (
    0 | OWN,
    1 | OWN,
    2 | OWN | ARRIVE,
    4 | OWN | ARRIVE,
    0,
    0,
    4 | OTHER | OUT,
    2 | OTHER,
    6 | OWN | OTHER | OUT | ARRIVE,
    0 | OTHER,
    7 | OWN | OTHER | OUT | ARRIVE,
    1 | OTHER,
    5 | OWN | OTHER | OUT | ARRIVE,
    2 | OUT,
    3 | OWN | OTHER | OUT | ARRIVE,
    0 | OUT,
    1 | OUT,
    0,
    0,
    0,
    0,
    0,
)
INNER_STEPS = (
    2 | OWN,
    3 | OWN,
    0 | OWN | ARRIVE | FORWARD,
    4 | OWN | ARRIVE | FORWARD,
    1 | OWN | ARRIVE | FORWARD,
    6 | OWN | ARRIVE | FORWARD,
    4 | OTHER,
    6 | OTHER,
    7 | OWN | OTHER | ARRIVE | FORWARD,
    4 | OUT,
    5 | OWN | OTHER | ARRIVE | FORWARD,
    6 | OUT,
    1 | OTHER,
    0 | OTHER,
    7 | OUT,
    0 | OUT,
    2 | OTHER,
    5 | OUT,
    1 | OUT,
    3 | OTHER,
    2 | OUT,
    3 | OUT,
)
WEIGHTS_STEP = 6
LATE_ACROSS = 4
LATE_OUTWARD = 10


def mega_kernel(
    co_hbm, ci_hbm, cx_hbm, taps, ow_hbm, mg_hbm, res_hbm, mgain, egain, ids, scores, group,
    g_hbm, u_hbm, d_hbm, out_hbm,
    ci, cx, co, ow, mg, res, mix, acc, part_out, part_in, x_out, x_in,
    X, T, P, S, H, g1, u1, g2, u2, wd, picks,
    load_sem, halo_s, halo_r, tab_s, tab_r, core_s, core_r, xsw_s, xsw_r,
    w_s, w_r, rows_s, rows_r, sum_s, sum_r, out_sem,
):
    sp = lax.axis_index("sp")
    tp = lax.axis_index("tp")
    z = sp // 2
    y = sp % 2
    half = z // 2
    outer = z * (3 - z) == 0
    inner = jnp.logical_not(outer)
    own = jnp.where(outer, 0, 1)
    core_peer = tp + 1 - 2 * (tp % 2)
    x_peer = (tp + 2) % 4
    y_peer = sp + 1 - 2 * y
    rows, depth = res.shape
    piece = rows // 2
    width = g1.shape[1]
    count = T.shape[1] // 2
    channels = ow.shape[0]
    halo = ci.shape[0] - co.shape[0]

    def line(slot):
        where = jnp.where(slot == 0, 3 * half, jnp.where(slot == 1, 1 + half, jnp.where(slot == 2, 2 - half, 3 - 3 * half)))
        return 2 * where + y

    def remote(src, dst, s, r, device):
        return pltpu.make_async_remote_copy(
            src_ref=src, dst_ref=dst, send_sem=s, recv_sem=r, device_id=device, device_id_type=MESH_ID
        )

    tokens = co.shape[0]
    loads = [
        pltpu.make_async_copy(ci_hbm, ci.at[pl.ds(halo, tokens)], load_sem.at[0]),
        pltpu.make_async_copy(cx_hbm, cx.at[pl.ds(halo, tokens)], load_sem.at[1]),
        pltpu.make_async_copy(co_hbm, co, load_sem.at[2]),
        pltpu.make_async_copy(ow_hbm, ow, load_sem.at[3]),
        pltpu.make_async_copy(mg_hbm, mg, load_sem.at[4]),
        pltpu.make_async_copy(res_hbm, res, load_sem.at[5]),
        pltpu.make_async_copy(g_hbm.at[0], g1, load_sem.at[6]),
        pltpu.make_async_copy(u_hbm.at[0], u1, load_sem.at[7]),
        pltpu.make_async_copy(d_hbm.at[0], wd.at[pl.ds(0, width)], load_sem.at[8]),
    ]
    for k in (0, 1, 3, 2):
        loads[k].start()

    raw = scores[...]
    top = jnp.maximum(raw[0:1], raw[1:2])
    up = jnp.exp(raw - top)
    weights = group[...] * (up / (up[0:1] + up[1:2]))
    coarse = f32(bf16(weights))
    fine = weights - coarse
    line_of = lax.broadcasted_iota(jnp.int32, (T.shape[1], rows), 0)
    entries = jnp.zeros((T.shape[1], rows), jnp.float32)
    for k in range(2):
        entries = entries + jnp.where(line_of == ids[k : k + 1], coarse[k : k + 1], 0.0)
        entries = entries + jnp.where(line_of == ids[k : k + 1] + count, fine[k : k + 1], 0.0)
    entries = bf16(entries)
    for p in range(2):
        T[2 * own + p] = entries[:, (1 - p) * piece : (2 - p) * piece]

    barrier = pltpu.get_barrier_semaphore()

    def greet(device):
        pl.semaphore_signal(barrier, inc=1, device_id=device, device_id_type=MESH_ID)

    greet((sp, core_peer))
    greet((sp, x_peer))
    greet((y_peer, tp))
    for away in range(1, 4):
        greet(((sp + 2 * away) % count, tp))
    has_next = jnp.logical_and(y == 1, sp < count - 1)
    has_last = jnp.logical_and(y == 0, sp > 0)

    @pl.when(has_next)
    def _():
        greet((sp + 1, tp))

    @pl.when(has_last)
    def _():
        greet((sp - 1, tp))

    pl.semaphore_wait(barrier, 6 + jnp.where(has_next, 1, 0) + jnp.where(has_last, 1, 0))

    def halo_copy(k, device):
        src = (ci_hbm, cx_hbm)[k].at[pl.ds(tokens - halo, halo)]
        return remote(src, (ci, cx)[k].at[pl.ds(0, halo)], halo_s.at[k], halo_r.at[k], device)

    @pl.when(sp < count - 1)
    def _():
        for k in range(2):
            halo_copy(k, (sp + 1, tp)).start()

    quarter = depth // 4
    wide = width // 2
    mine = pl.multiple_of(tp * quarter, quarter)
    theirs = pl.multiple_of(x_peer * quarter, quarter)
    side = tp % 2

    def weight_copy(k, leg):
        at = 4 * k + leg
        if k < 2:
            buf = (g2, u2)[k]
            rows_at = pl.ds(theirs if leg == 3 else mine, quarter)
            src = (g_hbm, u_hbm)[k].at[0, rows_at] if leg == 0 else buf.at[rows_at]
            dst = buf.at[rows_at]
        else:
            rows_at = pl.ds(pl.multiple_of(width + side * wide, wide), wide)
            src = d_hbm.at[0, pl.ds(pl.multiple_of(side * wide, wide), wide)] if leg == 0 else wd.at[rows_at]
            dst = wd.at[rows_at]
        device = ((y_peer, tp), (sp, core_peer), (sp, x_peer), (sp, core_peer))[leg]
        return remote(src, dst, w_s.at[at], w_r.at[at], device)

    for k in range(3):
        weight_copy(k, 0).start()

    def table_copy(away):
        zz = (z + away) % 4
        same = zz // 2 == half
        slot = jnp.where(same, own, 3 - own)
        return remote(
            T.at[pl.ds(2 * own, 2)],
            T.at[pl.ds(2 * slot, 2)],
            tab_s.at[away],
            tab_r.at[slot],
            ((sp + 2 * away) % count, tp),
        )

    for away in range(1, 4):
        table_copy(away).start()

    P[0] = jnp.zeros(P.shape[1:], P.dtype)
    lane = lax.broadcasted_iota(jnp.int32, (T.shape[1], width), 0)
    for k in range(2):
        picks[k] = jnp.where(lane % count == (sp, y_peer)[k], 1.0, 0.0).astype(picks.dtype)

    for k in range(3):
        loads[k].wait()
    for k in range(4, 9):
        loads[k].start()

    kept = taps.shape[0] - 1
    run = 32

    def conv(start):
        def some(i, c):
            at = pl.multiple_of(start + i * run, run)
            near = f32(ci[pl.ds(at, halo + run)]) * f32(cx[pl.ds(at, halo + run)])
            total = taps[0:1] * near[halo - kept : halo - kept + run]
            for j in range(1, kept + 1):
                total = total + taps[j : j + 1] * near[halo - kept + j : halo - kept + j + run]
            mix[pl.ds(at, run)] = bf16(f32(co[pl.ds(at, run)]) * total)
            return c

        lax.fori_loop(0, piece // run, some, 0)

    tile = min(512, depth)
    loads[3].wait()

    def core_copy(phase, p):
        at = 2 * phase + p
        return remote(part_out.at[at], part_in.at[at], core_s.at[at], core_r.at[at], (sp, core_peer))

    def x_copy(p):
        return remote(x_out.at[p], x_in.at[p], xsw_s.at[p], xsw_r.at[p], (sp, x_peer))

    def projected(i, carry):
        phase = i // 4
        p = i // 2 % 2
        second = i % 2 == 1
        owner = jnp.where(
            phase == 0, jnp.where(second, x_peer, 3 - tp), jnp.where(second, tp, core_peer)
        )
        start = pl.multiple_of(owner * rows + (1 - p) * piece, piece)

        @pl.when(jnp.logical_and(i == 2, sp == 0))
        def _():
            ci[pl.ds(0, halo)] = jnp.zeros((halo, channels), ci.dtype)
            cx[pl.ds(0, halo)] = jnp.zeros((halo, channels), cx.dtype)

        @pl.when(jnp.logical_and(i == 2, sp > 0))
        def _():
            for k in range(2):
                halo_copy(k, (sp, core_peer)).wait_recv()

        conv(start)

        def some(n, c):
            cols = pl.ds(pl.multiple_of(n * tile, tile), tile)
            got = jnp.dot(mix[pl.ds(start, piece)], ow[:, cols], preferred_element_type=jnp.float32)

            @pl.when(second)
            def _():
                acc[p, :, cols] = got

            @pl.when(jnp.logical_not(second))
            def _():
                part_out[2 * phase + p, :, cols] = bf16(got)

            return c

        lax.fori_loop(0, depth // tile, some, 0)

        @pl.when(jnp.logical_not(second))
        def _():
            core_copy(phase, p).start()

        @pl.when(jnp.logical_and(second, phase == 0))
        def _():
            core_copy(0, p).wait_recv()

            def add(r, c):
                at = pl.ds(pl.multiple_of(r * 16, 16), 16)
                x_out[p, at] = bf16(acc[p, at] + f32(part_in[p, at]))
                return c

            lax.fori_loop(0, piece // 16, add, 0)
            x_copy(p).start()

        return carry

    lax.fori_loop(0, 8, projected, 0)
    loads[4].wait()
    loads[5].wait()

    def rows_copy(item, device, dst, at):
        return remote(X.at[item], X.at[dst], rows_s.at[at], rows_r.at[dst], device)

    def normalize(c):
        def some(r, carry):
            at = pl.ds(pl.multiple_of(r * 16, 16), 16)
            src = pl.ds(pl.multiple_of((1 - c) * piece + r * 16, 16), 16)
            total = acc[c, at] + f32(part_in[2 + c, at]) + f32(x_in[c, at])
            mixed = jax.nn.sigmoid(f32(mg[src])) * total
            state = bf16(f32(res[src]) + rms_scale(mixed, mgain[...]))
            P[1 + c, at] = state
            X[2 * own + c, at] = bf16(rms_scale(f32(state), egain[...]))
            return carry

        lax.fori_loop(0, piece // 16, some, 0)

    def send_own(c, across):
        item = 2 * own + c
        if across:
            rows_copy(item, (line(2), tp), 4 + c, 8 + c).start()
        else:
            rows_copy(item, (line(1 - own), tp), item, item).start()

    def relay(k, leg):
        weight_copy(k, leg).wait_recv()

    relay(0, 0)
    weight_copy(0, 1).start()
    weight_copy(0, 2).start()
    core_copy(1, 0).wait_recv()
    x_copy(0).wait_recv()
    normalize(0)
    send_own(0, False)

    @pl.when(inner)
    def _():
        send_own(0, True)

    core_copy(1, 1).wait_recv()
    x_copy(1).wait_recv()
    normalize(1)

    @pl.when(outer)
    def _():
        send_own(1, False)

    relay(1, 0)
    weight_copy(1, 1).start()
    weight_copy(1, 2).start()
    for k in range(6, 9):
        loads[k].wait()
    for away in range(1, 4):
        slot = (own + away) % 4
        at = T.at[pl.ds(2 * slot, 2)]
        remote(at, at, tab_s.at[away], tab_r.at[slot], (sp, core_peer)).wait_recv()

    def hidden(item, k):
        gate, up = ((g1, u1), (g2, u2))[k]
        x = X[item]
        first = jnp.dot(x, gate[...], preferred_element_type=jnp.float32)
        second = jnp.dot(x, up[...], preferred_element_type=jnp.float32)
        share = lax.dot_general(
            T[item], picks[k], (((0,), (0,)), ((), ())), preferred_element_type=jnp.float32
        )
        H[item, :, k * width : (k + 1) * width] = bf16(jax.nn.silu(first) * second * share)

    def sum_copy(item):
        slot = item // 2
        c = item % 2
        to = jnp.where(outer, 1, jnp.where(slot == 0, 0, 2))
        dst = jnp.where(
            outer, 1 + item, jnp.where(slot == 0, 9 + c, jnp.where(slot == 2, 11 + c, 9 + c))
        )
        return remote(S.at[item], P.at[dst], sum_s.at[item], sum_r.at[dst], (line(to), tp))

    def out_copy(c):
        return pltpu.make_async_copy(
            S.at[2 * own + c], out_hbm.at[pl.ds(pl.multiple_of((1 - c) * piece, piece), piece)], out_sem.at[c]
        )

    def came(at):
        remote(S.at[0], P.at[at], sum_s.at[0], sum_r.at[at], (sp, core_peer)).wait_recv()

    def step(n, carry):
        code = 0
        for i, (a, b) in enumerate(zip(OUTER_STEPS, INNER_STEPS)):
            code = jnp.where(n == i, jnp.where(outer, a, b), code)
        item = code % 8

        def has(flag):
            return code // flag % 2 == 1

        slot = item // 2
        c = item % 2

        @pl.when(has(ARRIVE))
        def _():
            rows_copy(item, (sp, core_peer), item, item).wait_recv()

        @pl.when(has(FORWARD))
        def _():
            across = slot == 0
            rows_copy(
                item,
                (line(jnp.where(across, 2, 0)), tp),
                jnp.where(across, 6 + c, item),
                jnp.where(across, 10 + c, item),
            ).start()

        @pl.when(jnp.logical_and(inner, n == LATE_ACROSS))
        def _():
            send_own(1, True)

        @pl.when(jnp.logical_and(inner, n == LATE_OUTWARD))
        def _():
            send_own(1, False)

        @pl.when(n == WEIGHTS_STEP)
        def _():
            relay(0, 2)
            weight_copy(0, 3).start()
            relay(1, 2)
            weight_copy(1, 3).start()
            relay(2, 0)
            weight_copy(2, 1).start()
            for k, leg in ((0, 1), (1, 1), (0, 3), (1, 3), (2, 1)):
                got = pl.multiple_of((core_peer if leg == 1 else 3 - tp) * quarter, quarter)
                if k < 2:
                    at = (g2, u2)[k].at[pl.ds(got, quarter)]
                else:
                    at = wd.at[pl.ds(pl.multiple_of(width + (1 - side) * wide, wide), wide)]
                remote(at, at, w_s.at[4 * k + leg], w_r.at[4 * k + leg], (sp, core_peer)).wait_recv()

        @pl.when(has(OWN))
        def _():
            hidden(item, 0)

        @pl.when(has(OTHER))
        def _():
            hidden(item, 1)

        @pl.when(has(OUT))
        def _():
            a = jnp.where(slot == 0, 9 + c, jnp.where(outer, 0, 1 + item))
            b = jnp.where(outer, 0, jnp.where(slot == 1, 11 + c, 0))
            d = jnp.where(slot == own, 1 + c, 0)

            @pl.when(a > 0)
            def _():
                came(a)

            @pl.when(b > 0)
            def _():
                came(b)

            def some(m, carry):
                cols = pl.ds(pl.multiple_of(m * tile, tile), tile)
                got = jnp.dot(H[item], wd[:, cols], preferred_element_type=jnp.float32)
                got = got + f32(P[d, :, cols]) + f32(P[a, :, cols]) + f32(P[b, :, cols])
                S[item, :, cols] = bf16(got)
                return carry

            lax.fori_loop(0, depth // tile, some, 0)

            @pl.when(slot == own)
            def _():
                out_copy(c).start()

            @pl.when(slot != own)
            def _():
                sum_copy(item).start()

        return carry

    lax.fori_loop(0, len(OUTER_STEPS), step, 0)

    for c in range(2):
        out_copy(c).wait()
        core_copy(0, c).wait_send()
        core_copy(1, c).wait_send()
        x_copy(c).wait_send()

    @pl.when(sp < count - 1)
    def _():
        for k in range(2):
            halo_copy(k, (sp + 1, tp)).wait_send()

    for k in range(3):
        for leg in range(4 if k < 2 else 2):
            weight_copy(k, leg).wait_send()
    for away in range(1, 4):
        table_copy(away).wait_send()

    def gone(item, at):
        rows_copy(item, (sp, core_peer), item, at).wait_send()

    for c in range(2):
        gone(2 * own + c, 2 * own + c)
    for i in range(3):
        for c in range(2):
            item = 2 * ((own + 1 + i) % 4) + c
            remote(S.at[item], P.at[0], sum_s.at[item], sum_r.at[0], (sp, core_peer)).wait_send()

    @pl.when(inner)
    def _():
        for c in range(2):
            for at in (4 + c, 6 + c, 8 + c, 10 + c):
                gone(at % 8, at)


def mega(
    conv_outer, conv_inner, conv_input, conv_taps, out_weight, mix_gate, residual, mix_gain, expert_gain,
    expert_ids, group_share, pair_scores, gate_experts, up_experts, down_experts,
):
    count = lax.axis_size("sp")
    rows, depth = residual.shape
    tokens, channels = conv_inner.shape
    width = gate_experts.shape[2]
    piece = rows // 2
    halo = 16
    half_type, full = jnp.bfloat16, jnp.float32
    hbm = pl.BlockSpec(memory_space=pl.ANY)
    vmem = pl.BlockSpec(memory_space=pltpu.VMEM)
    dma = pltpu.SemaphoreType.DMA
    return pl.pallas_call(
        mega_kernel,
        out_shape=jax.ShapeDtypeStruct((rows, depth), half_type),
        in_specs=[hbm, hbm, hbm, vmem, hbm, hbm, hbm, vmem, vmem, vmem, vmem, vmem, hbm, hbm, hbm],
        out_specs=hbm,
        scratch_shapes=[
            pltpu.VMEM((halo + tokens, channels), half_type),
            pltpu.VMEM((halo + tokens, channels), half_type),
            pltpu.VMEM((tokens, channels), half_type),
            pltpu.VMEM((channels, depth), half_type),
            pltpu.VMEM((rows, depth), half_type),
            pltpu.VMEM((rows, depth), half_type),
            pltpu.VMEM((tokens, channels), half_type),
            pltpu.VMEM((2, piece, depth), full),
            pltpu.VMEM((4, piece, depth), half_type),
            pltpu.VMEM((4, piece, depth), half_type),
            pltpu.VMEM((2, piece, depth), half_type),
            pltpu.VMEM((2, piece, depth), half_type),
            pltpu.VMEM((8, piece, depth), half_type),
            pltpu.VMEM((8, 2 * count, piece), half_type),
            pltpu.VMEM((13, piece, depth), half_type),
            pltpu.VMEM((8, piece, depth), half_type),
            pltpu.VMEM((8, piece, 2 * width), half_type),
            pltpu.VMEM((depth, width), half_type),
            pltpu.VMEM((depth, width), half_type),
            pltpu.VMEM((depth, width), half_type),
            pltpu.VMEM((depth, width), half_type),
            pltpu.VMEM((2 * width, depth), half_type),
            pltpu.VMEM((2, 2 * count, width), half_type),
            dma((9,)),
            dma((2,)),
            dma((2,)),
            dma((4,)),
            dma((4,)),
            dma((4,)),
            dma((4,)),
            dma((2,)),
            dma((2,)),
            dma((12,)),
            dma((12,)),
            dma((16,)),
            dma((8,)),
            dma((8,)),
            dma((13,)),
            dma((2,)),
        ],
        compiler_params=pltpu.CompilerParams(
            collective_id=0, has_side_effects=True, vmem_limit_bytes=60 * 1024 * 1024
        ),
        name="layer",
    )(
        conv_outer, conv_inner, conv_input, conv_taps, out_weight, mix_gate, residual,
        mix_gain[None, :], expert_gain[None, :], expert_ids.T, pair_scores.T, group_share[None, :], gate_experts, up_experts, down_experts,
    )


def solution(mesh):
    placed = (
        P("sp", "tp"),
        P("sp", "tp"),
        P("sp", "tp"),
        P(None, "tp"),
        P("tp", None),
        P(("sp", "tp"), None),
        P(("sp", "tp"), None),
        P(),
        P(),
        P(("sp", "tp"), None),
        P(("sp", "tp")),
        P(("sp", "tp"), None),
        P("sp", None, None),
        P("sp", None, None),
        P("sp", None, None),
    )

    square = mesh.shape["tp"] == 4 and mesh.shape["sp"] == 8

    def layer(*arrays):
        return (mega if square else per_device)(*arrays)

    return jax.shard_map(
        layer, mesh=mesh, in_specs=placed, out_specs=P(("sp", "tp"), None), check_vma=False
    )
```

```python
import jax
import jax.numpy as jnp
from jax import lax
from jax.experimental import pallas as pl
from jax.experimental.pallas import tpu as pltpu
from jax.sharding import PartitionSpec as P

epsilon = 1e-06


def f32(value):
    return value.astype(jnp.float32)


def bf16(value):
    return value.astype(jnp.bfloat16)


def rms_scale(values, gain):
    return values * lax.rsqrt(jnp.mean(values * values, axis=-1, keepdims=True) + epsilon) * gain


def shifted(value, steps, senders):
    return lax.ppermute(value, "sp", [(s, s + steps) for s in senders])


def swapped(value, axis, bit):
    return lax.ppermute(value, axis, [(s, s ^ bit) for s in range(lax.axis_size(axis))])


def mixer_rows(conv_outer, conv_inner, conv_input, conv_taps):
    kept = conv_taps.shape[0] - 1
    inner = f32(conv_inner) * f32(conv_input)
    tail = f32(conv_inner[-kept:]) * f32(conv_input[-kept:])
    earlier = shifted(tail, 1, range(lax.axis_size("sp") - 1))
    length = conv_inner.shape[0]
    inner = jnp.concatenate([earlier, inner], 0)
    conv = conv_taps[0] * inner[0:length]
    for offset in range(1, kept + 1):
        conv = conv + conv_taps[offset] * inner[offset : offset + length]
    return bf16(f32(conv_outer) * conv)


def project(mixed_rows, out_weight, own_rows):
    parts = lax.axis_size("tp")
    me = lax.axis_index("tp")
    blocks = mixed_rows.reshape(parts, own_rows, -1)

    def partial(owner):
        rows = lax.dynamic_index_in_dim(blocks, owner, 0, keepdims=False)
        return jnp.dot(rows, out_weight, preferred_element_type=jnp.float32)

    def total(owner_bits, bit):
        if bit == 1:
            return partial(me ^ owner_bits)
        half = bit // 2
        sent = bf16(total(owner_bits | half, half))
        given = swapped(sent, "tp", half)
        return total(owner_bits, half) + f32(given)

    return total(0, parts)


def routing_table(expert_ids, group_share, pair_scores, own_rows, count):
    weights = group_share[:, None] * jax.nn.softmax(pair_scores, axis=-1)
    lanes = -(-2 * count // 128) * 128
    column = jnp.arange(lanes, dtype=jnp.int32)[None, :]
    coarse = lax.reduce_precision(weights, 8, 7)
    fine = weights - coarse
    table = jnp.zeros((own_rows, lanes), jnp.float32)
    for slot in range(expert_ids.shape[1]):
        at = expert_ids[:, slot : slot + 1]
        table = table + jnp.where(column == at, coarse[:, slot : slot + 1], 0.0)
        table = table + jnp.where(column == at + count, fine[:, slot : slot + 1], 0.0)
    return bf16(table)


def per_device(
    conv_outer,
    conv_inner,
    conv_input,
    conv_taps,
    out_weight,
    mix_gate,
    residual,
    mix_gain,
    expert_gain,
    expert_ids,
    group_share,
    pair_scores,
    gate_experts,
    up_experts,
    down_experts,
):
    count = lax.axis_size("sp")
    me = lax.axis_index("sp")
    own_rows = residual.shape[0]
    groups = count // 2
    place = me // 2
    side = lax.axis_index("tp") % 2
    half = gate_experts.shape[2] // 2

    def fetched(weight, axis):
        piece = lax.dynamic_slice_in_dim(weight[0], side * half, half, axis)
        first = swapped(piece, "sp", 1)
        second = swapped(first, "tp", 1)
        return jnp.concatenate([weight[0], first, second], axis)

    gate_both = fetched(gate_experts, 1)
    up_both = fetched(up_experts, 1)
    down_both = fetched(down_experts, 0)

    lanes = -(-2 * count // 128) * 128
    table = routing_table(expert_ids, group_share, pair_scores, own_rows, count)

    def spread(own):
        below, above = {0: own}, {0: own}
        for step in range(1, groups):
            below[step] = shifted(below[step - 1], 2, range(2 * (step - 1), count - 2))
            above[step] = shifted(above[step - 1], -2, range(2, count - 2 * (step - 1)))
        order = {0: own}
        for near in range(1, (groups - 1) // 2 + 1):
            far = groups - near
            early = jnp.where(place < near, above[near], below[near])
            _, over, under, away = lax.optimization_barrier(
                (early, above[near], below[far], above[far])
            )
            order[near] = early
            late = jnp.where(place < far, over, under)
            order[far] = jnp.where(place < near, away, late)
        if groups % 2 == 0:
            mid = groups // 2
            order[mid] = jnp.where(place < mid, above[mid], below[mid])
        return order

    mixed_rows = mixer_rows(conv_outer, conv_inner, conv_input, conv_taps)
    projected = project(mixed_rows, out_weight, own_rows)
    mixed = jax.nn.sigmoid(f32(mix_gate)) * projected
    hidden_state = bf16(f32(residual) + rms_scale(mixed, mix_gain))
    normed = bf16(rms_scale(f32(hidden_state), expert_gain))

    blocks = spread(jnp.concatenate([normed, table], 1))
    depth = normed.shape[1]

    def served(block):
        rows = block[:, :depth]
        chosen = jnp.arange(lanes, dtype=jnp.int32)[:, None] % count
        picks = bf16(chosen == jnp.stack([me, me ^ 1])[None, :])
        picks = jnp.where(jnp.arange(lanes)[:, None] < 2 * count, picks, 0)
        shares = jnp.dot(block[:, depth:], picks, preferred_element_type=jnp.float32)
        wide = 2 * half
        first = jnp.dot(rows, gate_both, preferred_element_type=jnp.float32)
        second = jnp.dot(rows, up_both, preferred_element_type=jnp.float32)
        mine = jnp.arange(2 * wide)[None, :] < wide
        share = jnp.where(mine, shares[:, :1], shares[:, 1:])
        hidden = lax.optimization_barrier(bf16(jax.nn.silu(first) * second * share))
        return lax.optimization_barrier(
            jnp.dot(hidden, down_both, preferred_element_type=jnp.float32)
        )

    results = {number: served(block) for number, block in blocks.items()}

    def for_upper(step):
        gone = groups - step
        if step == gone or step < gone:
            return results[gone]
        return jnp.where(place < gone, results[gone], results[step])

    down = up = None
    for step in range(1, groups):
        gone = groups - step
        lower, upper = results[gone], for_upper(step)
        if down is not None:
            lower, upper = lower + f32(down), upper + f32(up)
        down = shifted(bf16(lower), -2, range(2 * gone, count))
        up = shifted(bf16(upper), 2, range(0, count - 2 * gone))
    result = f32(hidden_state) + results[0]
    if down is not None:
        result = result + f32(down) + f32(up)
    return bf16(result)


MESH_ID = pl.DeviceIdType.MESH
OWN, OTHER, OUT, ARRIVE, FORWARD = 8, 16, 32, 64, 128

OUTER_STEPS = (
    0 | OWN,
    1 | OWN,
    2 | OWN | ARRIVE,
    4 | OWN | ARRIVE,
    6 | OWN | ARRIVE,
    0,
    6 | OTHER | OUT,
    4 | OTHER,
    7 | OWN | OTHER | OUT | ARRIVE,
    4 | OUT,
    2 | OTHER | OUT,
    5 | OWN | OTHER | OUT | ARRIVE,
    3 | OWN | OTHER | OUT | ARRIVE,
    0 | OTHER,
    1 | OTHER,
    0 | OUT,
    1 | OUT,
    0,
    0,
    0,
    0,
    0,
    0,
)
INNER_STEPS = (
    2 | OWN,
    3 | OWN,
    0 | OWN | ARRIVE | FORWARD,
    4 | OWN | ARRIVE | FORWARD,
    1 | OWN | ARRIVE | FORWARD,
    6 | OWN | ARRIVE | FORWARD,
    6 | OTHER,
    7 | OWN | OTHER | ARRIVE | FORWARD,
    6 | OUT,
    5 | OWN | ARRIVE | FORWARD,
    1 | OTHER,
    0 | OTHER,
    4 | OTHER,
    7 | OUT,
    0 | OUT,
    5 | OTHER,
    4 | OUT,
    1 | OUT,
    5 | OUT,
    2 | OTHER,
    3 | OTHER,
    2 | OUT,
    3 | OUT,
)
WEIGHTS_STEP = 6
LATE_ACROSS = 4
LATE_OUTWARD = 9
DOWN_RELAY = 15
DOWN_STEP = 16


def mega_kernel(
    co_hbm, ci_hbm, cx_hbm, taps, ow_hbm, mg_hbm, res_hbm, mgain, egain, ids, scores, group,
    g_hbm, u_hbm, d_hbm, out_hbm,
    ci, cx, co, ow, mg, res, mix, acc, part_out, part_in, x_out, x_in,
    X, T, P, S, H, HR, g1, u1, g2, u2, wd, wdo, picks,
    load_sem, halo_s, halo_r, tab_s, tab_r, core_s, core_r, xsw_s, xsw_r,
    w_s, w_r, rows_s, rows_r, sum_s, sum_r, hid_s, hid_r, do_s, do_r, out_sem,
):
    sp = lax.axis_index("sp")
    tp = lax.axis_index("tp")
    z = sp // 2
    y = sp % 2
    half = z // 2
    outer = z * (3 - z) == 0
    inner = jnp.logical_not(outer)
    own = jnp.where(outer, 0, 1)
    core_peer = tp + 1 - 2 * (tp % 2)
    x_peer = (tp + 2) % 4
    y_peer = sp + 1 - 2 * y
    rows, depth = res.shape
    piece = rows // 2
    width = g1.shape[1]
    count = T.shape[1] // 2
    channels = ow.shape[0]
    halo = ci.shape[0] - co.shape[0]

    def line(slot):
        where = jnp.where(slot == 0, 3 * half, jnp.where(slot == 1, 1 + half, jnp.where(slot == 2, 2 - half, 3 - 3 * half)))
        return 2 * where + y

    def remote(src, dst, s, r, device):
        return pltpu.make_async_remote_copy(
            src_ref=src, dst_ref=dst, send_sem=s, recv_sem=r, device_id=device, device_id_type=MESH_ID
        )

    barrier = pltpu.get_barrier_semaphore()

    def greet(device):
        pl.semaphore_signal(barrier, inc=1, device_id=device, device_id_type=MESH_ID)

    greet((sp, core_peer))
    greet((sp, x_peer))
    greet((y_peer, tp))
    for away in range(1, 4):
        greet(((sp + 2 * away) % count, tp))
    has_next = jnp.logical_and(y == 1, sp < count - 1)
    has_last = jnp.logical_and(y == 0, sp > 0)

    @pl.when(has_next)
    def _():
        greet((sp + 1, tp))

    @pl.when(has_last)
    def _():
        greet((sp - 1, tp))

    tokens = co.shape[0]
    loads = [
        pltpu.make_async_copy(ci_hbm, ci.at[pl.ds(halo, tokens)], load_sem.at[0]),
        pltpu.make_async_copy(cx_hbm, cx.at[pl.ds(halo, tokens)], load_sem.at[1]),
        pltpu.make_async_copy(co_hbm, co, load_sem.at[2]),
        pltpu.make_async_copy(ow_hbm, ow, load_sem.at[3]),
        pltpu.make_async_copy(mg_hbm, mg, load_sem.at[4]),
        pltpu.make_async_copy(res_hbm, res, load_sem.at[5]),
        pltpu.make_async_copy(g_hbm.at[0], g1, load_sem.at[6]),
        pltpu.make_async_copy(u_hbm.at[0], u1, load_sem.at[7]),
        pltpu.make_async_copy(d_hbm.at[0], wd.at[pl.ds(0, width)], load_sem.at[8]),
    ]
    for k in (0, 1, 3, 2):
        loads[k].start()

    raw = scores[...]
    top = jnp.maximum(raw[0:1], raw[1:2])
    up = jnp.exp(raw - top)
    weights = group[...] * (up / (up[0:1] + up[1:2]))
    coarse = f32(bf16(weights))
    fine = weights - coarse
    line_of = lax.broadcasted_iota(jnp.int32, (T.shape[1], rows), 0)
    entries = jnp.zeros((T.shape[1], rows), jnp.float32)
    for k in range(2):
        entries = entries + jnp.where(line_of == ids[k : k + 1], coarse[k : k + 1], 0.0)
        entries = entries + jnp.where(line_of == ids[k : k + 1] + count, fine[k : k + 1], 0.0)
    entries = bf16(entries)
    for p in range(2):
        T[2 * own + p] = entries[:, (1 - p) * piece : (2 - p) * piece]

    pl.semaphore_wait(barrier, 6 + jnp.where(has_next, 1, 0) + jnp.where(has_last, 1, 0))

    def halo_copy(k, device):
        src = (ci_hbm, cx_hbm)[k].at[pl.ds(tokens - halo, halo)]
        return remote(src, (ci, cx)[k].at[pl.ds(0, halo)], halo_s.at[k], halo_r.at[k], device)

    @pl.when(sp < count - 1)
    def _():
        for k in range(2):
            halo_copy(k, (sp + 1, tp)).start()

    quarter = depth // 4
    wide = width // 2
    mine = pl.multiple_of(tp * quarter, quarter)
    theirs = pl.multiple_of(x_peer * quarter, quarter)
    side = tp % 2

    def weight_copy(k, leg):
        at = 4 * k + leg
        if k < 2:
            buf = (g2, u2)[k]
            rows_at = pl.ds(theirs if leg == 3 else mine, quarter)
            src = (g_hbm, u_hbm)[k].at[0, rows_at] if leg == 0 else buf.at[rows_at]
            dst = buf.at[rows_at]
        else:
            rows_at = pl.ds(pl.multiple_of(width + side * wide, wide), wide)
            src = d_hbm.at[0, pl.ds(pl.multiple_of(side * wide, wide), wide)] if leg == 0 else wd.at[rows_at]
            dst = wd.at[rows_at]
        device = ((y_peer, tp), (sp, core_peer), (sp, x_peer), (sp, core_peer))[leg]
        return remote(src, dst, w_s.at[at], w_r.at[at], device)

    for k in range(3):
        weight_copy(k, 0).start()

    part = wide // 2

    def down_copy(leg):
        if leg < 2:
            src = d_hbm.at[0, pl.ds(pl.multiple_of(side * wide + leg * part, part), part)]
            dst = wdo.at[pl.ds(pl.multiple_of(side * wide + leg * part, part), part)]
            device = (line(1), tp)
        else:
            near = wdo.at[pl.ds(pl.multiple_of(side * wide, wide), wide)]
            far = wdo.at[pl.ds(pl.multiple_of(width + side * wide, wide), wide)]
            src, dst = ((near, near), (near, far), (far, far))[leg - 2]
            device = (y_peer, tp) if leg == 3 else (sp, core_peer)
        return remote(src, dst, do_s.at[leg], do_r.at[leg], device)

    @pl.when(outer)
    def _():
        down_copy(0).start()

    def table_copy(away):
        zz = (z + away) % 4
        same = zz // 2 == half
        slot = jnp.where(same, own, 3 - own)
        return remote(
            T.at[pl.ds(2 * own, 2)],
            T.at[pl.ds(2 * slot, 2)],
            tab_s.at[away],
            tab_r.at[slot],
            ((sp + 2 * away) % count, tp),
        )

    for away in range(1, 4):
        table_copy(away).start()

    P[0] = jnp.zeros(P.shape[1:], P.dtype)
    lane = lax.broadcasted_iota(jnp.int32, (T.shape[1], width), 0)
    for k in range(2):
        picks[k] = jnp.where(lane % count == (sp, y_peer)[k], 1.0, 0.0).astype(picks.dtype)

    for k in range(3):
        loads[k].wait()
    for k in range(4, 9):
        loads[k].start()

    kept = taps.shape[0] - 1
    run = 32

    def conv(start):
        def some(i, c):
            at = pl.multiple_of(start + i * run, run)
            near = f32(ci[pl.ds(at, halo + run)]) * f32(cx[pl.ds(at, halo + run)])
            total = taps[0:1] * near[halo - kept : halo - kept + run]
            for j in range(1, kept + 1):
                total = total + taps[j : j + 1] * near[halo - kept + j : halo - kept + j + run]
            mix[pl.ds(at, run)] = bf16(f32(co[pl.ds(at, run)]) * total)
            return c

        lax.fori_loop(0, piece // run, some, 0)

    tile = min(512, depth)
    loads[3].wait()

    def core_copy(phase, p):
        at = 2 * phase + p
        return remote(part_out.at[at], part_in.at[at], core_s.at[at], core_r.at[at], (sp, core_peer))

    def x_copy(p):
        return remote(x_out.at[p], x_in.at[p], xsw_s.at[p], xsw_r.at[p], (sp, x_peer))

    def projected(i, carry):
        phase = i // 4
        p = i // 2 % 2
        second = i % 2 == 1
        owner = jnp.where(
            phase == 0, jnp.where(second, x_peer, 3 - tp), jnp.where(second, tp, core_peer)
        )
        start = pl.multiple_of(owner * rows + (1 - p) * piece, piece)

        @pl.when(jnp.logical_and(i == 2, sp == 0))
        def _():
            ci[pl.ds(0, halo)] = jnp.zeros((halo, channels), ci.dtype)
            cx[pl.ds(0, halo)] = jnp.zeros((halo, channels), cx.dtype)

        @pl.when(jnp.logical_and(i == 2, sp > 0))
        def _():
            for k in range(2):
                halo_copy(k, (sp, core_peer)).wait_recv()

        conv(start)

        def some(n, c):
            cols = pl.ds(pl.multiple_of(n * tile, tile), tile)
            got = jnp.dot(mix[pl.ds(start, piece)], ow[:, cols], preferred_element_type=jnp.float32)

            @pl.when(second)
            def _():
                acc[p, :, cols] = got

            @pl.when(jnp.logical_not(second))
            def _():
                part_out[2 * phase + p, :, cols] = bf16(got)

            return c

        lax.fori_loop(0, depth // tile, some, 0)

        @pl.when(jnp.logical_not(second))
        def _():
            core_copy(phase, p).start()

        @pl.when(jnp.logical_and(second, phase == 0))
        def _():
            core_copy(0, p).wait_recv()

            def add(r, c):
                at = pl.ds(pl.multiple_of(r * 16, 16), 16)
                x_out[p, at] = bf16(acc[p, at] + f32(part_in[p, at]))
                return c

            lax.fori_loop(0, piece // 16, add, 0)
            x_copy(p).start()

        return carry

    lax.fori_loop(0, 8, projected, 0)
    loads[4].wait()
    loads[5].wait()

    cut = depth // 2

    def rows_copy(item, device, dst, at, k):
        cols = pl.ds(k * cut, cut)
        return remote(X.at[item, :, cols], X.at[dst, :, cols], rows_s.at[at, k], rows_r.at[dst, k], device)

    def normalize(c):
        def some(r, carry):
            at = pl.ds(pl.multiple_of(r * 16, 16), 16)
            src = pl.ds(pl.multiple_of((1 - c) * piece + r * 16, 16), 16)
            total = acc[c, at] + f32(part_in[2 + c, at]) + f32(x_in[c, at])
            mixed = jax.nn.sigmoid(f32(mg[src])) * total
            state = bf16(f32(res[src]) + rms_scale(mixed, mgain[...]))
            P[1 + c, at] = state
            X[2 * own + c, at] = bf16(rms_scale(f32(state), egain[...]))
            return carry

        lax.fori_loop(0, piece // 16, some, 0)

    def send_own(c, across):
        item = 2 * own + c
        for k in range(2):
            if across:
                rows_copy(item, (line(2), tp), 4 + c, 8 + c, k).start()
            else:
                rows_copy(item, (line(1 - own), tp), item, item, k).start()

    def relay(k, leg):
        weight_copy(k, leg).wait_recv()

    relay(0, 0)
    weight_copy(0, 1).start()
    weight_copy(0, 2).start()
    core_copy(1, 0).wait_recv()
    x_copy(0).wait_recv()
    normalize(0)
    send_own(0, False)

    @pl.when(inner)
    def _():
        send_own(0, True)

    core_copy(1, 1).wait_recv()
    x_copy(1).wait_recv()
    normalize(1)

    @pl.when(outer)
    def _():
        send_own(1, False)
        down_copy(1).start()

    relay(1, 0)
    weight_copy(1, 1).start()
    weight_copy(1, 2).start()
    for k in range(6, 9):
        loads[k].wait()
    for away in range(1, 4):
        slot = (own + away) % 4
        at = T.at[pl.ds(2 * slot, 2)]
        remote(at, at, tab_s.at[away], tab_r.at[slot], (sp, core_peer)).wait_recv()

    def hidden(item, k):
        gate, up = ((g1, u1), (g2, u2))[k]
        x = X[item]
        first = jnp.dot(x, gate[...], preferred_element_type=jnp.float32)
        second = jnp.dot(x, up[...], preferred_element_type=jnp.float32)
        share = lax.dot_general(
            T[item], picks[k], (((0,), (0,)), ((), ())), preferred_element_type=jnp.float32
        )
        H[item, :, k * width : (k + 1) * width] = bf16(jax.nn.silu(first) * second * share)

    def sum_copy(item, m):
        slot = item // 2
        c = item % 2
        to = jnp.where(outer, 1, jnp.where(slot == 0, 0, 2))
        dst = jnp.where(outer, 3 + c, jnp.where(slot == 2, 7 + c, 5 + c))
        cols = pl.ds(pl.multiple_of(m * tile, tile), tile)
        return remote(S.at[item, :, cols], P.at[dst, :, cols], sum_s.at[item, m], sum_r.at[dst, m], (line(to), tp))

    def hidden_copy(item):
        return remote(H.at[item], HR.at[item - 2], hid_s.at[item - 2], hid_r.at[item - 2], (line(1), tp))

    def out_copy(c, m):
        cols = pl.ds(pl.multiple_of(m * tile, tile), tile)
        return pltpu.make_async_copy(
            S.at[2 * own + c, :, cols],
            out_hbm.at[pl.ds(pl.multiple_of((1 - c) * piece, piece), piece), cols],
            out_sem.at[c, m],
        )

    def came(at, m):
        cols = pl.ds(pl.multiple_of(m * tile, tile), tile)
        ref = P.at[at, :, cols]
        remote(ref, ref, sum_s.at[0, m], sum_r.at[at, m], (sp, core_peer)).wait_recv()

    def step(n, carry):
        code = 0
        for i, (a, b) in enumerate(zip(OUTER_STEPS, INNER_STEPS)):
            code = jnp.where(n == i, jnp.where(outer, a, b), code)
        item = code % 8

        def has(flag):
            return code // flag % 2 == 1

        slot = item // 2
        c = item % 2

        for k in range(2):

            @pl.when(has(ARRIVE))
            def _():
                rows_copy(item, (sp, core_peer), item, item, k).wait_recv()

            @pl.when(has(FORWARD))
            def _():
                across = slot == 0
                rows_copy(
                    item,
                    (line(jnp.where(across, 2, 0)), tp),
                    jnp.where(across, 6 + c, item),
                    jnp.where(across, 10 + c, item),
                    k,
                ).start()

        @pl.when(jnp.logical_and(inner, n == LATE_ACROSS))
        def _():
            send_own(1, True)

        @pl.when(jnp.logical_and(inner, n == LATE_OUTWARD))
        def _():
            send_own(1, False)

        @pl.when(n == WEIGHTS_STEP)
        def _():
            relay(0, 2)
            weight_copy(0, 3).start()
            relay(1, 2)
            weight_copy(1, 3).start()
            relay(2, 0)
            weight_copy(2, 1).start()
            for k, leg in ((0, 1), (1, 1), (0, 3), (1, 3), (2, 1)):
                got = pl.multiple_of((core_peer if leg == 1 else 3 - tp) * quarter, quarter)
                if k < 2:
                    at = (g2, u2)[k].at[pl.ds(got, quarter)]
                else:
                    at = wd.at[pl.ds(pl.multiple_of(width + (1 - side) * wide, wide), wide)]
                remote(at, at, w_s.at[4 * k + leg], w_r.at[4 * k + leg], (sp, core_peer)).wait_recv()

            @pl.when(inner)
            def _():
                down_copy(0).wait_recv()
                down_copy(1).wait_recv()
                down_copy(2).start()
                down_copy(3).start()

        @pl.when(jnp.logical_and(inner, n == DOWN_RELAY))
        def _():
            down_copy(3).wait_recv()
            down_copy(4).start()

        @pl.when(jnp.logical_and(inner, n == DOWN_STEP))
        def _():
            down_copy(2).wait_recv()
            down_copy(4).wait_recv()

        @pl.when(has(OWN))
        def _():
            hidden(item, 0)

        @pl.when(has(OTHER))
        def _():
            hidden(item, 1)

        middle = jnp.logical_or(slot == 1, slot == 2)

        @pl.when(jnp.logical_and(has(OUT), jnp.logical_and(outer, middle)))
        def _():
            hidden_copy(item).start()

        @pl.when(jnp.logical_and(has(OUT), jnp.logical_not(jnp.logical_and(outer, middle))))
        def _():
            inner_at = jnp.where(slot == 1, 7 + c, jnp.where(slot == 2, 0, 3 + c))
            a = jnp.where(slot == 0, 5 + c, jnp.where(outer, 0, inner_at))
            d = jnp.where(slot == own, 1 + c, 0)

            @pl.when(middle)
            def _():
                ref = HR.at[item - 2]
                remote(ref, ref, hid_s.at[0], hid_r.at[item - 2], (sp, core_peer)).wait_recv()

            def some(m, carry):
                cols = pl.ds(pl.multiple_of(m * tile, tile), tile)

                @pl.when(a > 0)
                def _():
                    came(a, m)

                got = jnp.dot(H[item], wd[:, cols], preferred_element_type=jnp.float32)
                got = got + f32(P[d, :, cols]) + f32(P[a, :, cols])

                @pl.when(middle)
                def _():
                    more = jnp.dot(HR[item - 2], wdo[:, cols], preferred_element_type=jnp.float32)
                    S[item, :, cols] = bf16(got + more)

                @pl.when(jnp.logical_not(middle))
                def _():
                    S[item, :, cols] = bf16(got)

                @pl.when(slot == own)
                def _():
                    out_copy(c, m).start()

                @pl.when(slot != own)
                def _():
                    sum_copy(item, m).start()

                return carry

            lax.fori_loop(0, depth // tile, some, 0)

        return carry

    lax.fori_loop(0, len(OUTER_STEPS), step, 0)

    for c in range(2):
        for m in range(depth // tile):
            out_copy(c, m).wait()
        core_copy(0, c).wait_send()
        core_copy(1, c).wait_send()
        x_copy(c).wait_send()

    @pl.when(sp < count - 1)
    def _():
        for k in range(2):
            halo_copy(k, (sp + 1, tp)).wait_send()

    for k in range(3):
        for leg in range(4 if k < 2 else 2):
            weight_copy(k, leg).wait_send()
    for away in range(1, 4):
        table_copy(away).wait_send()

    def gone(at):
        for k in range(2):
            rows_copy(at % 8, (sp, core_peer), at % 8, at, k).wait_send()

    def summed(item):
        for m in range(depth // tile):
            sum_copy(item, m).wait_send()

    for c in range(2):
        gone(2 * own + c)

    @pl.when(outer)
    def _():
        for c in range(2):
            down_copy(c).wait_send()
            summed(6 + c)
            hidden_copy(2 + c).wait_send()
            hidden_copy(4 + c).wait_send()

    @pl.when(inner)
    def _():
        for leg in range(2, 5):
            down_copy(leg).wait_send()
        for c in range(2):
            for at in (4 + c, 6 + c, 8 + c, 10 + c):
                gone(at)
            for slot in (0, 2, 3):
                summed(2 * slot + c)


def mega(
    conv_outer, conv_inner, conv_input, conv_taps, out_weight, mix_gate, residual, mix_gain, expert_gain,
    expert_ids, group_share, pair_scores, gate_experts, up_experts, down_experts,
):
    count = lax.axis_size("sp")
    rows, depth = residual.shape
    tokens, channels = conv_inner.shape
    width = gate_experts.shape[2]
    piece = rows // 2
    halo = 16
    tiles = depth // min(512, depth)
    half_type, full = jnp.bfloat16, jnp.float32
    hbm = pl.BlockSpec(memory_space=pl.ANY)
    vmem = pl.BlockSpec(memory_space=pltpu.VMEM)
    dma = pltpu.SemaphoreType.DMA
    return pl.pallas_call(
        mega_kernel,
        out_shape=jax.ShapeDtypeStruct((rows, depth), half_type),
        in_specs=[hbm, hbm, hbm, vmem, hbm, hbm, hbm, vmem, vmem, vmem, vmem, vmem, hbm, hbm, hbm],
        out_specs=hbm,
        scratch_shapes=[
            pltpu.VMEM((halo + tokens, channels), half_type),
            pltpu.VMEM((halo + tokens, channels), half_type),
            pltpu.VMEM((tokens, channels), half_type),
            pltpu.VMEM((channels, depth), half_type),
            pltpu.VMEM((rows, depth), half_type),
            pltpu.VMEM((rows, depth), half_type),
            pltpu.VMEM((tokens, channels), half_type),
            pltpu.VMEM((2, piece, depth), full),
            pltpu.VMEM((4, piece, depth), half_type),
            pltpu.VMEM((4, piece, depth), half_type),
            pltpu.VMEM((2, piece, depth), half_type),
            pltpu.VMEM((2, piece, depth), half_type),
            pltpu.VMEM((8, piece, depth), half_type),
            pltpu.VMEM((8, 2 * count, piece), half_type),
            pltpu.VMEM((9, piece, depth), half_type),
            pltpu.VMEM((8, piece, depth), half_type),
            pltpu.VMEM((8, piece, 2 * width), half_type),
            pltpu.VMEM((4, piece, 2 * width), half_type),
            pltpu.VMEM((depth, width), half_type),
            pltpu.VMEM((depth, width), half_type),
            pltpu.VMEM((depth, width), half_type),
            pltpu.VMEM((depth, width), half_type),
            pltpu.VMEM((2 * width, depth), half_type),
            pltpu.VMEM((2 * width, depth), half_type),
            pltpu.VMEM((2, 2 * count, width), half_type),
            dma((9,)),
            dma((2,)),
            dma((2,)),
            dma((4,)),
            dma((4,)),
            dma((4,)),
            dma((4,)),
            dma((2,)),
            dma((2,)),
            dma((12,)),
            dma((12,)),
            dma((16, 2)),
            dma((8, 2)),
            dma((8, tiles)),
            dma((9, tiles)),
            dma((4,)),
            dma((4,)),
            dma((5,)),
            dma((5,)),
            dma((2, tiles)),
        ],
        compiler_params=pltpu.CompilerParams(
            collective_id=0, has_side_effects=True, vmem_limit_bytes=60 * 1024 * 1024
        ),
        name="layer",
    )(
        conv_outer, conv_inner, conv_input, conv_taps, out_weight, mix_gate, residual,
        mix_gain[None, :], expert_gain[None, :], expert_ids.T, pair_scores.T, group_share[None, :], gate_experts, up_experts, down_experts,
    )


def solution(mesh):
    placed = (
        P("sp", "tp"),
        P("sp", "tp"),
        P("sp", "tp"),
        P(None, "tp"),
        P("tp", None),
        P(("sp", "tp"), None),
        P(("sp", "tp"), None),
        P(),
        P(),
        P(("sp", "tp"), None),
        P(("sp", "tp")),
        P(("sp", "tp"), None),
        P("sp", None, None),
        P("sp", None, None),
        P("sp", None, None),
    )

    square = mesh.shape["tp"] == 4 and mesh.shape["sp"] == 8

    def layer(*arrays):
        return (mega if square else per_device)(*arrays)

    return jax.shard_map(
        layer, mesh=mesh, in_specs=placed, out_specs=P(("sp", "tp"), None), check_vma=False
    )
```

```python
import jax
import jax.numpy as jnp
from jax import lax
from jax.experimental import pallas as pl
from jax.experimental.pallas import tpu as pltpu
from jax.sharding import PartitionSpec as P

epsilon = 1e-06


def f32(value):
    return value.astype(jnp.float32)


def bf16(value):
    return value.astype(jnp.bfloat16)


def rms_scale(values, gain):
    return values * lax.rsqrt(jnp.mean(values * values, axis=-1, keepdims=True) + epsilon) * gain


def shifted(value, steps, senders):
    return lax.ppermute(value, "sp", [(s, s + steps) for s in senders])


def swapped(value, axis, bit):
    return lax.ppermute(value, axis, [(s, s ^ bit) for s in range(lax.axis_size(axis))])


def mixer_rows(conv_outer, conv_inner, conv_input, conv_taps):
    kept = conv_taps.shape[0] - 1
    inner = f32(conv_inner) * f32(conv_input)
    tail = f32(conv_inner[-kept:]) * f32(conv_input[-kept:])
    earlier = shifted(tail, 1, range(lax.axis_size("sp") - 1))
    length = conv_inner.shape[0]
    inner = jnp.concatenate([earlier, inner], 0)
    conv = conv_taps[0] * inner[0:length]
    for offset in range(1, kept + 1):
        conv = conv + conv_taps[offset] * inner[offset : offset + length]
    return bf16(f32(conv_outer) * conv)


def project(mixed_rows, out_weight, own_rows):
    parts = lax.axis_size("tp")
    me = lax.axis_index("tp")
    blocks = mixed_rows.reshape(parts, own_rows, -1)

    def partial(owner):
        rows = lax.dynamic_index_in_dim(blocks, owner, 0, keepdims=False)
        return jnp.dot(rows, out_weight, preferred_element_type=jnp.float32)

    def total(owner_bits, bit):
        if bit == 1:
            return partial(me ^ owner_bits)
        half = bit // 2
        sent = bf16(total(owner_bits | half, half))
        given = swapped(sent, "tp", half)
        return total(owner_bits, half) + f32(given)

    return total(0, parts)


def routing_table(expert_ids, group_share, pair_scores, own_rows, count):
    weights = group_share[:, None] * jax.nn.softmax(pair_scores, axis=-1)
    lanes = -(-2 * count // 128) * 128
    column = jnp.arange(lanes, dtype=jnp.int32)[None, :]
    coarse = lax.reduce_precision(weights, 8, 7)
    fine = weights - coarse
    table = jnp.zeros((own_rows, lanes), jnp.float32)
    for slot in range(expert_ids.shape[1]):
        at = expert_ids[:, slot : slot + 1]
        table = table + jnp.where(column == at, coarse[:, slot : slot + 1], 0.0)
        table = table + jnp.where(column == at + count, fine[:, slot : slot + 1], 0.0)
    return bf16(table)


def per_device(
    conv_outer,
    conv_inner,
    conv_input,
    conv_taps,
    out_weight,
    mix_gate,
    residual,
    mix_gain,
    expert_gain,
    expert_ids,
    group_share,
    pair_scores,
    gate_experts,
    up_experts,
    down_experts,
):
    count = lax.axis_size("sp")
    me = lax.axis_index("sp")
    own_rows = residual.shape[0]
    groups = count // 2
    place = me // 2
    side = lax.axis_index("tp") % 2
    half = gate_experts.shape[2] // 2

    def fetched(weight, axis):
        piece = lax.dynamic_slice_in_dim(weight[0], side * half, half, axis)
        first = swapped(piece, "sp", 1)
        second = swapped(first, "tp", 1)
        return jnp.concatenate([weight[0], first, second], axis)

    gate_both = fetched(gate_experts, 1)
    up_both = fetched(up_experts, 1)
    down_both = fetched(down_experts, 0)

    lanes = -(-2 * count // 128) * 128
    table = routing_table(expert_ids, group_share, pair_scores, own_rows, count)

    def spread(own):
        below, above = {0: own}, {0: own}
        for step in range(1, groups):
            below[step] = shifted(below[step - 1], 2, range(2 * (step - 1), count - 2))
            above[step] = shifted(above[step - 1], -2, range(2, count - 2 * (step - 1)))
        order = {0: own}
        for near in range(1, (groups - 1) // 2 + 1):
            far = groups - near
            early = jnp.where(place < near, above[near], below[near])
            _, over, under, away = lax.optimization_barrier(
                (early, above[near], below[far], above[far])
            )
            order[near] = early
            late = jnp.where(place < far, over, under)
            order[far] = jnp.where(place < near, away, late)
        if groups % 2 == 0:
            mid = groups // 2
            order[mid] = jnp.where(place < mid, above[mid], below[mid])
        return order

    mixed_rows = mixer_rows(conv_outer, conv_inner, conv_input, conv_taps)
    projected = project(mixed_rows, out_weight, own_rows)
    mixed = jax.nn.sigmoid(f32(mix_gate)) * projected
    hidden_state = bf16(f32(residual) + rms_scale(mixed, mix_gain))
    normed = bf16(rms_scale(f32(hidden_state), expert_gain))

    blocks = spread(jnp.concatenate([normed, table], 1))
    depth = normed.shape[1]

    def served(block):
        rows = block[:, :depth]
        chosen = jnp.arange(lanes, dtype=jnp.int32)[:, None] % count
        picks = bf16(chosen == jnp.stack([me, me ^ 1])[None, :])
        picks = jnp.where(jnp.arange(lanes)[:, None] < 2 * count, picks, 0)
        shares = jnp.dot(block[:, depth:], picks, preferred_element_type=jnp.float32)
        wide = 2 * half
        first = jnp.dot(rows, gate_both, preferred_element_type=jnp.float32)
        second = jnp.dot(rows, up_both, preferred_element_type=jnp.float32)
        mine = jnp.arange(2 * wide)[None, :] < wide
        share = jnp.where(mine, shares[:, :1], shares[:, 1:])
        hidden = lax.optimization_barrier(bf16(jax.nn.silu(first) * second * share))
        return lax.optimization_barrier(
            jnp.dot(hidden, down_both, preferred_element_type=jnp.float32)
        )

    results = {number: served(block) for number, block in blocks.items()}

    def for_upper(step):
        gone = groups - step
        if step == gone or step < gone:
            return results[gone]
        return jnp.where(place < gone, results[gone], results[step])

    down = up = None
    for step in range(1, groups):
        gone = groups - step
        lower, upper = results[gone], for_upper(step)
        if down is not None:
            lower, upper = lower + f32(down), upper + f32(up)
        down = shifted(bf16(lower), -2, range(2 * gone, count))
        up = shifted(bf16(upper), 2, range(0, count - 2 * gone))
    result = f32(hidden_state) + results[0]
    if down is not None:
        result = result + f32(down) + f32(up)
    return bf16(result)


MESH_ID = pl.DeviceIdType.MESH
OWN, OTHER, OUT, ARRIVE, FORWARD, SEND_ACROSS, SEND_OUTWARD = (8 << i for i in range(7))
HIDDEN_READY, DOWN_READY, FAR_PASS, FAR_READY = (1024 << i for i in range(4))
GATE_PASS, UP_PASS, DOWN_PASS = (16384 << i for i in range(3))

OUTER_STEPS = (
    1 | OWN,
    0 | OWN,
    GATE_PASS,
    6 | OWN | ARRIVE,
    2 | OWN | ARRIVE,
    UP_PASS,
    DOWN_PASS,
    HIDDEN_READY,
    6 | OTHER,
    DOWN_READY,
    6 | OUT,
    4 | OWN | ARRIVE,
    4 | OTHER,
    7 | OWN | ARRIVE,
    2 | OTHER,
    7 | OTHER,
    7 | OUT,
    4 | OUT,
    5 | OWN | ARRIVE,
    5 | OTHER,
    5 | OUT,
    3 | OWN | ARRIVE,
    0 | OTHER,
    2 | OUT,
    1 | OTHER,
    3 | OTHER,
    0 | OUT,
    3 | OUT,
    1 | OUT,
    0,
    0,
    0,
    0,
)
INNER_STEPS = (
    4 | OWN | ARRIVE | FORWARD,
    0 | OWN | ARRIVE | FORWARD,
    1 | OWN | ARRIVE | FORWARD,
    6 | OWN | ARRIVE | FORWARD,
    SEND_ACROSS,
    2 | OWN,
    FAR_PASS,
    7 | OWN | ARRIVE | FORWARD,
    GATE_PASS,
    UP_PASS,
    SEND_OUTWARD,
    DOWN_PASS,
    HIDDEN_READY,
    0 | OTHER,
    DOWN_READY,
    2 | OTHER,
    6 | OTHER,
    1 | OTHER,
    6 | OUT,
    5 | OWN | ARRIVE | FORWARD,
    5 | OTHER,
    7 | OTHER,
    7 | OUT,
    0 | OUT,
    4 | OTHER,
    FAR_READY,
    4 | OUT,
    1 | OUT,
    5 | OUT,
    3 | OWN,
    2 | OUT,
    3 | OTHER,
    3 | OUT,
)


def mega_kernel(
    co_hbm, ci_hbm, cx_hbm, taps, ow_hbm, mg_hbm, res_hbm, mgain, egain, ids, scores, group,
    g_hbm, u_hbm, d_hbm, out_hbm,
    ci, cx, co, ow, mg, res, mix, acc, part_out, part_in, x_out, x_in,
    X, T, P, S, H, HR, g1, u1, g2, u2, wd, wdo, picks,
    load_sem, halo_s, halo_r, tab_s, tab_r, core_s, core_r, xsw_s, xsw_r,
    w_s, w_r, rows_s, rows_r, sum_s, sum_r, hid_s, hid_r, do_s, do_r, out_sem,
):
    sp = lax.axis_index("sp")
    tp = lax.axis_index("tp")
    z = sp // 2
    y = sp % 2
    half = z // 2
    outer = z * (3 - z) == 0
    inner = jnp.logical_not(outer)
    own = jnp.where(outer, 0, 1)
    core_peer = tp + 1 - 2 * (tp % 2)
    x_peer = (tp + 2) % 4
    y_peer = sp + 1 - 2 * y
    rows, depth = res.shape
    piece = rows // 2
    width = g1.shape[1]
    count = T.shape[1] // 2
    channels = ow.shape[0]
    halo = ci.shape[0] - co.shape[0]

    def line(slot):
        where = jnp.where(slot == 0, 3 * half, jnp.where(slot == 1, 1 + half, jnp.where(slot == 2, 2 - half, 3 - 3 * half)))
        return 2 * where + y

    def remote(src, dst, s, r, device):
        return pltpu.make_async_remote_copy(
            src_ref=src, dst_ref=dst, send_sem=s, recv_sem=r, device_id=device, device_id_type=MESH_ID
        )

    barrier = pltpu.get_barrier_semaphore()

    def greet(device):
        pl.semaphore_signal(barrier, inc=1, device_id=device, device_id_type=MESH_ID)

    greet((sp, core_peer))
    greet((sp, x_peer))
    greet((y_peer, tp))
    greet((line(1 - own), tp))

    @pl.when(inner)
    def _():
        greet((line(2), tp))

    has_next = jnp.logical_and(y == 1, sp < count - 1)
    has_last = jnp.logical_and(y == 0, sp > 0)

    @pl.when(has_next)
    def _():
        greet((sp + 1, tp))

    @pl.when(has_last)
    def _():
        greet((sp - 1, tp))

    tokens = co.shape[0]
    loads = [
        pltpu.make_async_copy(ci_hbm, ci.at[pl.ds(halo, tokens)], load_sem.at[0]),
        pltpu.make_async_copy(cx_hbm, cx.at[pl.ds(halo, tokens)], load_sem.at[1]),
        pltpu.make_async_copy(co_hbm, co, load_sem.at[2]),
        pltpu.make_async_copy(ow_hbm, ow, load_sem.at[3]),
        pltpu.make_async_copy(mg_hbm, mg, load_sem.at[4]),
        pltpu.make_async_copy(res_hbm, res, load_sem.at[5]),
        pltpu.make_async_copy(g_hbm.at[0], g1, load_sem.at[6]),
        pltpu.make_async_copy(u_hbm.at[0], u1, load_sem.at[7]),
        pltpu.make_async_copy(d_hbm.at[0], wd.at[pl.ds(0, width)], load_sem.at[8]),
    ]
    for k in (0, 1, 3, 2):
        loads[k].start()

    raw = scores[...]
    top = jnp.maximum(raw[0:1], raw[1:2])
    up = jnp.exp(raw - top)
    weights = group[...] * (up / (up[0:1] + up[1:2]))
    coarse = f32(bf16(weights))
    fine = weights - coarse
    line_of = lax.broadcasted_iota(jnp.int32, (T.shape[1], rows), 0)
    entries = jnp.zeros((T.shape[1], rows), jnp.float32)
    for k in range(2):
        entries = entries + jnp.where(line_of == ids[k : k + 1], coarse[k : k + 1], 0.0)
        entries = entries + jnp.where(line_of == ids[k : k + 1] + count, fine[k : k + 1], 0.0)
    entries = bf16(entries)
    for p in range(2):
        T[2 * own + p] = entries[:, (1 - p) * piece : (2 - p) * piece]

    pl.semaphore_wait(barrier, 4 + jnp.where(inner, 1, 0) + jnp.where(has_next, 1, 0) + jnp.where(has_last, 1, 0))

    def halo_copy(k, device):
        src = (ci_hbm, cx_hbm)[k].at[pl.ds(tokens - halo, halo)]
        return remote(src, (ci, cx)[k].at[pl.ds(0, halo)], halo_s.at[k], halo_r.at[k], device)

    @pl.when(sp < count - 1)
    def _():
        for k in range(2):
            halo_copy(k, (sp + 1, tp)).start()

    quarter = depth // 4
    wide = width // 2
    mine = pl.multiple_of(tp * quarter, quarter)
    theirs = pl.multiple_of(x_peer * quarter, quarter)
    side = tp % 2

    def weight_copy(k, leg):
        at = 4 * k + leg
        if k < 2:
            buf = (g2, u2)[k]
            rows_at = pl.ds(theirs if leg == 3 else mine, quarter)
            src = (g_hbm, u_hbm)[k].at[0, rows_at] if leg == 0 else buf.at[rows_at]
            dst = buf.at[rows_at]
        else:
            rows_at = pl.ds(pl.multiple_of(width + side * wide, wide), wide)
            src = d_hbm.at[0, pl.ds(pl.multiple_of(side * wide, wide), wide)] if leg == 0 else wd.at[rows_at]
            dst = wd.at[rows_at]
        device = ((y_peer, tp), (sp, core_peer), (sp, x_peer), (sp, core_peer))[leg]
        return remote(src, dst, w_s.at[at], w_r.at[at], device)

    for k in range(3):
        weight_copy(k, 0).start()

    part = wide // 2

    def down_copy(leg):
        if leg < 2:
            src = d_hbm.at[0, pl.ds(pl.multiple_of(side * wide + leg * part, part), part)]
            dst = wdo.at[pl.ds(pl.multiple_of(side * wide + leg * part, part), part)]
            device = (line(1), tp)
        else:
            near = wdo.at[pl.ds(pl.multiple_of(side * wide, wide), wide)]
            far = wdo.at[pl.ds(pl.multiple_of(width + side * wide, wide), wide)]
            src, dst = ((near, near), (near, far), (far, far))[leg - 2]
            device = (y_peer, tp) if leg == 3 else (sp, core_peer)
        return remote(src, dst, do_s.at[leg], do_r.at[leg], device)

    @pl.when(outer)
    def _():
        down_copy(0).start()

    def table_copy(slot, across):
        dst = 3 - slot if across else slot
        at = slot + (4 if across else 0)
        return remote(
            T.at[pl.ds(2 * slot, 2)],
            T.at[pl.ds(2 * dst, 2)],
            tab_s.at[at],
            tab_r.at[dst],
            (line(2) if across else line(1 - own), tp),
        )

    def table_came(slot):
        at = T.at[pl.ds(2 * slot, 2)]
        remote(at, at, tab_s.at[0], tab_r.at[slot], (sp, core_peer)).wait_recv()

    table_copy(own, False).start()

    @pl.when(inner)
    def _():
        table_copy(1, True).start()

    P[0] = jnp.zeros(P.shape[1:], P.dtype)
    lane = lax.broadcasted_iota(jnp.int32, (T.shape[1], width), 0)
    for k in range(2):
        picks[k] = jnp.where(lane % count == (sp, y_peer)[k], 1.0, 0.0).astype(picks.dtype)

    for k in range(3):
        loads[k].wait()
    for k in range(4, 9):
        loads[k].start()

    kept = taps.shape[0] - 1
    run = 32

    def conv(start):
        def some(i, c):
            at = pl.multiple_of(start + i * run, run)
            near = f32(ci[pl.ds(at, halo + run)]) * f32(cx[pl.ds(at, halo + run)])
            total = taps[0:1] * near[halo - kept : halo - kept + run]
            for j in range(1, kept + 1):
                total = total + taps[j : j + 1] * near[halo - kept + j : halo - kept + j + run]
            mix[pl.ds(at, run)] = bf16(f32(co[pl.ds(at, run)]) * total)
            return c

        lax.fori_loop(0, piece // run, some, 0)

    tile = min(512, depth)
    loads[3].wait()

    def core_copy(phase, p):
        at = 2 * phase + p
        return remote(part_out.at[at], part_in.at[at], core_s.at[at], core_r.at[at], (sp, core_peer))

    some_rows = piece // 2

    def x_copy(p, k):
        at = pl.ds(k * some_rows, some_rows)
        return remote(
            x_out.at[p, at], x_in.at[p, at], xsw_s.at[2 * p + k], xsw_r.at[2 * p + k], (sp, x_peer)
        )

    def projected(i, carry):
        phase = i // 4
        p = i // 2 % 2
        second = i % 2 == 1
        owner = jnp.where(
            phase == 0, jnp.where(second, x_peer, 3 - tp), jnp.where(second, tp, core_peer)
        )
        start = pl.multiple_of(owner * rows + (1 - p) * piece, piece)

        @pl.when(jnp.logical_and(i == 2, sp == 0))
        def _():
            ci[pl.ds(0, halo)] = jnp.zeros((halo, channels), ci.dtype)
            cx[pl.ds(0, halo)] = jnp.zeros((halo, channels), cx.dtype)

        @pl.when(jnp.logical_and(i == 2, sp > 0))
        def _():
            for k in range(2):
                halo_copy(k, (sp, core_peer)).wait_recv()

        conv(start)

        def some(n, c):
            cols = pl.ds(pl.multiple_of(n * tile, tile), tile)
            got = jnp.dot(mix[pl.ds(start, piece)], ow[:, cols], preferred_element_type=jnp.float32)

            @pl.when(second)
            def _():
                acc[p, :, cols] = got

            @pl.when(jnp.logical_not(second))
            def _():
                part_out[2 * phase + p, :, cols] = bf16(got)

            return c

        lax.fori_loop(0, depth // tile, some, 0)

        @pl.when(jnp.logical_not(second))
        def _():
            core_copy(phase, p).start()

        @pl.when(jnp.logical_and(second, phase == 0))
        def _():
            core_copy(0, p).wait_recv()

            def add(r, c):
                at = pl.ds(pl.multiple_of(r * 16, 16), 16)
                x_out[p, at] = bf16(acc[p, at] + f32(part_in[p, at]))
                return c

            steps = some_rows // 16
            for k in range(2):
                lax.fori_loop(k * steps, (k + 1) * steps, add, 0)
                x_copy(p, k).start()

        return carry

    lax.fori_loop(0, 8, projected, 0)
    loads[4].wait()
    loads[5].wait()

    def rows_copy(item, device, dst, at, k):
        some = pl.ds(k * some_rows, some_rows)
        return remote(X.at[item, some], X.at[dst, some], rows_s.at[at, k], rows_r.at[dst, k], device)

    def normalize(c, k):
        def some(r, carry):
            at = pl.ds(pl.multiple_of(r * 16, 16), 16)
            src = pl.ds(pl.multiple_of((1 - c) * piece + r * 16, 16), 16)
            total = acc[c, at] + f32(part_in[2 + c, at]) + f32(x_in[c, at])
            mixed = jax.nn.sigmoid(f32(mg[src])) * total
            state = bf16(f32(res[src]) + rms_scale(mixed, mgain[...]))
            P[1 + c, at] = state
            X[2 * own + c, at] = bf16(rms_scale(f32(state), egain[...]))
            return carry

        steps = some_rows // 16
        lax.fori_loop(k * steps, (k + 1) * steps, some, 0)

    def send_own(c, k, across):
        item = 2 * own + c
        if across:
            rows_copy(item, (line(2), tp), 4 + c, 8 + c, k).start()
        else:
            rows_copy(item, (line(1 - own), tp), item, item, k).start()

    def relay(k, leg):
        weight_copy(k, leg).wait_recv()

    @pl.when(inner)
    def _():
        table_came(0)
        table_copy(0, True).start()
        table_came(2)
        table_copy(2, False).start()

    core_copy(1, 0).wait_recv()
    for k in range(2):
        x_copy(0, k).wait_recv()
        normalize(0, k)
        send_own(0, k, False)

        @pl.when(inner)
        def _():
            send_own(0, k, True)

    @pl.when(inner)
    def _():
        table_came(3)
        table_copy(3, False).start()

    relay(0, 0)
    weight_copy(0, 1).start()
    weight_copy(0, 2).start()
    core_copy(1, 1).wait_recv()
    for k in range(2):
        x_copy(1, k).wait_recv()
        normalize(1, k)

        @pl.when(outer)
        def _():
            send_own(1, k, False)

    @pl.when(outer)
    def _():
        down_copy(1).start()

    relay(1, 0)
    weight_copy(1, 1).start()
    weight_copy(1, 2).start()
    for k in range(6, 9):
        loads[k].wait()

    @pl.when(outer)
    def _():
        for slot in range(1, 4):
            table_came(slot)

    def hidden(item, k):
        gate, up = ((g1, u1), (g2, u2))[k]
        x = X[item]
        first = jnp.dot(x, gate[...], preferred_element_type=jnp.float32)
        second = jnp.dot(x, up[...], preferred_element_type=jnp.float32)
        share = lax.dot_general(
            T[item], picks[k], (((0,), (0,)), ((), ())), preferred_element_type=jnp.float32
        )
        H[item, :, k * width : (k + 1) * width] = bf16(jax.nn.silu(first) * second * share)

    def sum_copy(item, m):
        slot = item // 2
        c = item % 2
        to = jnp.where(outer, 1, jnp.where(slot == 0, 0, 2))
        dst = jnp.where(outer, 3 + c, jnp.where(slot == 2, 7 + c, 5 + c))
        cols = pl.ds(pl.multiple_of(m * tile, tile), tile)
        return remote(S.at[item, :, cols], P.at[dst, :, cols], sum_s.at[item, m], sum_r.at[dst, m], (line(to), tp))

    def hidden_copy(item):
        return remote(H.at[item], HR.at[item - 2], hid_s.at[item - 2], hid_r.at[item - 2], (line(1), tp))

    def out_copy(c, m):
        cols = pl.ds(pl.multiple_of(m * tile, tile), tile)
        return pltpu.make_async_copy(
            S.at[2 * own + c, :, cols],
            out_hbm.at[pl.ds(pl.multiple_of((1 - c) * piece, piece), piece), cols],
            out_sem.at[c, m],
        )

    def came(at, m):
        cols = pl.ds(pl.multiple_of(m * tile, tile), tile)
        ref = P.at[at, :, cols]
        remote(ref, ref, sum_s.at[0, m], sum_r.at[at, m], (sp, core_peer)).wait_recv()

    def step(n, carry):
        code = 0
        for i, (a, b) in enumerate(zip(OUTER_STEPS, INNER_STEPS)):
            code = jnp.where(n == i, jnp.where(outer, a, b), code)
        item = code % 8

        def has(flag):
            return code // flag % 2 == 1

        slot = item // 2
        c = item % 2

        for k in range(2):

            @pl.when(has(ARRIVE))
            def _():
                rows_copy(item, (sp, core_peer), item, item, k).wait_recv()

            @pl.when(has(FORWARD))
            def _():
                across = slot == 0
                rows_copy(
                    item,
                    (line(jnp.where(across, 2, 0)), tp),
                    jnp.where(across, 6 + c, item),
                    jnp.where(across, 10 + c, item),
                    k,
                ).start()

        @pl.when(has(SEND_ACROSS))
        def _():
            for k in range(2):
                send_own(1, k, True)

        @pl.when(has(SEND_OUTWARD))
        def _():
            for k in range(2):
                send_own(1, k, False)

        @pl.when(has(GATE_PASS))
        def _():
            relay(0, 2)
            weight_copy(0, 3).start()

        @pl.when(has(UP_PASS))
        def _():
            relay(1, 2)
            weight_copy(1, 3).start()

        @pl.when(has(DOWN_PASS))
        def _():
            relay(2, 0)
            weight_copy(2, 1).start()

        def weight_came(k, leg):
            got = pl.multiple_of((core_peer if leg == 1 else 3 - tp) * quarter, quarter)
            if k < 2:
                at = (g2, u2)[k].at[pl.ds(got, quarter)]
            else:
                at = wd.at[pl.ds(pl.multiple_of(width + (1 - side) * wide, wide), wide)]
            remote(at, at, w_s.at[4 * k + leg], w_r.at[4 * k + leg], (sp, core_peer)).wait_recv()

        @pl.when(has(HIDDEN_READY))
        def _():
            for k in range(2):
                weight_came(k, 1)
                weight_came(k, 3)

        @pl.when(has(DOWN_READY))
        def _():
            weight_came(2, 1)

        @pl.when(has(FAR_PASS))
        def _():
            down_copy(0).wait_recv()
            down_copy(1).wait_recv()
            down_copy(2).start()
            down_copy(3).start()

        @pl.when(has(FAR_READY))
        def _():
            down_copy(3).wait_recv()
            down_copy(4).start()
            down_copy(2).wait_recv()
            down_copy(4).wait_recv()

        @pl.when(has(OWN))
        def _():
            hidden(item, 0)

        @pl.when(has(OTHER))
        def _():
            hidden(item, 1)

        middle = jnp.logical_or(slot == 1, slot == 2)

        @pl.when(jnp.logical_and(has(OUT), jnp.logical_and(outer, middle)))
        def _():
            hidden_copy(item).start()

        @pl.when(jnp.logical_and(has(OUT), jnp.logical_not(jnp.logical_and(outer, middle))))
        def _():
            inner_at = jnp.where(slot == 1, 7 + c, jnp.where(slot == 2, 0, 3 + c))
            a = jnp.where(slot == 0, 5 + c, jnp.where(outer, 0, inner_at))
            d = jnp.where(slot == own, 1 + c, 0)

            @pl.when(middle)
            def _():
                ref = HR.at[item - 2]
                remote(ref, ref, hid_s.at[0], hid_r.at[item - 2], (sp, core_peer)).wait_recv()

            def some(m, carry):
                cols = pl.ds(pl.multiple_of(m * tile, tile), tile)

                @pl.when(a > 0)
                def _():
                    came(a, m)

                got = jnp.dot(H[item], wd[:, cols], preferred_element_type=jnp.float32)
                got = got + f32(P[d, :, cols]) + f32(P[a, :, cols])

                @pl.when(middle)
                def _():
                    more = jnp.dot(HR[item - 2], wdo[:, cols], preferred_element_type=jnp.float32)
                    S[item, :, cols] = bf16(got + more)

                @pl.when(jnp.logical_not(middle))
                def _():
                    S[item, :, cols] = bf16(got)

                @pl.when(slot == own)
                def _():
                    out_copy(c, m).start()

                @pl.when(slot != own)
                def _():
                    sum_copy(item, m).start()

                return carry

            lax.fori_loop(0, depth // tile, some, 0)

        return carry

    lax.fori_loop(0, len(OUTER_STEPS), step, 0)

    for c in range(2):
        for m in range(depth // tile):
            out_copy(c, m).wait()
        core_copy(0, c).wait_send()
        core_copy(1, c).wait_send()
        x_copy(c, 0).wait_send()
        x_copy(c, 1).wait_send()

    @pl.when(sp < count - 1)
    def _():
        for k in range(2):
            halo_copy(k, (sp + 1, tp)).wait_send()

    for k in range(3):
        for leg in range(4 if k < 2 else 2):
            weight_copy(k, leg).wait_send()
    table_copy(own, False).wait_send()

    @pl.when(inner)
    def _():
        table_copy(1, True).wait_send()
        table_copy(0, True).wait_send()
        table_copy(2, False).wait_send()
        table_copy(3, False).wait_send()


    def gone(at):
        for k in range(2):
            rows_copy(at % 8, (sp, core_peer), at % 8, at, k).wait_send()

    def summed(item):
        for m in range(depth // tile):
            sum_copy(item, m).wait_send()

    for c in range(2):
        gone(2 * own + c)

    @pl.when(outer)
    def _():
        for c in range(2):
            down_copy(c).wait_send()
            summed(6 + c)
            hidden_copy(2 + c).wait_send()
            hidden_copy(4 + c).wait_send()

    @pl.when(inner)
    def _():
        for leg in range(2, 5):
            down_copy(leg).wait_send()
        for c in range(2):
            for at in (4 + c, 6 + c, 8 + c, 10 + c):
                gone(at)
            for slot in (0, 2, 3):
                summed(2 * slot + c)


def mega(
    conv_outer, conv_inner, conv_input, conv_taps, out_weight, mix_gate, residual, mix_gain, expert_gain,
    expert_ids, group_share, pair_scores, gate_experts, up_experts, down_experts,
):
    count = lax.axis_size("sp")
    rows, depth = residual.shape
    tokens, channels = conv_inner.shape
    width = gate_experts.shape[2]
    piece = rows // 2
    halo = 16
    tiles = depth // min(512, depth)
    half_type, full = jnp.bfloat16, jnp.float32
    hbm = pl.BlockSpec(memory_space=pl.ANY)
    vmem = pl.BlockSpec(memory_space=pltpu.VMEM)
    dma = pltpu.SemaphoreType.DMA
    return pl.pallas_call(
        mega_kernel,
        out_shape=jax.ShapeDtypeStruct((rows, depth), half_type),
        in_specs=[hbm, hbm, hbm, vmem, hbm, hbm, hbm, vmem, vmem, vmem, vmem, vmem, hbm, hbm, hbm],
        out_specs=hbm,
        scratch_shapes=[
            pltpu.VMEM((halo + tokens, channels), half_type),
            pltpu.VMEM((halo + tokens, channels), half_type),
            pltpu.VMEM((tokens, channels), half_type),
            pltpu.VMEM((channels, depth), half_type),
            pltpu.VMEM((rows, depth), half_type),
            pltpu.VMEM((rows, depth), half_type),
            pltpu.VMEM((tokens, channels), half_type),
            pltpu.VMEM((2, piece, depth), full),
            pltpu.VMEM((4, piece, depth), half_type),
            pltpu.VMEM((4, piece, depth), half_type),
            pltpu.VMEM((2, piece, depth), half_type),
            pltpu.VMEM((2, piece, depth), half_type),
            pltpu.VMEM((8, piece, depth), half_type),
            pltpu.VMEM((8, 2 * count, piece), half_type),
            pltpu.VMEM((9, piece, depth), half_type),
            pltpu.VMEM((8, piece, depth), half_type),
            pltpu.VMEM((8, piece, 2 * width), half_type),
            pltpu.VMEM((4, piece, 2 * width), half_type),
            pltpu.VMEM((depth, width), half_type),
            pltpu.VMEM((depth, width), half_type),
            pltpu.VMEM((depth, width), half_type),
            pltpu.VMEM((depth, width), half_type),
            pltpu.VMEM((2 * width, depth), half_type),
            pltpu.VMEM((2 * width, depth), half_type),
            pltpu.VMEM((2, 2 * count, width), half_type),
            dma((9,)),
            dma((2,)),
            dma((2,)),
            dma((8,)),
            dma((4,)),
            dma((4,)),
            dma((4,)),
            dma((4,)),
            dma((4,)),
            dma((12,)),
            dma((12,)),
            dma((16, 2)),
            dma((8, 2)),
            dma((8, tiles)),
            dma((9, tiles)),
            dma((4,)),
            dma((4,)),
            dma((5,)),
            dma((5,)),
            dma((2, tiles)),
        ],
        compiler_params=pltpu.CompilerParams(
            collective_id=0, has_side_effects=True, vmem_limit_bytes=60 * 1024 * 1024
        ),
        name="layer",
    )(
        conv_outer, conv_inner, conv_input, conv_taps, out_weight, mix_gate, residual,
        mix_gain[None, :], expert_gain[None, :], expert_ids.T, pair_scores.T, group_share[None, :], gate_experts, up_experts, down_experts,
    )


def solution(mesh):
    placed = (
        P("sp", "tp"),
        P("sp", "tp"),
        P("sp", "tp"),
        P(None, "tp"),
        P("tp", None),
        P(("sp", "tp"), None),
        P(("sp", "tp"), None),
        P(),
        P(),
        P(("sp", "tp"), None),
        P(("sp", "tp")),
        P(("sp", "tp"), None),
        P("sp", None, None),
        P("sp", None, None),
        P("sp", None, None),
    )

    square = mesh.shape["tp"] == 4 and mesh.shape["sp"] == 8

    def layer(*arrays):
        return (mega if square else per_device)(*arrays)

    return jax.shard_map(
        layer, mesh=mesh, in_specs=placed, out_specs=P(("sp", "tp"), None), check_vma=False
    )
```

```python
import jax
import jax.numpy as jnp
from jax import lax
from jax.experimental import pallas as pl
from jax.experimental.pallas import tpu as pltpu
from jax.sharding import PartitionSpec as P

epsilon = 1e-06


def f32(value):
    return value.astype(jnp.float32)


def bf16(value):
    return value.astype(jnp.bfloat16)


def rms_scale(values, gain):
    return values * lax.rsqrt(jnp.mean(values * values, axis=-1, keepdims=True) + epsilon) * gain


def shifted(value, steps, senders):
    return lax.ppermute(value, "sp", [(s, s + steps) for s in senders])


def swapped(value, axis, bit):
    return lax.ppermute(value, axis, [(s, s ^ bit) for s in range(lax.axis_size(axis))])


def mixer_rows(conv_outer, conv_inner, conv_input, conv_taps):
    kept = conv_taps.shape[0] - 1
    inner = f32(conv_inner) * f32(conv_input)
    tail = f32(conv_inner[-kept:]) * f32(conv_input[-kept:])
    earlier = shifted(tail, 1, range(lax.axis_size("sp") - 1))
    length = conv_inner.shape[0]
    inner = jnp.concatenate([earlier, inner], 0)
    conv = conv_taps[0] * inner[0:length]
    for offset in range(1, kept + 1):
        conv = conv + conv_taps[offset] * inner[offset : offset + length]
    return bf16(f32(conv_outer) * conv)


def project(mixed_rows, out_weight, own_rows):
    parts = lax.axis_size("tp")
    me = lax.axis_index("tp")
    blocks = mixed_rows.reshape(parts, own_rows, -1)

    def partial(owner):
        rows = lax.dynamic_index_in_dim(blocks, owner, 0, keepdims=False)
        return jnp.dot(rows, out_weight, preferred_element_type=jnp.float32)

    def total(owner_bits, bit):
        if bit == 1:
            return partial(me ^ owner_bits)
        half = bit // 2
        sent = bf16(total(owner_bits | half, half))
        given = swapped(sent, "tp", half)
        return total(owner_bits, half) + f32(given)

    return total(0, parts)


def routing_table(expert_ids, group_share, pair_scores, own_rows, count):
    weights = group_share[:, None] * jax.nn.softmax(pair_scores, axis=-1)
    lanes = -(-2 * count // 128) * 128
    column = jnp.arange(lanes, dtype=jnp.int32)[None, :]
    coarse = lax.reduce_precision(weights, 8, 7)
    fine = weights - coarse
    table = jnp.zeros((own_rows, lanes), jnp.float32)
    for slot in range(expert_ids.shape[1]):
        at = expert_ids[:, slot : slot + 1]
        table = table + jnp.where(column == at, coarse[:, slot : slot + 1], 0.0)
        table = table + jnp.where(column == at + count, fine[:, slot : slot + 1], 0.0)
    return bf16(table)


def per_device(
    conv_outer,
    conv_inner,
    conv_input,
    conv_taps,
    out_weight,
    mix_gate,
    residual,
    mix_gain,
    expert_gain,
    expert_ids,
    group_share,
    pair_scores,
    gate_experts,
    up_experts,
    down_experts,
):
    count = lax.axis_size("sp")
    me = lax.axis_index("sp")
    own_rows = residual.shape[0]
    groups = count // 2
    place = me // 2
    side = lax.axis_index("tp") % 2
    half = gate_experts.shape[2] // 2

    def fetched(weight, axis):
        piece = lax.dynamic_slice_in_dim(weight[0], side * half, half, axis)
        first = swapped(piece, "sp", 1)
        second = swapped(first, "tp", 1)
        return jnp.concatenate([weight[0], first, second], axis)

    gate_both = fetched(gate_experts, 1)
    up_both = fetched(up_experts, 1)
    down_both = fetched(down_experts, 0)

    lanes = -(-2 * count // 128) * 128
    table = routing_table(expert_ids, group_share, pair_scores, own_rows, count)

    def spread(own):
        below, above = {0: own}, {0: own}
        for step in range(1, groups):
            below[step] = shifted(below[step - 1], 2, range(2 * (step - 1), count - 2))
            above[step] = shifted(above[step - 1], -2, range(2, count - 2 * (step - 1)))
        order = {0: own}
        for near in range(1, (groups - 1) // 2 + 1):
            far = groups - near
            early = jnp.where(place < near, above[near], below[near])
            _, over, under, away = lax.optimization_barrier(
                (early, above[near], below[far], above[far])
            )
            order[near] = early
            late = jnp.where(place < far, over, under)
            order[far] = jnp.where(place < near, away, late)
        if groups % 2 == 0:
            mid = groups // 2
            order[mid] = jnp.where(place < mid, above[mid], below[mid])
        return order

    mixed_rows = mixer_rows(conv_outer, conv_inner, conv_input, conv_taps)
    projected = project(mixed_rows, out_weight, own_rows)
    mixed = jax.nn.sigmoid(f32(mix_gate)) * projected
    hidden_state = bf16(f32(residual) + rms_scale(mixed, mix_gain))
    normed = bf16(rms_scale(f32(hidden_state), expert_gain))

    blocks = spread(jnp.concatenate([normed, table], 1))
    depth = normed.shape[1]

    def served(block):
        rows = block[:, :depth]
        chosen = jnp.arange(lanes, dtype=jnp.int32)[:, None] % count
        picks = bf16(chosen == jnp.stack([me, me ^ 1])[None, :])
        picks = jnp.where(jnp.arange(lanes)[:, None] < 2 * count, picks, 0)
        shares = jnp.dot(block[:, depth:], picks, preferred_element_type=jnp.float32)
        wide = 2 * half
        first = jnp.dot(rows, gate_both, preferred_element_type=jnp.float32)
        second = jnp.dot(rows, up_both, preferred_element_type=jnp.float32)
        mine = jnp.arange(2 * wide)[None, :] < wide
        share = jnp.where(mine, shares[:, :1], shares[:, 1:])
        hidden = lax.optimization_barrier(bf16(jax.nn.silu(first) * second * share))
        return lax.optimization_barrier(
            jnp.dot(hidden, down_both, preferred_element_type=jnp.float32)
        )

    results = {number: served(block) for number, block in blocks.items()}

    def for_upper(step):
        gone = groups - step
        if step == gone or step < gone:
            return results[gone]
        return jnp.where(place < gone, results[gone], results[step])

    down = up = None
    for step in range(1, groups):
        gone = groups - step
        lower, upper = results[gone], for_upper(step)
        if down is not None:
            lower, upper = lower + f32(down), upper + f32(up)
        down = shifted(bf16(lower), -2, range(2 * gone, count))
        up = shifted(bf16(upper), 2, range(0, count - 2 * gone))
    result = f32(hidden_state) + results[0]
    if down is not None:
        result = result + f32(down) + f32(up)
    return bf16(result)


MESH_ID = pl.DeviceIdType.MESH
OWN, OTHER, OUT, ARRIVE, FORWARD, SEND_ACROSS, SEND_OUTWARD = (8 << i for i in range(7))
HIDDEN_READY, DOWN_READY, FAR_PASS, FAR_READY = (8 << i for i in range(7, 11))
GATE_PASS, UP_PASS, FIRST_PASS, DOWN_PASS = (8 << i for i in range(11, 15))
LATE_RELAY, LATE_PASS, LATER, LATE_READY = (8 << i for i in range(15, 19))

OUTER_STEPS = (
    1 | OWN,
    4 | OWN | ARRIVE,
    DOWN_PASS,
    FIRST_PASS,
    UP_PASS,
    GATE_PASS,
    DOWN_READY,
    HIDDEN_READY,
    4 | OTHER,
    4 | OUT,
    6 | OWN | ARRIVE,
    LATE_RELAY,
    6 | OTHER,
    6 | OUT,
    7 | OWN | ARRIVE,
    7 | OTHER,
    7 | OUT,
    LATE_PASS,
    LATE_READY,
    7 | OUT | LATER,
    6 | OUT | LATER,
    2 | OWN | ARRIVE,
    5 | OWN | ARRIVE,
    5 | OTHER,
    5 | OUT,
    4 | OUT | LATER,
    2 | OTHER,
    3 | OWN | ARRIVE,
    3 | OTHER,
    3 | OUT,
    0 | OWN,
    0 | OTHER,
    1 | OTHER,
    1 | OUT,
    2 | OUT,
    1 | OUT | LATER,
    0 | OUT,
    0 | OUT | LATER,
    0,
    0,
    0,
    0,
    0,
    0,
    0,
)
INNER_STEPS = (
    4 | OWN | ARRIVE | FORWARD,
    0 | OWN | ARRIVE | FORWARD,
    2 | OWN,
    3 | OWN,
    1 | OWN | ARRIVE | FORWARD,
    6 | OWN | ARRIVE | FORWARD,
    DOWN_PASS,
    SEND_ACROSS,
    FIRST_PASS,
    GATE_PASS,
    7 | OWN | ARRIVE | FORWARD,
    DOWN_READY,
    UP_PASS,
    FAR_PASS,
    HIDDEN_READY,
    4 | OTHER,
    LATE_RELAY,
    6 | OTHER,
    4 | OUT,
    5 | OWN | ARRIVE | FORWARD,
    7 | OTHER,
    6 | OUT,
    SEND_OUTWARD,
    7 | OUT,
    LATE_PASS,
    5 | OTHER,
    0 | OTHER,
    LATE_READY,
    1 | OTHER,
    7 | OUT | LATER,
    1 | OUT,
    6 | OUT | LATER,
    2 | OTHER,
    1 | OUT | LATER,
    FAR_READY,
    5 | OUT,
    0 | OUT,
    3 | OTHER,
    5 | OUT | LATER,
    0 | OUT | LATER,
    4 | OUT | LATER,
    3 | OUT,
    3 | OUT | LATER,
    2 | OUT,
    2 | OUT | LATER,
)


def mega_kernel(
    co_hbm, ci_hbm, cx_hbm, taps, ow_hbm, mg_hbm, res_hbm, mgain, egain, ids, scores, group,
    g_hbm, u_hbm, d_hbm, out_hbm,
    ci, cx, co, ow, mg, res, mix, acc, part_out, part_in, x_out, x_in,
    X, T, P, S, H, HR, g1, u1, g2, u2, wd, wdo, picks,
    load_sem, halo_s, halo_r, tab_s, tab_r, core_s, core_r, xsw_s, xsw_r,
    w_s, w_r, rows_s, rows_r, sum_s, sum_r, hid_s, hid_r, do_s, do_r, out_sem,
):
    sp = lax.axis_index("sp")
    tp = lax.axis_index("tp")
    z = sp // 2
    y = sp % 2
    half = z // 2
    outer = z * (3 - z) == 0
    inner = jnp.logical_not(outer)
    own = jnp.where(outer, 0, 1)
    core_peer = tp + 1 - 2 * (tp % 2)
    x_peer = (tp + 2) % 4
    y_peer = sp + 1 - 2 * y
    rows, depth = res.shape
    piece = rows // 2
    width = g1.shape[1]
    count = T.shape[1] // 2
    channels = ow.shape[0]
    halo = ci.shape[0] - co.shape[0]

    def line(slot):
        where = jnp.where(slot == 0, 3 * half, jnp.where(slot == 1, 1 + half, jnp.where(slot == 2, 2 - half, 3 - 3 * half)))
        return 2 * where + y

    def remote(src, dst, s, r, device):
        return pltpu.make_async_remote_copy(
            src_ref=src, dst_ref=dst, send_sem=s, recv_sem=r, device_id=device, device_id_type=MESH_ID
        )

    barrier = pltpu.get_barrier_semaphore()

    def greet(device):
        pl.semaphore_signal(barrier, inc=1, device_id=device, device_id_type=MESH_ID)

    greet((sp, core_peer))
    greet((sp, x_peer))
    greet((y_peer, tp))
    greet((line(1 - own), tp))

    @pl.when(inner)
    def _():
        greet((line(2), tp))

    has_next = jnp.logical_and(y == 1, sp < count - 1)
    has_last = jnp.logical_and(y == 0, sp > 0)

    @pl.when(has_next)
    def _():
        greet((sp + 1, tp))

    @pl.when(has_last)
    def _():
        greet((sp - 1, tp))

    tokens = co.shape[0]
    loads = [
        pltpu.make_async_copy(ci_hbm, ci.at[pl.ds(halo, tokens)], load_sem.at[0]),
        pltpu.make_async_copy(cx_hbm, cx.at[pl.ds(halo, tokens)], load_sem.at[1]),
        pltpu.make_async_copy(co_hbm, co, load_sem.at[2]),
        pltpu.make_async_copy(ow_hbm, ow, load_sem.at[3]),
        pltpu.make_async_copy(mg_hbm, mg, load_sem.at[4]),
        pltpu.make_async_copy(res_hbm, res, load_sem.at[5]),
        pltpu.make_async_copy(g_hbm.at[0], g1, load_sem.at[6]),
        pltpu.make_async_copy(u_hbm.at[0], u1, load_sem.at[7]),
        pltpu.make_async_copy(d_hbm.at[0], wd.at[pl.ds(0, width)], load_sem.at[8]),
    ]
    for k in (0, 1, 3, 2):
        loads[k].start()

    raw = scores[...]
    top = jnp.maximum(raw[0:1], raw[1:2])
    up = jnp.exp(raw - top)
    weights = group[...] * (up / (up[0:1] + up[1:2]))
    coarse = f32(bf16(weights))
    fine = weights - coarse
    line_of = lax.broadcasted_iota(jnp.int32, (T.shape[1], rows), 0)
    entries = jnp.zeros((T.shape[1], rows), jnp.float32)
    for k in range(2):
        entries = entries + jnp.where(line_of == ids[k : k + 1], coarse[k : k + 1], 0.0)
        entries = entries + jnp.where(line_of == ids[k : k + 1] + count, fine[k : k + 1], 0.0)
    entries = bf16(entries)
    for p in range(2):
        T[2 * own + p] = entries[:, (1 - p) * piece : (2 - p) * piece]

    pl.semaphore_wait(barrier, 4 + jnp.where(inner, 1, 0) + jnp.where(has_next, 1, 0) + jnp.where(has_last, 1, 0))

    def halo_copy(k, device):
        src = (ci_hbm, cx_hbm)[k].at[pl.ds(tokens - halo, halo)]
        return remote(src, (ci, cx)[k].at[pl.ds(0, halo)], halo_s.at[k], halo_r.at[k], device)

    @pl.when(sp < count - 1)
    def _():
        for k in range(2):
            halo_copy(k, (sp + 1, tp)).start()

    eighth = depth // 8
    wide = width // 2
    side = tp % 2
    tile = min(512, depth)
    tiles = depth // tile
    quarter = width // 4
    first = jnp.where(tp // 2 == 0, side, 6 + side)
    lacking = jnp.where(tp // 2 == 0, 6 + side, side)

    def weight_copy(k, leg):
        block = (first, 2 + side, 4 + side, first, 2 + side, 4 + side, lacking, first)[leg]
        at = pl.ds(pl.multiple_of(block * eighth, eighth), eighth)
        buf = (g2, u2)[k]
        src = (g_hbm, u_hbm)[k].at[0, at] if leg < 3 else buf.at[at]
        device = (y_peer, tp) if leg < 3 else (sp, core_peer) if leg < 7 else (sp, x_peer)
        return remote(src, buf.at[at], w_s.at[8 * k + leg], w_r.at[8 * k + leg], device)

    def tile_copy(t, leg):
        row = (x_peer if leg == 3 else tp) * quarter
        cols = pl.ds(t * tile, tile)
        dst = wd.at[pl.ds(pl.multiple_of(width + row, quarter), quarter), cols]
        src = d_hbm.at[0, pl.ds(pl.multiple_of(row, quarter), quarter), cols] if leg == 0 else dst
        device = ((y_peer, tp), (sp, core_peer), (sp, x_peer), (sp, core_peer))[leg]
        return remote(src, dst, w_s.at[16 + 4 * t + leg], w_r.at[16 + 4 * t + leg], device)

    early = range(tiles // 2)
    late = range(tiles // 2, tiles)
    for k in range(2):
        weight_copy(k, 0).start()
    for t in early:
        tile_copy(t, 0).start()
    for k in range(2):
        weight_copy(k, 1).start()
        weight_copy(k, 2).start()
    for t in late:
        tile_copy(t, 0).start()

    part = wide // 2

    def down_copy(leg):
        if leg < 2:
            src = d_hbm.at[0, pl.ds(pl.multiple_of(side * wide + leg * part, part), part)]
            dst = wdo.at[pl.ds(pl.multiple_of(side * wide + leg * part, part), part)]
            device = (line(1), tp)
        else:
            near = wdo.at[pl.ds(pl.multiple_of(side * wide, wide), wide)]
            far = wdo.at[pl.ds(pl.multiple_of(width + side * wide, wide), wide)]
            src, dst = ((near, near), (near, far), (far, far))[leg - 2]
            device = (y_peer, tp) if leg == 3 else (sp, core_peer)
        return remote(src, dst, do_s.at[leg], do_r.at[leg], device)

    @pl.when(outer)
    def _():
        down_copy(0).start()

    def table_copy(slot, across):
        dst = 3 - slot if across else slot
        at = slot + (4 if across else 0)
        return remote(
            T.at[pl.ds(2 * slot, 2)],
            T.at[pl.ds(2 * dst, 2)],
            tab_s.at[at],
            tab_r.at[dst],
            (line(2) if across else line(1 - own), tp),
        )

    def table_came(slot):
        at = T.at[pl.ds(2 * slot, 2)]
        remote(at, at, tab_s.at[0], tab_r.at[slot], (sp, core_peer)).wait_recv()

    table_copy(own, False).start()

    @pl.when(inner)
    def _():
        table_copy(1, True).start()

    P[0] = jnp.zeros(P.shape[1:], P.dtype)
    lane = lax.broadcasted_iota(jnp.int32, (T.shape[1], width), 0)
    for k in range(2):
        picks[k] = jnp.where(lane % count == (sp, y_peer)[k], 1.0, 0.0).astype(picks.dtype)

    for k in range(3):
        loads[k].wait()
    for k in range(4, 9):
        loads[k].start()

    kept = taps.shape[0] - 1
    run = 32

    def conv(start):
        def some(i, c):
            at = pl.multiple_of(start + i * run, run)
            near = f32(ci[pl.ds(at, halo + run)]) * f32(cx[pl.ds(at, halo + run)])
            total = taps[0:1] * near[halo - kept : halo - kept + run]
            for j in range(1, kept + 1):
                total = total + taps[j : j + 1] * near[halo - kept + j : halo - kept + j + run]
            mix[pl.ds(at, run)] = bf16(f32(co[pl.ds(at, run)]) * total)
            return c

        lax.fori_loop(0, piece // run, some, 0)

    loads[3].wait()

    def core_copy(phase, p):
        at = 2 * phase + p
        return remote(part_out.at[at], part_in.at[at], core_s.at[at], core_r.at[at], (sp, core_peer))

    some_rows = piece // 2

    def x_copy(p, k):
        at = pl.ds(k * some_rows, some_rows)
        return remote(
            x_out.at[p, at], x_in.at[p, at], xsw_s.at[2 * p + k], xsw_r.at[2 * p + k], (sp, x_peer)
        )

    def projected(i, carry):
        phase = i // 4
        p = i // 2 % 2
        second = i % 2 == 1
        owner = jnp.where(
            phase == 0, jnp.where(second, x_peer, 3 - tp), jnp.where(second, tp, core_peer)
        )
        start = pl.multiple_of(owner * rows + (1 - p) * piece, piece)

        @pl.when(jnp.logical_and(i == 2, sp == 0))
        def _():
            ci[pl.ds(0, halo)] = jnp.zeros((halo, channels), ci.dtype)
            cx[pl.ds(0, halo)] = jnp.zeros((halo, channels), cx.dtype)

        @pl.when(jnp.logical_and(i == 2, sp > 0))
        def _():
            for k in range(2):
                halo_copy(k, (sp, core_peer)).wait_recv()

        conv(start)

        def some(n, c):
            cols = pl.ds(pl.multiple_of(n * tile, tile), tile)
            got = jnp.dot(mix[pl.ds(start, piece)], ow[:, cols], preferred_element_type=jnp.float32)

            @pl.when(second)
            def _():
                acc[p, :, cols] = got

            @pl.when(jnp.logical_not(second))
            def _():
                part_out[2 * phase + p, :, cols] = bf16(got)

            return c

        lax.fori_loop(0, depth // tile, some, 0)

        @pl.when(jnp.logical_not(second))
        def _():
            core_copy(phase, p).start()

        @pl.when(jnp.logical_and(second, phase == 0))
        def _():
            core_copy(0, p).wait_recv()

            def add(r, c):
                at = pl.ds(pl.multiple_of(r * 16, 16), 16)
                x_out[p, at] = bf16(acc[p, at] + f32(part_in[p, at]))
                return c

            steps = some_rows // 16
            for k in range(2):
                lax.fori_loop(k * steps, (k + 1) * steps, add, 0)
                x_copy(p, k).start()

        return carry

    lax.fori_loop(0, 8, projected, 0)
    loads[4].wait()
    loads[5].wait()

    def rows_copy(item, device, dst, at, k):
        some = pl.ds(k * some_rows, some_rows)
        return remote(X.at[item, some], X.at[dst, some], rows_s.at[at, k], rows_r.at[dst, k], device)

    def normalize(c, k):
        def some(r, carry):
            at = pl.ds(pl.multiple_of(r * 16, 16), 16)
            src = pl.ds(pl.multiple_of((1 - c) * piece + r * 16, 16), 16)
            total = acc[c, at] + f32(part_in[2 + c, at]) + f32(x_in[c, at])
            mixed = jax.nn.sigmoid(f32(mg[src])) * total
            state = bf16(f32(res[src]) + rms_scale(mixed, mgain[...]))
            P[1 + c, at] = state
            X[2 * own + c, at] = bf16(rms_scale(f32(state), egain[...]))
            return carry

        steps = some_rows // 16
        lax.fori_loop(k * steps, (k + 1) * steps, some, 0)

    def send_own(c, k, across):
        item = 2 * own + c
        if across:
            rows_copy(item, (line(2), tp), 4 + c, 8 + c, k).start()
        else:
            rows_copy(item, (line(1 - own), tp), item, item, k).start()

    def weight_on(k, came, *legs):
        weight_copy(k, came).wait_recv()
        for leg in legs:
            weight_copy(k, leg).start()

    def tile_on(t, came, *legs):
        tile_copy(t, came).wait_recv()
        for leg in legs:
            tile_copy(t, leg).start()

    @pl.when(inner)
    def _():
        table_came(0)
        table_copy(0, True).start()
        table_came(2)
        table_copy(2, False).start()

    weight_on(0, 0, 3, 7)
    core_copy(1, 0).wait_recv()
    for k in range(2):
        x_copy(0, k).wait_recv()
        normalize(0, k)
        send_own(0, k, False)

        @pl.when(inner)
        def _():
            send_own(0, k, True)

    @pl.when(inner)
    def _():
        table_came(3)
        table_copy(3, False).start()

    weight_on(1, 0, 3, 7)
    core_copy(1, 1).wait_recv()
    for k in range(2):
        x_copy(1, k).wait_recv()
        normalize(1, k)

        @pl.when(outer)
        def _():
            send_own(1, k, False)

    @pl.when(outer)
    def _():
        down_copy(1).start()

    for t in early:
        tile_on(t, 0, 1, 2)
    for k in range(6, 9):
        loads[k].wait()

    @pl.when(outer)
    def _():
        for slot in range(1, 4):
            table_came(slot)

    def hidden(item, k):
        gate, up = ((g1, u1), (g2, u2))[k]
        x = X[item]
        first = jnp.dot(x, gate[...], preferred_element_type=jnp.float32)
        second = jnp.dot(x, up[...], preferred_element_type=jnp.float32)
        share = lax.dot_general(
            T[item], picks[k], (((0,), (0,)), ((), ())), preferred_element_type=jnp.float32
        )
        H[item, :, k * width : (k + 1) * width] = bf16(jax.nn.silu(first) * second * share)

    def sum_copy(item, m):
        slot = item // 2
        c = item % 2
        to = jnp.where(outer, 1, jnp.where(slot == 0, 0, 2))
        dst = jnp.where(outer, jnp.where(slot == 2, 9 + c, 3 + c), jnp.where(slot == 2, 7 + c, 5 + c))
        cols = pl.ds(pl.multiple_of(m * tile, tile), tile)
        return remote(S.at[item, :, cols], P.at[dst, :, cols], sum_s.at[item, m], sum_r.at[dst, m], (line(to), tp))

    def held(item):
        return jnp.where(item == 5, 2, item - 2)

    def hidden_copy(item):
        at = held(item)
        return remote(H.at[item], HR.at[at], hid_s.at[at], hid_r.at[at], (line(1), tp))

    def out_copy(c, m):
        cols = pl.ds(pl.multiple_of(m * tile, tile), tile)
        return pltpu.make_async_copy(
            S.at[2 * own + c, :, cols],
            out_hbm.at[pl.ds(pl.multiple_of((1 - c) * piece, piece), piece), cols],
            out_sem.at[c, m],
        )

    def came(at, m):
        cols = pl.ds(pl.multiple_of(m * tile, tile), tile)
        ref = P.at[at, :, cols]
        remote(ref, ref, sum_s.at[0, m], sum_r.at[at, m], (sp, core_peer)).wait_recv()

    def step(n, carry):
        code = 0
        for i, (a, b) in enumerate(zip(OUTER_STEPS, INNER_STEPS)):
            code = jnp.where(n == i, jnp.where(outer, a, b), code)
        item = code % 8

        def has(flag):
            return code // flag % 2 == 1

        slot = item // 2
        c = item % 2

        for k in range(2):

            @pl.when(has(ARRIVE))
            def _():
                rows_copy(item, (sp, core_peer), item, item, k).wait_recv()

            @pl.when(has(FORWARD))
            def _():
                across = slot == 0
                rows_copy(
                    item,
                    (line(jnp.where(across, 2, 0)), tp),
                    jnp.where(across, 6 + c, item),
                    jnp.where(across, 10 + c, item),
                    k,
                ).start()

        @pl.when(has(SEND_ACROSS))
        def _():
            for k in range(2):
                send_own(1, k, True)

        @pl.when(has(SEND_OUTWARD))
        def _():
            for k in range(2):
                send_own(1, k, False)

        for k in range(2):

            @pl.when(has((GATE_PASS, UP_PASS)[k]))
            def _():
                weight_on(k, 1, 4)
                weight_on(k, 2, 5)

        @pl.when(has(FIRST_PASS))
        def _():
            weight_on(0, 7, 6)
            weight_on(1, 7, 6)

        @pl.when(has(DOWN_PASS))
        def _():
            for t in early:
                tile_on(t, 2, 3)

        @pl.when(has(LATE_RELAY))
        def _():
            for t in late:
                tile_on(t, 0, 1, 2)

        @pl.when(has(LATE_PASS))
        def _():
            for t in late:
                tile_on(t, 2, 3)

        @pl.when(has(HIDDEN_READY))
        def _():
            for k in range(2):
                for leg in range(3, 7):
                    weight_copy(k, leg).wait_recv()

        for flag, some_tiles in ((DOWN_READY, early), (LATE_READY, late)):

            @pl.when(has(flag))
            def _():
                for t in some_tiles:
                    tile_copy(t, 1).wait_recv()
                    tile_copy(t, 3).wait_recv()

        @pl.when(has(FAR_PASS))
        def _():
            down_copy(0).wait_recv()
            down_copy(1).wait_recv()
            down_copy(2).start()
            down_copy(3).start()

        @pl.when(has(FAR_READY))
        def _():
            down_copy(3).wait_recv()
            down_copy(4).start()
            down_copy(2).wait_recv()
            down_copy(4).wait_recv()

        @pl.when(has(OWN))
        def _():
            hidden(item, 0)

        @pl.when(has(OTHER))
        def _():
            hidden(item, 1)

        middle = jnp.logical_or(slot == 1, item == 5)
        begins = code // LATER % 2 == 0

        @pl.when(jnp.logical_and(has(OUT), jnp.logical_and(outer, middle)))
        def _():
            hidden_copy(item).start()

        @pl.when(jnp.logical_and(has(OUT), jnp.logical_not(jnp.logical_and(outer, middle))))
        def _():
            inner_at = jnp.where(slot == 1, 7 + c, jnp.where(slot == 2, jnp.where(c == 0, 9, 0), 3 + c))
            a = jnp.where(slot == 0, 5 + c, jnp.where(outer, 0, inner_at))
            d = jnp.where(slot == own, 1 + c, 0)

            @pl.when(jnp.logical_and(middle, begins))
            def _():
                ref = HR.at[held(item)]
                remote(ref, ref, hid_s.at[0], hid_r.at[held(item)], (sp, core_peer)).wait_recv()

            def some(m, carry):
                cols = pl.ds(pl.multiple_of(m * tile, tile), tile)

                @pl.when(a > 0)
                def _():
                    came(a, m)

                got = jnp.dot(H[item], wd[:, cols], preferred_element_type=jnp.float32)
                got = got + f32(P[d, :, cols]) + f32(P[a, :, cols])

                @pl.when(middle)
                def _():
                    more = jnp.dot(HR[held(item)], wdo[:, cols], preferred_element_type=jnp.float32)
                    S[item, :, cols] = bf16(got + more)

                @pl.when(jnp.logical_not(middle))
                def _():
                    S[item, :, cols] = bf16(got)

                @pl.when(slot == own)
                def _():
                    out_copy(c, m).start()

                @pl.when(slot != own)
                def _():
                    sum_copy(item, m).start()

                return carry

            begin = jnp.where(begins, 0, tiles // 2)
            lax.fori_loop(begin, begin + tiles // 2, some, 0)

        return carry

    lax.fori_loop(0, len(OUTER_STEPS), step, 0)

    for c in range(2):
        for m in range(depth // tile):
            out_copy(c, m).wait()
        core_copy(0, c).wait_send()
        core_copy(1, c).wait_send()
        x_copy(c, 0).wait_send()
        x_copy(c, 1).wait_send()

    @pl.when(sp < count - 1)
    def _():
        for k in range(2):
            halo_copy(k, (sp + 1, tp)).wait_send()

    for k in range(2):
        for leg in range(8):
            weight_copy(k, leg).wait_send()
    for t in range(tiles):
        for leg in range(4):
            tile_copy(t, leg).wait_send()
    table_copy(own, False).wait_send()

    @pl.when(inner)
    def _():
        table_copy(1, True).wait_send()
        table_copy(0, True).wait_send()
        table_copy(2, False).wait_send()
        table_copy(3, False).wait_send()


    def gone(at):
        for k in range(2):
            rows_copy(at % 8, (sp, core_peer), at % 8, at, k).wait_send()

    def summed(item):
        for m in range(depth // tile):
            sum_copy(item, m).wait_send()

    for c in range(2):
        gone(2 * own + c)

    @pl.when(outer)
    def _():
        summed(4)
        hidden_copy(5).wait_send()
        for c in range(2):
            down_copy(c).wait_send()
            summed(6 + c)
            hidden_copy(2 + c).wait_send()

    @pl.when(inner)
    def _():
        for leg in range(2, 5):
            down_copy(leg).wait_send()
        for c in range(2):
            for at in (4 + c, 6 + c, 8 + c, 10 + c):
                gone(at)
            for slot in (0, 2, 3):
                summed(2 * slot + c)


def mega(
    conv_outer, conv_inner, conv_input, conv_taps, out_weight, mix_gate, residual, mix_gain, expert_gain,
    expert_ids, group_share, pair_scores, gate_experts, up_experts, down_experts,
):
    count = lax.axis_size("sp")
    rows, depth = residual.shape
    tokens, channels = conv_inner.shape
    width = gate_experts.shape[2]
    piece = rows // 2
    halo = 16
    tiles = depth // min(512, depth)
    half_type, full = jnp.bfloat16, jnp.float32
    hbm = pl.BlockSpec(memory_space=pl.ANY)
    vmem = pl.BlockSpec(memory_space=pltpu.VMEM)
    dma = pltpu.SemaphoreType.DMA
    return pl.pallas_call(
        mega_kernel,
        out_shape=jax.ShapeDtypeStruct((rows, depth), half_type),
        in_specs=[hbm, hbm, hbm, vmem, hbm, hbm, hbm, vmem, vmem, vmem, vmem, vmem, hbm, hbm, hbm],
        out_specs=hbm,
        scratch_shapes=[
            pltpu.VMEM((halo + tokens, channels), half_type),
            pltpu.VMEM((halo + tokens, channels), half_type),
            pltpu.VMEM((tokens, channels), half_type),
            pltpu.VMEM((channels, depth), half_type),
            pltpu.VMEM((rows, depth), half_type),
            pltpu.VMEM((rows, depth), half_type),
            pltpu.VMEM((tokens, channels), half_type),
            pltpu.VMEM((2, piece, depth), full),
            pltpu.VMEM((4, piece, depth), half_type),
            pltpu.VMEM((4, piece, depth), half_type),
            pltpu.VMEM((2, piece, depth), half_type),
            pltpu.VMEM((2, piece, depth), half_type),
            pltpu.VMEM((8, piece, depth), half_type),
            pltpu.VMEM((8, 2 * count, piece), half_type),
            pltpu.VMEM((11, piece, depth), half_type),
            pltpu.VMEM((8, piece, depth), half_type),
            pltpu.VMEM((8, piece, 2 * width), half_type),
            pltpu.VMEM((3, piece, 2 * width), half_type),
            pltpu.VMEM((depth, width), half_type),
            pltpu.VMEM((depth, width), half_type),
            pltpu.VMEM((depth, width), half_type),
            pltpu.VMEM((depth, width), half_type),
            pltpu.VMEM((2 * width, depth), half_type),
            pltpu.VMEM((2 * width, depth), half_type),
            pltpu.VMEM((2, 2 * count, width), half_type),
            dma((9,)),
            dma((2,)),
            dma((2,)),
            dma((8,)),
            dma((4,)),
            dma((4,)),
            dma((4,)),
            dma((4,)),
            dma((4,)),
            dma((16 + 4 * tiles,)),
            dma((16 + 4 * tiles,)),
            dma((16, 2)),
            dma((8, 2)),
            dma((8, tiles)),
            dma((11, tiles)),
            dma((3,)),
            dma((3,)),
            dma((5,)),
            dma((5,)),
            dma((2, tiles)),
        ],
        compiler_params=pltpu.CompilerParams(
            collective_id=0, has_side_effects=True, vmem_limit_bytes=60 * 1024 * 1024
        ),
        name="layer",
    )(
        conv_outer, conv_inner, conv_input, conv_taps, out_weight, mix_gate, residual,
        mix_gain[None, :], expert_gain[None, :], expert_ids.T, pair_scores.T, group_share[None, :], gate_experts, up_experts, down_experts,
    )


def solution(mesh):
    placed = (
        P("sp", "tp"),
        P("sp", "tp"),
        P("sp", "tp"),
        P(None, "tp"),
        P("tp", None),
        P(("sp", "tp"), None),
        P(("sp", "tp"), None),
        P(),
        P(),
        P(("sp", "tp"), None),
        P(("sp", "tp")),
        P(("sp", "tp"), None),
        P("sp", None, None),
        P("sp", None, None),
        P("sp", None, None),
    )

    square = mesh.shape["tp"] == 4 and mesh.shape["sp"] == 8

    def layer(*arrays):
        return (mega if square else per_device)(*arrays)

    return jax.shard_map(
        layer, mesh=mesh, in_specs=placed, out_specs=P(("sp", "tp"), None), check_vma=False
    )
```

```python
import jax
import jax.numpy as jnp
from jax import lax
from jax.experimental import pallas as pl
from jax.experimental.pallas import tpu as pltpu
from jax.sharding import PartitionSpec as P

epsilon = 1e-06


def f32(value):
    return value.astype(jnp.float32)


def bf16(value):
    return value.astype(jnp.bfloat16)


def rms_scale(values, gain):
    return values * lax.rsqrt(jnp.mean(values * values, axis=-1, keepdims=True) + epsilon) * gain


def shifted(value, steps, senders):
    return lax.ppermute(value, "sp", [(s, s + steps) for s in senders])


def swapped(value, axis, bit):
    return lax.ppermute(value, axis, [(s, s ^ bit) for s in range(lax.axis_size(axis))])


def mixer_rows(conv_outer, conv_inner, conv_input, conv_taps):
    kept = conv_taps.shape[0] - 1
    inner = f32(conv_inner) * f32(conv_input)
    tail = f32(conv_inner[-kept:]) * f32(conv_input[-kept:])
    earlier = shifted(tail, 1, range(lax.axis_size("sp") - 1))
    length = conv_inner.shape[0]
    inner = jnp.concatenate([earlier, inner], 0)
    conv = conv_taps[0] * inner[0:length]
    for offset in range(1, kept + 1):
        conv = conv + conv_taps[offset] * inner[offset : offset + length]
    return bf16(f32(conv_outer) * conv)


def project(mixed_rows, out_weight, own_rows):
    parts = lax.axis_size("tp")
    me = lax.axis_index("tp")
    blocks = mixed_rows.reshape(parts, own_rows, -1)

    def partial(owner):
        rows = lax.dynamic_index_in_dim(blocks, owner, 0, keepdims=False)
        return jnp.dot(rows, out_weight, preferred_element_type=jnp.float32)

    def total(owner_bits, bit):
        if bit == 1:
            return partial(me ^ owner_bits)
        half = bit // 2
        sent = bf16(total(owner_bits | half, half))
        given = swapped(sent, "tp", half)
        return total(owner_bits, half) + f32(given)

    return total(0, parts)


def routing_table(expert_ids, group_share, pair_scores, own_rows, count):
    weights = group_share[:, None] * jax.nn.softmax(pair_scores, axis=-1)
    lanes = -(-2 * count // 128) * 128
    column = jnp.arange(lanes, dtype=jnp.int32)[None, :]
    coarse = lax.reduce_precision(weights, 8, 7)
    fine = weights - coarse
    table = jnp.zeros((own_rows, lanes), jnp.float32)
    for slot in range(expert_ids.shape[1]):
        at = expert_ids[:, slot : slot + 1]
        table = table + jnp.where(column == at, coarse[:, slot : slot + 1], 0.0)
        table = table + jnp.where(column == at + count, fine[:, slot : slot + 1], 0.0)
    return bf16(table)


def per_device(
    conv_outer,
    conv_inner,
    conv_input,
    conv_taps,
    out_weight,
    mix_gate,
    residual,
    mix_gain,
    expert_gain,
    expert_ids,
    group_share,
    pair_scores,
    gate_experts,
    up_experts,
    down_experts,
):
    count = lax.axis_size("sp")
    me = lax.axis_index("sp")
    own_rows = residual.shape[0]
    groups = count // 2
    place = me // 2
    side = lax.axis_index("tp") % 2
    half = gate_experts.shape[2] // 2

    def fetched(weight, axis):
        piece = lax.dynamic_slice_in_dim(weight[0], side * half, half, axis)
        first = swapped(piece, "sp", 1)
        second = swapped(first, "tp", 1)
        return jnp.concatenate([weight[0], first, second], axis)

    gate_both = fetched(gate_experts, 1)
    up_both = fetched(up_experts, 1)
    down_both = fetched(down_experts, 0)

    lanes = -(-2 * count // 128) * 128
    table = routing_table(expert_ids, group_share, pair_scores, own_rows, count)

    def spread(own):
        below, above = {0: own}, {0: own}
        for step in range(1, groups):
            below[step] = shifted(below[step - 1], 2, range(2 * (step - 1), count - 2))
            above[step] = shifted(above[step - 1], -2, range(2, count - 2 * (step - 1)))
        order = {0: own}
        for near in range(1, (groups - 1) // 2 + 1):
            far = groups - near
            early = jnp.where(place < near, above[near], below[near])
            _, over, under, away = lax.optimization_barrier(
                (early, above[near], below[far], above[far])
            )
            order[near] = early
            late = jnp.where(place < far, over, under)
            order[far] = jnp.where(place < near, away, late)
        if groups % 2 == 0:
            mid = groups // 2
            order[mid] = jnp.where(place < mid, above[mid], below[mid])
        return order

    mixed_rows = mixer_rows(conv_outer, conv_inner, conv_input, conv_taps)
    projected = project(mixed_rows, out_weight, own_rows)
    mixed = jax.nn.sigmoid(f32(mix_gate)) * projected
    hidden_state = bf16(f32(residual) + rms_scale(mixed, mix_gain))
    normed = bf16(rms_scale(f32(hidden_state), expert_gain))

    blocks = spread(jnp.concatenate([normed, table], 1))
    depth = normed.shape[1]

    def served(block):
        rows = block[:, :depth]
        chosen = jnp.arange(lanes, dtype=jnp.int32)[:, None] % count
        picks = bf16(chosen == jnp.stack([me, me ^ 1])[None, :])
        picks = jnp.where(jnp.arange(lanes)[:, None] < 2 * count, picks, 0)
        shares = jnp.dot(block[:, depth:], picks, preferred_element_type=jnp.float32)
        wide = 2 * half
        first = jnp.dot(rows, gate_both, preferred_element_type=jnp.float32)
        second = jnp.dot(rows, up_both, preferred_element_type=jnp.float32)
        mine = jnp.arange(2 * wide)[None, :] < wide
        share = jnp.where(mine, shares[:, :1], shares[:, 1:])
        hidden = lax.optimization_barrier(bf16(jax.nn.silu(first) * second * share))
        return lax.optimization_barrier(
            jnp.dot(hidden, down_both, preferred_element_type=jnp.float32)
        )

    results = {number: served(block) for number, block in blocks.items()}

    def for_upper(step):
        gone = groups - step
        if step == gone or step < gone:
            return results[gone]
        return jnp.where(place < gone, results[gone], results[step])

    down = up = None
    for step in range(1, groups):
        gone = groups - step
        lower, upper = results[gone], for_upper(step)
        if down is not None:
            lower, upper = lower + f32(down), upper + f32(up)
        down = shifted(bf16(lower), -2, range(2 * gone, count))
        up = shifted(bf16(upper), 2, range(0, count - 2 * gone))
    result = f32(hidden_state) + results[0]
    if down is not None:
        result = result + f32(down) + f32(up)
    return bf16(result)


MESH_ID = pl.DeviceIdType.MESH
OWN, OTHER, OUT, ARRIVE, FORWARD, LATER = (8 << i for i in range(6))
SPECIAL = 8 << 6
(DOWN_PASS, SEND_ACROSS, FIRST_PASS, GATE_PASS, UP_PASS, DOWN_READY, FAR_PASS, HIDDEN_READY, SEND_OUTWARD, LATE_RELAY, LATE_PASS, LATE_READY, FAR_READY,) = (SPECIAL << i for i in range(13))

OUTER_STEPS = (
    1 | OWN,
    4 | OWN | ARRIVE,
    0 | DOWN_PASS | FIRST_PASS | UP_PASS,
    4 | OTHER | OUT | GATE_PASS | DOWN_READY | HIDDEN_READY,
    6 | OWN | ARRIVE,
    6 | OTHER | OUT | LATE_RELAY,
    7 | OWN | OTHER | OUT | ARRIVE,
    7 | OUT | LATER | LATE_PASS | LATE_READY,
    6 | OUT | LATER,
    2 | OWN | ARRIVE,
    5 | OWN | OTHER | OUT | ARRIVE,
    4 | OUT | LATER,
    2 | OTHER,
    3 | OWN | OTHER | OUT | ARRIVE,
    0 | OWN | OTHER,
    1 | OTHER | OUT,
    2 | OUT,
    1 | OUT | LATER,
    0 | OUT,
    0 | OUT | LATER,
    0,
    0,
    0,
    0,
    0,
    0,
    0,
    0,
    0,
    0,
    0,
    0,
    0,
    0,
)
INNER_STEPS = (
    4 | OWN | ARRIVE | FORWARD,
    0 | OWN | ARRIVE | FORWARD,
    2 | OWN,
    3 | OWN,
    1 | OWN | ARRIVE | FORWARD,
    6 | OWN | ARRIVE | FORWARD,
    0 | DOWN_PASS | SEND_ACROSS | FIRST_PASS | GATE_PASS,
    7 | OWN | ARRIVE | FORWARD,
    0 | DOWN_READY,
    4 | OTHER | UP_PASS | FAR_PASS | HIDDEN_READY,
    6 | OTHER | LATE_RELAY,
    4 | OUT,
    5 | OWN | ARRIVE | FORWARD,
    7 | OTHER,
    6 | OUT,
    7 | OUT | SEND_OUTWARD,
    5 | OTHER | LATE_PASS,
    0 | OTHER,
    1 | OTHER | LATE_READY,
    7 | OUT | LATER,
    1 | OUT,
    6 | OUT | LATER,
    2 | OTHER,
    1 | OUT | LATER,
    5 | OUT | FAR_READY,
    0 | OUT,
    3 | OTHER,
    5 | OUT | LATER,
    0 | OUT | LATER,
    4 | OUT | LATER,
    3 | OUT,
    3 | OUT | LATER,
    2 | OUT,
    2 | OUT | LATER,
)


def mega_kernel(
    co_hbm, ci_hbm, cx_hbm, taps, ow_hbm, mg_hbm, res_hbm, mgain, egain, ids, scores, group,
    g_hbm, u_hbm, d_hbm, out_hbm,
    ci, cx, co, ow, mg, res, mix, acc, part_out, part_in, x_out, x_in,
    X, T, P, S, H, HR, g1, u1, g2, u2, wd, wdo, picks,
    load_sem, halo_s, halo_r, tab_s, tab_r, core_s, core_r, xsw_s, xsw_r,
    w_s, w_r, rows_s, rows_r, sum_s, sum_r, hid_s, hid_r, do_s, do_r, out_sem,
):
    sp = lax.axis_index("sp")
    tp = lax.axis_index("tp")
    z = sp // 2
    y = sp % 2
    half = z // 2
    outer = z * (3 - z) == 0
    inner = jnp.logical_not(outer)
    own = jnp.where(outer, 0, 1)
    core_peer = tp + 1 - 2 * (tp % 2)
    x_peer = (tp + 2) % 4
    y_peer = sp + 1 - 2 * y
    rows, depth = res.shape
    piece = rows // 2
    width = g1.shape[1]
    count = T.shape[1] // 2
    channels = ow.shape[0]
    halo = ci.shape[0] - co.shape[0]

    def line(slot):
        where = jnp.where(slot == 0, 3 * half, jnp.where(slot == 1, 1 + half, jnp.where(slot == 2, 2 - half, 3 - 3 * half)))
        return 2 * where + y

    def remote(src, dst, s, r, device):
        return pltpu.make_async_remote_copy(
            src_ref=src, dst_ref=dst, send_sem=s, recv_sem=r, device_id=device, device_id_type=MESH_ID
        )

    barrier = pltpu.get_barrier_semaphore()

    def greet(device):
        pl.semaphore_signal(barrier, inc=1, device_id=device, device_id_type=MESH_ID)

    greet((sp, core_peer))
    greet((sp, x_peer))
    greet((y_peer, tp))
    greet((line(1 - own), tp))

    @pl.when(inner)
    def _():
        greet((line(2), tp))

    has_next = jnp.logical_and(y == 1, sp < count - 1)
    has_last = jnp.logical_and(y == 0, sp > 0)

    @pl.when(has_next)
    def _():
        greet((sp + 1, tp))

    @pl.when(has_last)
    def _():
        greet((sp - 1, tp))

    tokens = co.shape[0]
    loads = [
        pltpu.make_async_copy(ci_hbm, ci.at[pl.ds(halo, tokens)], load_sem.at[0]),
        pltpu.make_async_copy(cx_hbm, cx.at[pl.ds(halo, tokens)], load_sem.at[1]),
        pltpu.make_async_copy(co_hbm, co, load_sem.at[2]),
        pltpu.make_async_copy(ow_hbm, ow, load_sem.at[3]),
        pltpu.make_async_copy(mg_hbm, mg, load_sem.at[4]),
        pltpu.make_async_copy(res_hbm, res, load_sem.at[5]),
        pltpu.make_async_copy(g_hbm.at[0], g1, load_sem.at[6]),
        pltpu.make_async_copy(u_hbm.at[0], u1, load_sem.at[7]),
        pltpu.make_async_copy(d_hbm.at[0], wd.at[pl.ds(0, width)], load_sem.at[8]),
    ]
    for k in (0, 1, 3, 2):
        loads[k].start()

    raw = scores[...]
    top = jnp.maximum(raw[0:1], raw[1:2])
    up = jnp.exp(raw - top)
    weights = group[...] * (up / (up[0:1] + up[1:2]))
    coarse = f32(bf16(weights))
    fine = weights - coarse
    line_of = lax.broadcasted_iota(jnp.int32, (T.shape[1], rows), 0)
    entries = jnp.zeros((T.shape[1], rows), jnp.float32)
    for k in range(2):
        entries = entries + jnp.where(line_of == ids[k : k + 1], coarse[k : k + 1], 0.0)
        entries = entries + jnp.where(line_of == ids[k : k + 1] + count, fine[k : k + 1], 0.0)
    entries = bf16(entries)
    for p in range(2):
        T[2 * own + p] = entries[:, (1 - p) * piece : (2 - p) * piece]

    pl.semaphore_wait(barrier, 4 + jnp.where(inner, 1, 0) + jnp.where(has_next, 1, 0) + jnp.where(has_last, 1, 0))

    def halo_copy(k, device):
        src = (ci_hbm, cx_hbm)[k].at[pl.ds(tokens - halo, halo)]
        return remote(src, (ci, cx)[k].at[pl.ds(0, halo)], halo_s.at[k], halo_r.at[k], device)

    @pl.when(sp < count - 1)
    def _():
        for k in range(2):
            halo_copy(k, (sp + 1, tp)).start()

    eighth = depth // 8
    wide = width // 2
    side = tp % 2
    tile = min(512, depth)
    tiles = depth // tile
    quarter = width // 4
    first = jnp.where(tp // 2 == 0, side, 6 + side)
    lacking = jnp.where(tp // 2 == 0, 6 + side, side)

    def weight_copy(k, leg):
        block = (first, 2 + side, 4 + side, first, 2 + side, 4 + side, lacking, first)[leg]
        at = pl.ds(pl.multiple_of(block * eighth, eighth), eighth)
        buf = (g2, u2)[k]
        src = (g_hbm, u_hbm)[k].at[0, at] if leg < 3 else buf.at[at]
        device = (y_peer, tp) if leg < 3 else (sp, core_peer) if leg < 7 else (sp, x_peer)
        return remote(src, buf.at[at], w_s.at[8 * k + leg], w_r.at[8 * k + leg], device)

    def tile_copy(t, leg):
        row = (x_peer if leg == 3 else tp) * quarter
        cols = pl.ds(t * tile, tile)
        dst = wd.at[pl.ds(pl.multiple_of(width + row, quarter), quarter), cols]
        src = d_hbm.at[0, pl.ds(pl.multiple_of(row, quarter), quarter), cols] if leg == 0 else dst
        device = ((y_peer, tp), (sp, core_peer), (sp, x_peer), (sp, core_peer))[leg]
        return remote(src, dst, w_s.at[16 + 4 * t + leg], w_r.at[16 + 4 * t + leg], device)

    early = range(tiles // 2)
    late = range(tiles // 2, tiles)
    for k in range(2):
        weight_copy(k, 0).start()
    for t in early:
        tile_copy(t, 0).start()
    for k in range(2):
        weight_copy(k, 1).start()
        weight_copy(k, 2).start()
    for t in late:
        tile_copy(t, 0).start()

    part = wide // 2

    def down_copy(leg):
        if leg < 2:
            src = d_hbm.at[0, pl.ds(pl.multiple_of(side * wide + leg * part, part), part)]
            dst = wdo.at[pl.ds(pl.multiple_of(side * wide + leg * part, part), part)]
            device = (line(1), tp)
        else:
            near = wdo.at[pl.ds(pl.multiple_of(side * wide, wide), wide)]
            far = wdo.at[pl.ds(pl.multiple_of(width + side * wide, wide), wide)]
            src, dst = ((near, near), (near, far), (far, far))[leg - 2]
            device = (y_peer, tp) if leg == 3 else (sp, core_peer)
        return remote(src, dst, do_s.at[leg], do_r.at[leg], device)

    @pl.when(outer)
    def _():
        down_copy(0).start()

    def table_copy(slot, across):
        dst = 3 - slot if across else slot
        at = slot + (4 if across else 0)
        return remote(
            T.at[pl.ds(2 * slot, 2)],
            T.at[pl.ds(2 * dst, 2)],
            tab_s.at[at],
            tab_r.at[dst],
            (line(2) if across else line(1 - own), tp),
        )

    def table_came(slot):
        at = T.at[pl.ds(2 * slot, 2)]
        remote(at, at, tab_s.at[0], tab_r.at[slot], (sp, core_peer)).wait_recv()

    table_copy(own, False).start()

    @pl.when(inner)
    def _():
        table_copy(1, True).start()

    P[0] = jnp.zeros(P.shape[1:], P.dtype)
    lane = lax.broadcasted_iota(jnp.int32, (T.shape[1], width), 0)
    for k in range(2):
        picks[k] = jnp.where(lane % count == (sp, y_peer)[k], 1.0, 0.0).astype(picks.dtype)

    for k in range(3):
        loads[k].wait()
    for k in range(4, 9):
        loads[k].start()

    kept = taps.shape[0] - 1
    run = 32

    def conv(start):
        def some(i, c):
            at = pl.multiple_of(start + i * run, run)
            near = f32(ci[pl.ds(at, halo + run)]) * f32(cx[pl.ds(at, halo + run)])
            total = taps[0:1] * near[halo - kept : halo - kept + run]
            for j in range(1, kept + 1):
                total = total + taps[j : j + 1] * near[halo - kept + j : halo - kept + j + run]
            mix[pl.ds(at, run)] = bf16(f32(co[pl.ds(at, run)]) * total)
            return c

        lax.fori_loop(0, piece // run, some, 0)

    loads[3].wait()

    def core_copy(phase, p):
        at = 2 * phase + p
        return remote(part_out.at[at], part_in.at[at], core_s.at[at], core_r.at[at], (sp, core_peer))

    some_rows = piece // 2

    def x_copy(p, k):
        at = pl.ds(k * some_rows, some_rows)
        return remote(
            x_out.at[p, at], x_in.at[p, at], xsw_s.at[2 * p + k], xsw_r.at[2 * p + k], (sp, x_peer)
        )

    def projected(i, carry):
        phase = i // 4
        p = i // 2 % 2
        second = i % 2 == 1
        owner = jnp.where(
            phase == 0, jnp.where(second, x_peer, 3 - tp), jnp.where(second, tp, core_peer)
        )
        start = pl.multiple_of(owner * rows + (1 - p) * piece, piece)

        @pl.when(jnp.logical_and(i == 2, sp == 0))
        def _():
            ci[pl.ds(0, halo)] = jnp.zeros((halo, channels), ci.dtype)
            cx[pl.ds(0, halo)] = jnp.zeros((halo, channels), cx.dtype)

        @pl.when(jnp.logical_and(i == 2, sp > 0))
        def _():
            for k in range(2):
                halo_copy(k, (sp, core_peer)).wait_recv()

        conv(start)

        def some(n, c):
            cols = pl.ds(pl.multiple_of(n * tile, tile), tile)
            got = jnp.dot(mix[pl.ds(start, piece)], ow[:, cols], preferred_element_type=jnp.float32)

            @pl.when(second)
            def _():
                acc[p, :, cols] = got

            @pl.when(jnp.logical_not(second))
            def _():
                part_out[2 * phase + p, :, cols] = bf16(got)

            return c

        lax.fori_loop(0, depth // tile, some, 0)

        @pl.when(jnp.logical_not(second))
        def _():
            core_copy(phase, p).start()

        @pl.when(jnp.logical_and(second, phase == 0))
        def _():
            core_copy(0, p).wait_recv()

            def add(r, c):
                at = pl.ds(pl.multiple_of(r * 16, 16), 16)
                x_out[p, at] = bf16(acc[p, at] + f32(part_in[p, at]))
                return c

            steps = some_rows // 16
            for k in range(2):
                lax.fori_loop(k * steps, (k + 1) * steps, add, 0)
                x_copy(p, k).start()

        return carry

    lax.fori_loop(0, 8, projected, 0)
    loads[4].wait()
    loads[5].wait()

    def rows_copy(item, device, dst, at, k):
        some = pl.ds(k * some_rows, some_rows)
        return remote(X.at[item, some], X.at[dst, some], rows_s.at[at, k], rows_r.at[dst, k], device)

    def normalize(c, k):
        def some(r, carry):
            at = pl.ds(pl.multiple_of(r * 16, 16), 16)
            src = pl.ds(pl.multiple_of((1 - c) * piece + r * 16, 16), 16)
            total = acc[c, at] + f32(part_in[2 + c, at]) + f32(x_in[c, at])
            mixed = jax.nn.sigmoid(f32(mg[src])) * total
            state = bf16(f32(res[src]) + rms_scale(mixed, mgain[...]))
            P[1 + c, at] = state
            X[2 * own + c, at] = bf16(rms_scale(f32(state), egain[...]))
            return carry

        steps = some_rows // 16
        lax.fori_loop(k * steps, (k + 1) * steps, some, 0)

    def send_own(c, k, across):
        item = 2 * own + c
        if across:
            rows_copy(item, (line(2), tp), 4 + c, 8 + c, k).start()
        else:
            rows_copy(item, (line(1 - own), tp), item, item, k).start()

    def weight_on(k, came, *legs):
        weight_copy(k, came).wait_recv()
        for leg in legs:
            weight_copy(k, leg).start()

    def tile_on(t, came, *legs):
        tile_copy(t, came).wait_recv()
        for leg in legs:
            tile_copy(t, leg).start()

    @pl.when(inner)
    def _():
        table_came(0)
        table_copy(0, True).start()
        table_came(2)
        table_copy(2, False).start()

    weight_on(0, 0, 3, 7)
    core_copy(1, 0).wait_recv()
    for k in range(2):
        x_copy(0, k).wait_recv()
        normalize(0, k)
        send_own(0, k, False)

        @pl.when(inner)
        def _():
            send_own(0, k, True)

    @pl.when(inner)
    def _():
        table_came(3)
        table_copy(3, False).start()

    weight_on(1, 0, 3, 7)
    core_copy(1, 1).wait_recv()
    for k in range(2):
        x_copy(1, k).wait_recv()
        normalize(1, k)

        @pl.when(outer)
        def _():
            send_own(1, k, False)

    @pl.when(outer)
    def _():
        down_copy(1).start()

    for t in early:
        tile_on(t, 0, 1, 2)
    for k in range(6, 9):
        loads[k].wait()

    @pl.when(outer)
    def _():
        for slot in range(1, 4):
            table_came(slot)

    def hidden(item, k):
        gate, up = ((g1, u1), (g2, u2))[k]
        x = X[item]
        first = jnp.dot(x, gate[...], preferred_element_type=jnp.float32)
        second = jnp.dot(x, up[...], preferred_element_type=jnp.float32)
        share = lax.dot_general(
            T[item], picks[k], (((0,), (0,)), ((), ())), preferred_element_type=jnp.float32
        )
        H[item, :, k * width : (k + 1) * width] = bf16(jax.nn.silu(first) * second * share)

    def sum_copy(item, m):
        slot = item // 2
        c = item % 2
        to = jnp.where(outer, 1, jnp.where(slot == 0, 0, 2))
        dst = jnp.where(outer, jnp.where(slot == 2, 9 + c, 3 + c), jnp.where(slot == 2, 7 + c, 5 + c))
        cols = pl.ds(pl.multiple_of(m * tile, tile), tile)
        return remote(S.at[item, :, cols], P.at[dst, :, cols], sum_s.at[item, m], sum_r.at[dst, m], (line(to), tp))

    def held(item):
        return jnp.where(item == 5, 2, item - 2)

    def hidden_copy(item):
        at = held(item)
        return remote(H.at[item], HR.at[at], hid_s.at[at], hid_r.at[at], (line(1), tp))

    def out_copy(c, m):
        cols = pl.ds(pl.multiple_of(m * tile, tile), tile)
        return pltpu.make_async_copy(
            S.at[2 * own + c, :, cols],
            out_hbm.at[pl.ds(pl.multiple_of((1 - c) * piece, piece), piece), cols],
            out_sem.at[c, m],
        )

    def came(at, m):
        cols = pl.ds(pl.multiple_of(m * tile, tile), tile)
        ref = P.at[at, :, cols]
        remote(ref, ref, sum_s.at[0, m], sum_r.at[at, m], (sp, core_peer)).wait_recv()

    def step(n, carry):
        code = 0
        for i, (a, b) in enumerate(zip(OUTER_STEPS, INNER_STEPS)):
            code = jnp.where(n == i, jnp.where(outer, a, b), code)
        item = code % 8

        def has(flag):
            return code // flag % 2 == 1

        slot = item // 2
        c = item % 2

        @pl.when(has(ARRIVE))
        def _():
            forwards = has(FORWARD)
            across = slot == 0
            for k in range(2):
                rows_copy(item, (sp, core_peer), item, item, k).wait_recv()

                @pl.when(forwards)
                def _():
                    rows_copy(
                        item,
                        (line(jnp.where(across, 2, 0)), tp),
                        jnp.where(across, 6 + c, item),
                        jnp.where(across, 10 + c, item),
                        k,
                    ).start()

        def specials():
            @pl.when(has(DOWN_PASS))
            def _():
                for t in early:
                    tile_on(t, 2, 3)

            @pl.when(has(SEND_ACROSS))
            def _():
                for k in range(2):
                    send_own(1, k, True)

            @pl.when(has(FIRST_PASS))
            def _():
                weight_on(0, 7, 6)
                weight_on(1, 7, 6)

            for k in range(2):

                @pl.when(has((GATE_PASS, UP_PASS)[k]))
                def _():
                    weight_on(k, 1, 4)
                    weight_on(k, 2, 5)

            @pl.when(has(DOWN_READY))
            def _():
                for t in early:
                    tile_copy(t, 1).wait_recv()
                    tile_copy(t, 3).wait_recv()

            @pl.when(has(FAR_PASS))
            def _():
                down_copy(0).wait_recv()
                down_copy(1).wait_recv()
                down_copy(2).start()
                down_copy(3).start()

            @pl.when(has(HIDDEN_READY))
            def _():
                for k in range(2):
                    for leg in range(3, 7):
                        weight_copy(k, leg).wait_recv()

            @pl.when(has(SEND_OUTWARD))
            def _():
                for k in range(2):
                    send_own(1, k, False)

            @pl.when(has(LATE_RELAY))
            def _():
                for t in late:
                    tile_on(t, 0, 1, 2)

            @pl.when(has(LATE_PASS))
            def _():
                for t in late:
                    tile_on(t, 2, 3)

            @pl.when(has(LATE_READY))
            def _():
                for t in late:
                    tile_copy(t, 1).wait_recv()
                    tile_copy(t, 3).wait_recv()

            @pl.when(has(FAR_READY))
            def _():
                down_copy(3).wait_recv()
                down_copy(4).start()
                down_copy(2).wait_recv()
                down_copy(4).wait_recv()

        pl.when(code >= SPECIAL)(specials)

        @pl.when(has(OWN))
        def _():
            hidden(item, 0)

        @pl.when(has(OTHER))
        def _():
            hidden(item, 1)

        middle = jnp.logical_or(slot == 1, item == 5)
        begins = code // LATER % 2 == 0

        short = jnp.logical_and(outer, middle)

        @pl.when(jnp.logical_and(has(OUT), short))
        def _():
            hidden_copy(item).start()

        @pl.when(jnp.logical_and(has(OUT), jnp.logical_not(short)))
        def _():
            inner_at = jnp.where(slot == 1, 7 + c, jnp.where(slot == 2, jnp.where(c == 0, 9, 0), 3 + c))
            a = jnp.where(slot == 0, 5 + c, jnp.where(outer, 0, inner_at))
            d = jnp.where(slot == own, 1 + c, 0)

            @pl.when(jnp.logical_and(middle, begins))
            def _():
                ref = HR.at[held(item)]
                remote(ref, ref, hid_s.at[0], hid_r.at[held(item)], (sp, core_peer)).wait_recv()

            def some(m, carry):
                cols = pl.ds(pl.multiple_of(m * tile, tile), tile)

                @pl.when(a > 0)
                def _():
                    came(a, m)

                got = jnp.dot(H[item], wd[:, cols], preferred_element_type=jnp.float32)
                got = got + f32(P[d, :, cols]) + f32(P[a, :, cols])

                @pl.when(middle)
                def _():
                    more = jnp.dot(HR[held(item)], wdo[:, cols], preferred_element_type=jnp.float32)
                    S[item, :, cols] = bf16(got + more)

                @pl.when(jnp.logical_not(middle))
                def _():
                    S[item, :, cols] = bf16(got)

                @pl.when(slot == own)
                def _():
                    out_copy(c, m).start()

                @pl.when(slot != own)
                def _():
                    sum_copy(item, m).start()

                return carry

            begin = jnp.where(begins, 0, tiles // 2)
            lax.fori_loop(begin, begin + tiles // 2, some, 0)

        return carry

    lax.fori_loop(0, len(OUTER_STEPS), step, 0)

    for c in range(2):
        for m in range(depth // tile):
            out_copy(c, m).wait()
        core_copy(0, c).wait_send()
        core_copy(1, c).wait_send()
        x_copy(c, 0).wait_send()
        x_copy(c, 1).wait_send()

    @pl.when(sp < count - 1)
    def _():
        for k in range(2):
            halo_copy(k, (sp + 1, tp)).wait_send()

    for k in range(2):
        for leg in range(8):
            weight_copy(k, leg).wait_send()
    for t in range(tiles):
        for leg in range(4):
            tile_copy(t, leg).wait_send()
    table_copy(own, False).wait_send()

    @pl.when(inner)
    def _():
        table_copy(1, True).wait_send()
        table_copy(0, True).wait_send()
        table_copy(2, False).wait_send()
        table_copy(3, False).wait_send()


    def gone(at):
        for k in range(2):
            rows_copy(at % 8, (sp, core_peer), at % 8, at, k).wait_send()

    def summed(item):
        for m in range(depth // tile):
            sum_copy(item, m).wait_send()

    for c in range(2):
        gone(2 * own + c)

    @pl.when(outer)
    def _():
        summed(4)
        hidden_copy(5).wait_send()
        for c in range(2):
            down_copy(c).wait_send()
            summed(6 + c)
            hidden_copy(2 + c).wait_send()

    @pl.when(inner)
    def _():
        for leg in range(2, 5):
            down_copy(leg).wait_send()
        for c in range(2):
            for at in (4 + c, 6 + c, 8 + c, 10 + c):
                gone(at)
            for slot in (0, 2, 3):
                summed(2 * slot + c)


def mega(
    conv_outer, conv_inner, conv_input, conv_taps, out_weight, mix_gate, residual, mix_gain, expert_gain,
    expert_ids, group_share, pair_scores, gate_experts, up_experts, down_experts,
):
    count = lax.axis_size("sp")
    rows, depth = residual.shape
    tokens, channels = conv_inner.shape
    width = gate_experts.shape[2]
    piece = rows // 2
    halo = 16
    tiles = depth // min(512, depth)
    half_type, full = jnp.bfloat16, jnp.float32
    hbm = pl.BlockSpec(memory_space=pl.ANY)
    vmem = pl.BlockSpec(memory_space=pltpu.VMEM)
    dma = pltpu.SemaphoreType.DMA
    return pl.pallas_call(
        mega_kernel,
        out_shape=jax.ShapeDtypeStruct((rows, depth), half_type),
        in_specs=[hbm, hbm, hbm, vmem, hbm, hbm, hbm, vmem, vmem, vmem, vmem, vmem, hbm, hbm, hbm],
        out_specs=hbm,
        scratch_shapes=[
            pltpu.VMEM((halo + tokens, channels), half_type),
            pltpu.VMEM((halo + tokens, channels), half_type),
            pltpu.VMEM((tokens, channels), half_type),
            pltpu.VMEM((channels, depth), half_type),
            pltpu.VMEM((rows, depth), half_type),
            pltpu.VMEM((rows, depth), half_type),
            pltpu.VMEM((tokens, channels), half_type),
            pltpu.VMEM((2, piece, depth), full),
            pltpu.VMEM((4, piece, depth), half_type),
            pltpu.VMEM((4, piece, depth), half_type),
            pltpu.VMEM((2, piece, depth), half_type),
            pltpu.VMEM((2, piece, depth), half_type),
            pltpu.VMEM((8, piece, depth), half_type),
            pltpu.VMEM((8, 2 * count, piece), half_type),
            pltpu.VMEM((11, piece, depth), half_type),
            pltpu.VMEM((8, piece, depth), half_type),
            pltpu.VMEM((8, piece, 2 * width), half_type),
            pltpu.VMEM((3, piece, 2 * width), half_type),
            pltpu.VMEM((depth, width), half_type),
            pltpu.VMEM((depth, width), half_type),
            pltpu.VMEM((depth, width), half_type),
            pltpu.VMEM((depth, width), half_type),
            pltpu.VMEM((2 * width, depth), half_type),
            pltpu.VMEM((2 * width, depth), half_type),
            pltpu.VMEM((2, 2 * count, width), half_type),
            dma((9,)),
            dma((2,)),
            dma((2,)),
            dma((8,)),
            dma((4,)),
            dma((4,)),
            dma((4,)),
            dma((4,)),
            dma((4,)),
            dma((16 + 4 * tiles,)),
            dma((16 + 4 * tiles,)),
            dma((16, 2)),
            dma((8, 2)),
            dma((8, tiles)),
            dma((11, tiles)),
            dma((3,)),
            dma((3,)),
            dma((5,)),
            dma((5,)),
            dma((2, tiles)),
        ],
        compiler_params=pltpu.CompilerParams(
            collective_id=0, has_side_effects=True, vmem_limit_bytes=60 * 1024 * 1024
        ),
        name="layer",
    )(
        conv_outer, conv_inner, conv_input, conv_taps, out_weight, mix_gate, residual,
        mix_gain[None, :], expert_gain[None, :], expert_ids.T, pair_scores.T, group_share[None, :], gate_experts, up_experts, down_experts,
    )


def solution(mesh):
    placed = (
        P("sp", "tp"),
        P("sp", "tp"),
        P("sp", "tp"),
        P(None, "tp"),
        P("tp", None),
        P(("sp", "tp"), None),
        P(("sp", "tp"), None),
        P(),
        P(),
        P(("sp", "tp"), None),
        P(("sp", "tp")),
        P(("sp", "tp"), None),
        P("sp", None, None),
        P("sp", None, None),
        P("sp", None, None),
    )

    square = mesh.shape["tp"] == 4 and mesh.shape["sp"] == 8

    def layer(*arrays):
        return (mega if square else per_device)(*arrays)

    return jax.shard_map(
        layer, mesh=mesh, in_specs=placed, out_specs=P(("sp", "tp"), None), check_vma=False
    )
```

```python
import jax
import jax.numpy as jnp
from jax import lax
from jax.experimental import pallas as pl
from jax.experimental.pallas import tpu as pltpu
from jax.sharding import PartitionSpec as P

epsilon = 1e-06


def f32(value):
    return value.astype(jnp.float32)


def bf16(value):
    return value.astype(jnp.bfloat16)


def rms_scale(values, gain):
    return values * lax.rsqrt(jnp.mean(values * values, axis=-1, keepdims=True) + epsilon) * gain


def shifted(value, steps, senders):
    return lax.ppermute(value, "sp", [(s, s + steps) for s in senders])


def swapped(value, axis, bit):
    return lax.ppermute(value, axis, [(s, s ^ bit) for s in range(lax.axis_size(axis))])


def mixer_rows(conv_outer, conv_inner, conv_input, conv_taps):
    kept = conv_taps.shape[0] - 1
    inner = f32(conv_inner) * f32(conv_input)
    tail = f32(conv_inner[-kept:]) * f32(conv_input[-kept:])
    earlier = shifted(tail, 1, range(lax.axis_size("sp") - 1))
    length = conv_inner.shape[0]
    inner = jnp.concatenate([earlier, inner], 0)
    conv = conv_taps[0] * inner[0:length]
    for offset in range(1, kept + 1):
        conv = conv + conv_taps[offset] * inner[offset : offset + length]
    return bf16(f32(conv_outer) * conv)


def project(mixed_rows, out_weight, own_rows):
    parts = lax.axis_size("tp")
    me = lax.axis_index("tp")
    blocks = mixed_rows.reshape(parts, own_rows, -1)

    def partial(owner):
        rows = lax.dynamic_index_in_dim(blocks, owner, 0, keepdims=False)
        return jnp.dot(rows, out_weight, preferred_element_type=jnp.float32)

    def total(owner_bits, bit):
        if bit == 1:
            return partial(me ^ owner_bits)
        half = bit // 2
        sent = bf16(total(owner_bits | half, half))
        given = swapped(sent, "tp", half)
        return total(owner_bits, half) + f32(given)

    return total(0, parts)


def routing_table(expert_ids, group_share, pair_scores, own_rows, count):
    weights = group_share[:, None] * jax.nn.softmax(pair_scores, axis=-1)
    lanes = -(-2 * count // 128) * 128
    column = jnp.arange(lanes, dtype=jnp.int32)[None, :]
    coarse = lax.reduce_precision(weights, 8, 7)
    fine = weights - coarse
    table = jnp.zeros((own_rows, lanes), jnp.float32)
    for slot in range(expert_ids.shape[1]):
        at = expert_ids[:, slot : slot + 1]
        table = table + jnp.where(column == at, coarse[:, slot : slot + 1], 0.0)
        table = table + jnp.where(column == at + count, fine[:, slot : slot + 1], 0.0)
    return bf16(table)


def per_device(
    conv_outer,
    conv_inner,
    conv_input,
    conv_taps,
    out_weight,
    mix_gate,
    residual,
    mix_gain,
    expert_gain,
    expert_ids,
    group_share,
    pair_scores,
    gate_experts,
    up_experts,
    down_experts,
):
    count = lax.axis_size("sp")
    me = lax.axis_index("sp")
    own_rows = residual.shape[0]
    groups = count // 2
    place = me // 2
    side = lax.axis_index("tp") % 2
    half = gate_experts.shape[2] // 2

    def fetched(weight, axis):
        piece = lax.dynamic_slice_in_dim(weight[0], side * half, half, axis)
        first = swapped(piece, "sp", 1)
        second = swapped(first, "tp", 1)
        return jnp.concatenate([weight[0], first, second], axis)

    gate_both = fetched(gate_experts, 1)
    up_both = fetched(up_experts, 1)
    down_both = fetched(down_experts, 0)

    lanes = -(-2 * count // 128) * 128
    table = routing_table(expert_ids, group_share, pair_scores, own_rows, count)

    def spread(own):
        below, above = {0: own}, {0: own}
        for step in range(1, groups):
            below[step] = shifted(below[step - 1], 2, range(2 * (step - 1), count - 2))
            above[step] = shifted(above[step - 1], -2, range(2, count - 2 * (step - 1)))
        order = {0: own}
        for near in range(1, (groups - 1) // 2 + 1):
            far = groups - near
            early = jnp.where(place < near, above[near], below[near])
            _, over, under, away = lax.optimization_barrier(
                (early, above[near], below[far], above[far])
            )
            order[near] = early
            late = jnp.where(place < far, over, under)
            order[far] = jnp.where(place < near, away, late)
        if groups % 2 == 0:
            mid = groups // 2
            order[mid] = jnp.where(place < mid, above[mid], below[mid])
        return order

    mixed_rows = mixer_rows(conv_outer, conv_inner, conv_input, conv_taps)
    projected = project(mixed_rows, out_weight, own_rows)
    mixed = jax.nn.sigmoid(f32(mix_gate)) * projected
    hidden_state = bf16(f32(residual) + rms_scale(mixed, mix_gain))
    normed = bf16(rms_scale(f32(hidden_state), expert_gain))

    blocks = spread(jnp.concatenate([normed, table], 1))
    depth = normed.shape[1]

    def served(block):
        rows = block[:, :depth]
        chosen = jnp.arange(lanes, dtype=jnp.int32)[:, None] % count
        picks = bf16(chosen == jnp.stack([me, me ^ 1])[None, :])
        picks = jnp.where(jnp.arange(lanes)[:, None] < 2 * count, picks, 0)
        shares = jnp.dot(block[:, depth:], picks, preferred_element_type=jnp.float32)
        wide = 2 * half
        first = jnp.dot(rows, gate_both, preferred_element_type=jnp.float32)
        second = jnp.dot(rows, up_both, preferred_element_type=jnp.float32)
        mine = jnp.arange(2 * wide)[None, :] < wide
        share = jnp.where(mine, shares[:, :1], shares[:, 1:])
        hidden = lax.optimization_barrier(bf16(jax.nn.silu(first) * second * share))
        return lax.optimization_barrier(
            jnp.dot(hidden, down_both, preferred_element_type=jnp.float32)
        )

    results = {number: served(block) for number, block in blocks.items()}

    def for_upper(step):
        gone = groups - step
        if step == gone or step < gone:
            return results[gone]
        return jnp.where(place < gone, results[gone], results[step])

    down = up = None
    for step in range(1, groups):
        gone = groups - step
        lower, upper = results[gone], for_upper(step)
        if down is not None:
            lower, upper = lower + f32(down), upper + f32(up)
        down = shifted(bf16(lower), -2, range(2 * gone, count))
        up = shifted(bf16(upper), 2, range(0, count - 2 * gone))
    result = f32(hidden_state) + results[0]
    if down is not None:
        result = result + f32(down) + f32(up)
    return bf16(result)


MESH_ID = pl.DeviceIdType.MESH
OWN, OTHER, OUT, ARRIVE, FORWARD, LATER = (8 << i for i in range(6))
SPECIAL = 8 << 6
(DOWN_PASS, SEND_ACROSS, FIRST_PASS, GATE_PASS, UP_PASS, DOWN_READY, FAR_PASS, HIDDEN_READY, SEND_OUTWARD, LATE_RELAY, LATE_PASS, LATE_READY, FAR_READY,) = (SPECIAL << i for i in range(13))

OUTER_STEPS = (
    0 | FIRST_PASS,
    4 | OWN | ARRIVE,
    0 | OWN,
    0 | GATE_PASS | UP_PASS,
    4 | OTHER | OUT | DOWN_PASS | DOWN_READY | HIDDEN_READY,
    6 | OWN | OTHER | ARRIVE,
    6 | OUT | LATE_RELAY,
    7 | OWN | OTHER | OUT | ARRIVE,
    2 | OWN | ARRIVE,
    7 | OUT | LATER | LATE_PASS | LATE_READY,
    1 | OWN,
    2 | OTHER,
    6 | OUT | LATER,
    0 | OTHER,
    4 | OUT | LATER,
    5 | OWN | OTHER | OUT | ARRIVE,
    1 | OTHER | OUT,
    3 | OWN | ARRIVE,
    2 | OUT,
    0 | OUT,
    3 | OTHER | OUT,
    1 | OUT | LATER,
    0 | OUT | LATER,
    0,
    0,
    0,
    0,
    0,
    0,
    0,
    0,
    0,
    0,
    0,
    0,
)
INNER_STEPS = (
    4 | OWN | ARRIVE | FORWARD,
    0 | OWN | ARRIVE | FORWARD,
    1 | OWN | ARRIVE | FORWARD,
    6 | OWN | ARRIVE | FORWARD,
    0 | SEND_ACROSS | FIRST_PASS,
    0 | DOWN_PASS | GATE_PASS,
    7 | OWN | ARRIVE | FORWARD,
    3 | OWN | UP_PASS,
    0 | FAR_PASS | SEND_OUTWARD | LATE_RELAY,
    4 | OTHER | HIDDEN_READY,
    7 | OTHER | DOWN_READY,
    6 | OTHER,
    4 | OUT,
    0 | OTHER,
    5 | OWN | ARRIVE | FORWARD,
    6 | OUT,
    1 | OTHER | LATE_PASS,
    7 | OUT,
    5 | OTHER,
    2 | OWN,
    7 | OUT | LATER | LATE_READY,
    1 | OUT,
    0 | OUT,
    6 | OUT | LATER,
    2 | OTHER,
    3 | OTHER,
    4 | OUT | LATER,
    1 | OUT | LATER,
    0 | OUT | LATER,
    5 | OUT | FAR_READY,
    5 | OUT | LATER,
    2 | OUT,
    2 | OUT | LATER,
    3 | OUT,
    3 | OUT | LATER,
)


def mega_kernel(
    co_hbm, ci_hbm, cx_hbm, taps, ow_hbm, mg_hbm, res_hbm, mgain, egain, ids, scores, group,
    g_hbm, u_hbm, d_hbm, out_hbm,
    ci, cx, co, ow, mg, res, mix, acc, part_out, part_in, x_out, x_in,
    X, T, P, S, H, HR, stage, g1, u1, g2, u2, wd, wdo, picks,
    load_sem, halo_s, halo_r, tab_s, tab_r, core_s, core_r, xsw_s, xsw_r,
    w_s, w_r, rows_s, rows_r, sum_s, sum_r, hid_s, hid_r, do_s, do_r, out_sem,
):
    sp = lax.axis_index("sp")
    tp = lax.axis_index("tp")
    z = sp // 2
    y = sp % 2
    half = z // 2
    outer = z * (3 - z) == 0
    inner = jnp.logical_not(outer)
    own = jnp.where(outer, 0, 1)
    core_peer = tp + 1 - 2 * (tp % 2)
    x_peer = (tp + 2) % 4
    y_peer = sp + 1 - 2 * y
    rows, depth = res.shape
    piece = rows // 2
    width = g1.shape[1]
    count = T.shape[1] // 2
    channels = ow.shape[0]
    halo = ci.shape[0] - co.shape[0]

    def line(slot):
        where = jnp.where(slot == 0, 3 * half, jnp.where(slot == 1, 1 + half, jnp.where(slot == 2, 2 - half, 3 - 3 * half)))
        return 2 * where + y

    def remote(src, dst, s, r, device):
        return pltpu.make_async_remote_copy(
            src_ref=src, dst_ref=dst, send_sem=s, recv_sem=r, device_id=device, device_id_type=MESH_ID
        )

    barrier = pltpu.get_barrier_semaphore()

    def greet(device):
        pl.semaphore_signal(barrier, inc=1, device_id=device, device_id_type=MESH_ID)

    greet((sp, core_peer))
    greet((sp, x_peer))
    greet((y_peer, tp))
    greet((line(1 - own), tp))

    @pl.when(inner)
    def _():
        greet((line(2), tp))

    has_next = jnp.logical_and(y == 1, sp < count - 1)
    has_last = jnp.logical_and(y == 0, sp > 0)

    @pl.when(has_next)
    def _():
        greet((sp + 1, tp))

    @pl.when(has_last)
    def _():
        greet((sp - 1, tp))

    tokens = co.shape[0]
    loads = [
        pltpu.make_async_copy(ci_hbm, ci.at[pl.ds(halo, tokens)], load_sem.at[0]),
        pltpu.make_async_copy(cx_hbm, cx.at[pl.ds(halo, tokens)], load_sem.at[1]),
        pltpu.make_async_copy(co_hbm, co, load_sem.at[2]),
        pltpu.make_async_copy(ow_hbm, ow, load_sem.at[3]),
        pltpu.make_async_copy(mg_hbm, mg, load_sem.at[4]),
        pltpu.make_async_copy(res_hbm, res, load_sem.at[5]),
        pltpu.make_async_copy(g_hbm.at[0], g1, load_sem.at[6]),
        pltpu.make_async_copy(u_hbm.at[0], u1, load_sem.at[7]),
        pltpu.make_async_copy(d_hbm.at[0], wd.at[pl.ds(0, width)], load_sem.at[8]),
    ]
    for k in (0, 1, 3, 2):
        loads[k].start()

    raw = scores[...]
    top = jnp.maximum(raw[0:1], raw[1:2])
    up = jnp.exp(raw - top)
    weights = group[...] * (up / (up[0:1] + up[1:2]))
    coarse = f32(bf16(weights))
    fine = weights - coarse
    line_of = lax.broadcasted_iota(jnp.int32, (T.shape[1], rows), 0)
    entries = jnp.zeros((T.shape[1], rows), jnp.float32)
    for k in range(2):
        entries = entries + jnp.where(line_of == ids[k : k + 1], coarse[k : k + 1], 0.0)
        entries = entries + jnp.where(line_of == ids[k : k + 1] + count, fine[k : k + 1], 0.0)
    entries = bf16(entries)
    for p in range(2):
        T[2 * own + p] = entries[:, (1 - p) * piece : (2 - p) * piece]

    pl.semaphore_wait(barrier, 4 + jnp.where(inner, 1, 0) + jnp.where(has_next, 1, 0) + jnp.where(has_last, 1, 0))

    def halo_copy(k, device):
        src = (ci_hbm, cx_hbm)[k].at[pl.ds(tokens - halo, halo)]
        return remote(src, (ci, cx)[k].at[pl.ds(0, halo)], halo_s.at[k], halo_r.at[k], device)

    @pl.when(sp < count - 1)
    def _():
        for k in range(2):
            halo_copy(k, (sp + 1, tp)).start()

    eighth = depth // 8
    wide = width // 2
    side = tp % 2
    tile = min(512, depth)
    tiles = depth // tile
    quarter = width // 4
    first = jnp.where(tp // 2 == 0, side, 6 + side)
    lacking = jnp.where(tp // 2 == 0, 6 + side, side)

    def weight_copy(k, leg):
        block = (first, 2 + side, 4 + side, first, 2 + side, 4 + side, lacking, first)[leg]
        at = pl.ds(pl.multiple_of(block * eighth, eighth), eighth)
        buf = (g2, u2)[k]
        src = (g_hbm, u_hbm)[k].at[0, at] if leg < 3 else buf.at[at]
        device = (y_peer, tp) if leg < 3 else (sp, core_peer) if leg < 7 else (sp, x_peer)
        return remote(src, buf.at[at], w_s.at[8 * k + leg], w_r.at[8 * k + leg], device)

    def tile_copy(t, leg):
        row = (x_peer if leg == 3 else tp) * quarter
        cols = pl.ds(t * tile, tile)
        dst = wd.at[pl.ds(pl.multiple_of(width + row, quarter), quarter), cols]
        src = d_hbm.at[0, pl.ds(pl.multiple_of(row, quarter), quarter), cols] if leg == 0 else dst
        device = ((y_peer, tp), (sp, core_peer), (sp, x_peer), (sp, core_peer))[leg]
        return remote(src, dst, w_s.at[16 + 4 * t + leg], w_r.at[16 + 4 * t + leg], device)

    early = range(tiles // 2)
    late = range(tiles // 2, tiles)
    for k in range(2):
        weight_copy(k, 0).start()
    for t in early:
        tile_copy(t, 0).start()
    for k in range(2):
        weight_copy(k, 1).start()
        weight_copy(k, 2).start()
    for t in late:
        tile_copy(t, 0).start()

    part = wide // 2

    def down_copy(leg):
        if leg < 2:
            src = d_hbm.at[0, pl.ds(pl.multiple_of(side * wide + leg * part, part), part)]
            dst = wdo.at[pl.ds(pl.multiple_of(side * wide + leg * part, part), part)]
            device = (line(1), tp)
        else:
            near = wdo.at[pl.ds(pl.multiple_of(side * wide, wide), wide)]
            far = wdo.at[pl.ds(pl.multiple_of(width + side * wide, wide), wide)]
            src, dst = ((near, near), (near, far), (far, far))[leg - 2]
            device = (y_peer, tp) if leg == 3 else (sp, core_peer)
        return remote(src, dst, do_s.at[leg], do_r.at[leg], device)

    @pl.when(outer)
    def _():
        down_copy(0).start()

    def table_copy(slot, across):
        dst = 3 - slot if across else slot
        at = slot + (4 if across else 0)
        return remote(
            T.at[pl.ds(2 * slot, 2)],
            T.at[pl.ds(2 * dst, 2)],
            tab_s.at[at],
            tab_r.at[dst],
            (line(2) if across else line(1 - own), tp),
        )

    def table_came(slot):
        at = T.at[pl.ds(2 * slot, 2)]
        remote(at, at, tab_s.at[0], tab_r.at[slot], (sp, core_peer)).wait_recv()

    table_copy(own, False).start()

    @pl.when(inner)
    def _():
        table_copy(1, True).start()

    P[0] = jnp.zeros(P.shape[1:], P.dtype)
    lane = lax.broadcasted_iota(jnp.int32, (T.shape[1], width), 0)
    for k in range(2):
        picks[k] = jnp.where(lane % count == (sp, y_peer)[k], 1.0, 0.0).astype(picks.dtype)

    for k in range(3):
        loads[k].wait()
    for k in range(4, 9):
        loads[k].start()

    kept = taps.shape[0] - 1
    run = 32

    def conv(start):
        def some(i, c):
            at = pl.multiple_of(start + i * run, run)
            near = f32(ci[pl.ds(at, halo + run)]) * f32(cx[pl.ds(at, halo + run)])
            total = taps[0:1] * near[halo - kept : halo - kept + run]
            for j in range(1, kept + 1):
                total = total + taps[j : j + 1] * near[halo - kept + j : halo - kept + j + run]
            mix[pl.ds(at, run)] = bf16(f32(co[pl.ds(at, run)]) * total)
            return c

        lax.fori_loop(0, piece // run, some, 0)

    loads[3].wait()

    def core_copy(phase, p):
        at = 2 * phase + p
        return remote(part_out.at[at], part_in.at[at], core_s.at[at], core_r.at[at], (sp, core_peer))

    some_rows = piece // 2

    def x_copy(p, k):
        at = pl.ds(k * some_rows, some_rows)
        return remote(
            x_out.at[p, at], x_in.at[p, at], xsw_s.at[2 * p + k], xsw_r.at[2 * p + k], (sp, x_peer)
        )

    def projected(i, carry):
        phase = i // 4
        p = i // 2 % 2
        second = i % 2 == 1
        owner = jnp.where(
            phase == 0, jnp.where(second, x_peer, 3 - tp), jnp.where(second, tp, core_peer)
        )
        start = pl.multiple_of(owner * rows + (1 - p) * piece, piece)

        @pl.when(jnp.logical_and(i == 2, sp == 0))
        def _():
            ci[pl.ds(0, halo)] = jnp.zeros((halo, channels), ci.dtype)
            cx[pl.ds(0, halo)] = jnp.zeros((halo, channels), cx.dtype)

        @pl.when(jnp.logical_and(i == 2, sp > 0))
        def _():
            for k in range(2):
                halo_copy(k, (sp, core_peer)).wait_recv()

        conv(start)

        def some(n, c):
            cols = pl.ds(pl.multiple_of(n * tile, tile), tile)
            got = jnp.dot(mix[pl.ds(start, piece)], ow[:, cols], preferred_element_type=jnp.float32)

            @pl.when(second)
            def _():
                acc[p, :, cols] = got

            @pl.when(jnp.logical_not(second))
            def _():
                part_out[2 * phase + p, :, cols] = bf16(got)

            return c

        lax.fori_loop(0, depth // tile, some, 0)

        @pl.when(jnp.logical_not(second))
        def _():
            core_copy(phase, p).start()

        @pl.when(jnp.logical_and(second, phase == 0))
        def _():
            core_copy(0, p).wait_recv()

            def add(r, c):
                at = pl.ds(pl.multiple_of(r * 16, 16), 16)
                x_out[p, at] = bf16(acc[p, at] + f32(part_in[p, at]))
                return c

            steps = some_rows // 16
            for k in range(2):
                lax.fori_loop(k * steps, (k + 1) * steps, add, 0)
                x_copy(p, k).start()

        return carry

    lax.fori_loop(0, 8, projected, 0)
    loads[4].wait()
    loads[5].wait()

    def rows_copy(item, device, dst, at, k):
        some = pl.ds(k * some_rows, some_rows)
        return remote(X.at[item, some], X.at[dst, some], rows_s.at[at, k], rows_r.at[dst, k], device)

    def normalize(c, k):
        def some(r, carry):
            at = pl.ds(pl.multiple_of(r * 16, 16), 16)
            src = pl.ds(pl.multiple_of((1 - c) * piece + r * 16, 16), 16)
            total = acc[c, at] + f32(part_in[2 + c, at]) + f32(x_in[c, at])
            mixed = jax.nn.sigmoid(f32(mg[src])) * total
            state = bf16(f32(res[src]) + rms_scale(mixed, mgain[...]))
            P[1 + c, at] = state
            X[2 * own + c, at] = bf16(rms_scale(f32(state), egain[...]))
            return carry

        steps = some_rows // 16
        lax.fori_loop(k * steps, (k + 1) * steps, some, 0)

    def send_own(c, k, across):
        item = 2 * own + c
        if across:
            rows_copy(item, (line(2), tp), 4 + c, 8 + c, k).start()
        else:
            rows_copy(item, (line(1 - own), tp), item, item, k).start()

    def weight_on(k, came, *legs):
        weight_copy(k, came).wait_recv()
        for leg in legs:
            weight_copy(k, leg).start()

    def tile_on(t, came, *legs):
        tile_copy(t, came).wait_recv()
        for leg in legs:
            tile_copy(t, leg).start()

    @pl.when(inner)
    def _():
        table_came(0)
        table_copy(0, True).start()
        table_came(2)
        table_copy(2, False).start()

    weight_on(0, 0, 3, 7)
    core_copy(1, 0).wait_recv()
    for k in range(2):
        x_copy(0, k).wait_recv()
        normalize(0, k)
        send_own(0, k, False)

        @pl.when(inner)
        def _():
            send_own(0, k, True)

    @pl.when(inner)
    def _():
        table_came(3)
        table_copy(3, False).start()

    weight_on(1, 0, 3, 7)
    core_copy(1, 1).wait_recv()
    for k in range(2):
        x_copy(1, k).wait_recv()
        normalize(1, k)

        @pl.when(outer)
        def _():
            send_own(1, k, False)

    @pl.when(outer)
    def _():
        down_copy(1).start()

    for t in early:
        tile_on(t, 0, 1, 2)
    for k in range(6, 9):
        loads[k].wait()

    @pl.when(outer)
    def _():
        for slot in range(1, 4):
            table_came(slot)

    def hidden(item, k):
        gate, up = ((g1, u1), (g2, u2))[k]
        x = X[item]
        first = jnp.dot(x, gate[...], preferred_element_type=jnp.float32)
        second = jnp.dot(x, up[...], preferred_element_type=jnp.float32)
        share = lax.dot_general(
            T[item], picks[k], (((0,), (0,)), ((), ())), preferred_element_type=jnp.float32
        )
        H[item, :, k * width : (k + 1) * width] = bf16(jax.nn.silu(first) * second * share)

    def sum_copy(item, m):
        slot = item // 2
        c = item % 2
        to = jnp.where(outer, 1, jnp.where(slot == 0, 0, 2))
        dst = jnp.where(outer, jnp.where(slot == 2, 9 + c, 3 + c), jnp.where(slot == 2, 7 + c, 5 + c))
        cols = pl.ds(pl.multiple_of(m * tile, tile), tile)
        return remote(S.at[item, :, cols], P.at[dst, :, cols], sum_s.at[item, m], sum_r.at[dst, m], (line(to), tp))

    def held(item):
        return jnp.where(item == 5, 2, item - 2)

    def hidden_copy(item):
        at = held(item)
        return remote(H.at[item], HR.at[at], hid_s.at[at], hid_r.at[at], (line(1), tp))

    def out_copy(c, m):
        cols = pl.ds(pl.multiple_of(m * tile, tile), tile)
        return pltpu.make_async_copy(
            S.at[2 * own + c, :, cols],
            out_hbm.at[pl.ds(pl.multiple_of((1 - c) * piece, piece), piece), cols],
            out_sem.at[c, m],
        )

    def came(at, m):
        cols = pl.ds(pl.multiple_of(m * tile, tile), tile)
        ref = P.at[at, :, cols]
        remote(ref, ref, sum_s.at[0, m], sum_r.at[at, m], (sp, core_peer)).wait_recv()

    def step(n, carry):
        code = 0
        for i, (a, b) in enumerate(zip(OUTER_STEPS, INNER_STEPS)):
            code = jnp.where(n == i, jnp.where(outer, a, b), code)
        item = code % 8

        def has(flag):
            return code // flag % 2 == 1

        slot = item // 2
        c = item % 2

        @pl.when(has(ARRIVE))
        def _():
            forwards = has(FORWARD)
            across = slot == 0
            for k in range(2):
                rows_copy(item, (sp, core_peer), item, item, k).wait_recv()

                @pl.when(forwards)
                def _():
                    rows_copy(
                        item,
                        (line(jnp.where(across, 2, 0)), tp),
                        jnp.where(across, 6 + c, item),
                        jnp.where(across, 10 + c, item),
                        k,
                    ).start()

        def specials():
            @pl.when(has(DOWN_PASS))
            def _():
                for t in early:
                    tile_on(t, 2, 3)

            @pl.when(has(SEND_ACROSS))
            def _():
                for k in range(2):
                    send_own(1, k, True)

            @pl.when(has(FIRST_PASS))
            def _():
                weight_on(0, 7, 6)
                weight_on(1, 7, 6)

            for k in range(2):

                @pl.when(has((GATE_PASS, UP_PASS)[k]))
                def _():
                    weight_on(k, 1, 4)
                    weight_on(k, 2, 5)

            @pl.when(has(DOWN_READY))
            def _():
                for t in early:
                    tile_copy(t, 1).wait_recv()
                    tile_copy(t, 3).wait_recv()

            @pl.when(has(FAR_PASS))
            def _():
                down_copy(0).wait_recv()
                down_copy(1).wait_recv()
                down_copy(2).start()
                down_copy(3).start()

            @pl.when(has(HIDDEN_READY))
            def _():
                for k in range(2):
                    for leg in range(3, 7):
                        weight_copy(k, leg).wait_recv()

            @pl.when(has(SEND_OUTWARD))
            def _():
                for k in range(2):
                    send_own(1, k, False)

            @pl.when(has(LATE_RELAY))
            def _():
                for t in late:
                    tile_on(t, 0, 1, 2)

            @pl.when(has(LATE_PASS))
            def _():
                for t in late:
                    tile_on(t, 2, 3)

            @pl.when(has(LATE_READY))
            def _():
                for t in late:
                    tile_copy(t, 1).wait_recv()
                    tile_copy(t, 3).wait_recv()

            @pl.when(has(FAR_READY))
            def _():
                down_copy(3).wait_recv()
                down_copy(4).start()
                down_copy(2).wait_recv()
                down_copy(4).wait_recv()

        pl.when(code >= SPECIAL)(specials)

        @pl.when(has(OWN))
        def _():
            hidden(item, 0)

        @pl.when(has(OTHER))
        def _():
            hidden(item, 1)

        middle = jnp.logical_or(slot == 1, item == 5)
        begins = code // LATER % 2 == 0

        short = jnp.logical_and(outer, middle)

        @pl.when(jnp.logical_and(has(OUT), short))
        def _():
            hidden_copy(item).start()

        @pl.when(jnp.logical_and(has(OUT), jnp.logical_not(short)))
        def _():
            inner_at = jnp.where(slot == 1, 7 + c, jnp.where(slot == 2, jnp.where(c == 0, 9, 0), 3 + c))
            a = jnp.where(slot == 0, 5 + c, jnp.where(outer, 0, inner_at))
            d = jnp.where(slot == own, 1 + c, 0)

            @pl.when(jnp.logical_and(middle, begins))
            def _():
                ref = HR.at[held(item)]
                remote(ref, ref, hid_s.at[0], hid_r.at[held(item)], (sp, core_peer)).wait_recv()

            def some(m, carry):
                cols = pl.ds(pl.multiple_of(m * tile, tile), tile)

                stage[...] = jnp.dot(H[item], wd[:, cols], preferred_element_type=jnp.float32)

                @pl.when(middle)
                def _():
                    stage[...] += jnp.dot(HR[held(item)], wdo[:, cols], preferred_element_type=jnp.float32)

                @pl.when(a > 0)
                def _():
                    came(a, m)

                S[item, :, cols] = bf16(stage[...] + f32(P[d, :, cols]) + f32(P[a, :, cols]))

                @pl.when(slot == own)
                def _():
                    out_copy(c, m).start()

                @pl.when(slot != own)
                def _():
                    sum_copy(item, m).start()

                return carry

            begin = jnp.where(begins, 0, tiles // 2)
            lax.fori_loop(begin, begin + tiles // 2, some, 0)

        return carry

    lax.fori_loop(0, len(OUTER_STEPS), step, 0)

    for c in range(2):
        for m in range(depth // tile):
            out_copy(c, m).wait()
        core_copy(0, c).wait_send()
        core_copy(1, c).wait_send()
        x_copy(c, 0).wait_send()
        x_copy(c, 1).wait_send()

    @pl.when(sp < count - 1)
    def _():
        for k in range(2):
            halo_copy(k, (sp + 1, tp)).wait_send()

    for k in range(2):
        for leg in range(8):
            weight_copy(k, leg).wait_send()
    for t in range(tiles):
        for leg in range(4):
            tile_copy(t, leg).wait_send()
    table_copy(own, False).wait_send()

    @pl.when(inner)
    def _():
        table_copy(1, True).wait_send()
        table_copy(0, True).wait_send()
        table_copy(2, False).wait_send()
        table_copy(3, False).wait_send()


    def gone(at):
        for k in range(2):
            rows_copy(at % 8, (sp, core_peer), at % 8, at, k).wait_send()

    def summed(item):
        for m in range(depth // tile):
            sum_copy(item, m).wait_send()

    for c in range(2):
        gone(2 * own + c)

    @pl.when(outer)
    def _():
        summed(4)
        hidden_copy(5).wait_send()
        for c in range(2):
            down_copy(c).wait_send()
            summed(6 + c)
            hidden_copy(2 + c).wait_send()

    @pl.when(inner)
    def _():
        for leg in range(2, 5):
            down_copy(leg).wait_send()
        for c in range(2):
            for at in (4 + c, 6 + c, 8 + c, 10 + c):
                gone(at)
            for slot in (0, 2, 3):
                summed(2 * slot + c)


def mega(
    conv_outer, conv_inner, conv_input, conv_taps, out_weight, mix_gate, residual, mix_gain, expert_gain,
    expert_ids, group_share, pair_scores, gate_experts, up_experts, down_experts,
):
    count = lax.axis_size("sp")
    rows, depth = residual.shape
    tokens, channels = conv_inner.shape
    width = gate_experts.shape[2]
    piece = rows // 2
    halo = 16
    tiles = depth // min(512, depth)
    half_type, full = jnp.bfloat16, jnp.float32
    hbm = pl.BlockSpec(memory_space=pl.ANY)
    vmem = pl.BlockSpec(memory_space=pltpu.VMEM)
    dma = pltpu.SemaphoreType.DMA
    return pl.pallas_call(
        mega_kernel,
        out_shape=jax.ShapeDtypeStruct((rows, depth), half_type),
        in_specs=[hbm, hbm, hbm, vmem, hbm, hbm, hbm, vmem, vmem, vmem, vmem, vmem, hbm, hbm, hbm],
        out_specs=hbm,
        scratch_shapes=[
            pltpu.VMEM((halo + tokens, channels), half_type),
            pltpu.VMEM((halo + tokens, channels), half_type),
            pltpu.VMEM((tokens, channels), half_type),
            pltpu.VMEM((channels, depth), half_type),
            pltpu.VMEM((rows, depth), half_type),
            pltpu.VMEM((rows, depth), half_type),
            pltpu.VMEM((tokens, channels), half_type),
            pltpu.VMEM((2, piece, depth), full),
            pltpu.VMEM((4, piece, depth), half_type),
            pltpu.VMEM((4, piece, depth), half_type),
            pltpu.VMEM((2, piece, depth), half_type),
            pltpu.VMEM((2, piece, depth), half_type),
            pltpu.VMEM((8, piece, depth), half_type),
            pltpu.VMEM((8, 2 * count, piece), half_type),
            pltpu.VMEM((11, piece, depth), half_type),
            pltpu.VMEM((8, piece, depth), half_type),
            pltpu.VMEM((8, piece, 2 * width), half_type),
            pltpu.VMEM((3, piece, 2 * width), half_type),
            pltpu.VMEM((piece, min(512, depth)), full),
            pltpu.VMEM((depth, width), half_type),
            pltpu.VMEM((depth, width), half_type),
            pltpu.VMEM((depth, width), half_type),
            pltpu.VMEM((depth, width), half_type),
            pltpu.VMEM((2 * width, depth), half_type),
            pltpu.VMEM((2 * width, depth), half_type),
            pltpu.VMEM((2, 2 * count, width), half_type),
            dma((9,)),
            dma((2,)),
            dma((2,)),
            dma((8,)),
            dma((4,)),
            dma((4,)),
            dma((4,)),
            dma((4,)),
            dma((4,)),
            dma((16 + 4 * tiles,)),
            dma((16 + 4 * tiles,)),
            dma((16, 2)),
            dma((8, 2)),
            dma((8, tiles)),
            dma((11, tiles)),
            dma((3,)),
            dma((3,)),
            dma((5,)),
            dma((5,)),
            dma((2, tiles)),
        ],
        compiler_params=pltpu.CompilerParams(
            collective_id=0, has_side_effects=True, vmem_limit_bytes=60 * 1024 * 1024
        ),
        name="layer",
    )(
        conv_outer, conv_inner, conv_input, conv_taps, out_weight, mix_gate, residual,
        mix_gain[None, :], expert_gain[None, :], expert_ids.T, pair_scores.T, group_share[None, :], gate_experts, up_experts, down_experts,
    )


def solution(mesh):
    placed = (
        P("sp", "tp"),
        P("sp", "tp"),
        P("sp", "tp"),
        P(None, "tp"),
        P("tp", None),
        P(("sp", "tp"), None),
        P(("sp", "tp"), None),
        P(),
        P(),
        P(("sp", "tp"), None),
        P(("sp", "tp")),
        P(("sp", "tp"), None),
        P("sp", None, None),
        P("sp", None, None),
        P("sp", None, None),
    )

    square = mesh.shape["tp"] == 4 and mesh.shape["sp"] == 8

    def layer(*arrays):
        return (mega if square else per_device)(*arrays)

    return jax.shard_map(
        layer, mesh=mesh, in_specs=placed, out_specs=P(("sp", "tp"), None), check_vma=False
    )
```

```python
import jax
import jax.numpy as jnp
from jax import lax
from jax.experimental import pallas as pl
from jax.experimental.pallas import tpu as pltpu
from jax.sharding import PartitionSpec as P

epsilon = 1e-06


def f32(value):
    return value.astype(jnp.float32)


def bf16(value):
    return value.astype(jnp.bfloat16)


def rms_scale(values, gain):
    return values * lax.rsqrt(jnp.mean(values * values, axis=-1, keepdims=True) + epsilon) * gain


def shifted(value, steps, senders):
    return lax.ppermute(value, "sp", [(s, s + steps) for s in senders])


def swapped(value, axis, bit):
    return lax.ppermute(value, axis, [(s, s ^ bit) for s in range(lax.axis_size(axis))])


def mixer_rows(conv_outer, conv_inner, conv_input, conv_taps):
    kept = conv_taps.shape[0] - 1
    inner = f32(conv_inner) * f32(conv_input)
    tail = f32(conv_inner[-kept:]) * f32(conv_input[-kept:])
    earlier = shifted(tail, 1, range(lax.axis_size("sp") - 1))
    length = conv_inner.shape[0]
    inner = jnp.concatenate([earlier, inner], 0)
    conv = conv_taps[0] * inner[0:length]
    for offset in range(1, kept + 1):
        conv = conv + conv_taps[offset] * inner[offset : offset + length]
    return bf16(f32(conv_outer) * conv)


def project(mixed_rows, out_weight, own_rows):
    parts = lax.axis_size("tp")
    me = lax.axis_index("tp")
    blocks = mixed_rows.reshape(parts, own_rows, -1)

    def partial(owner):
        rows = lax.dynamic_index_in_dim(blocks, owner, 0, keepdims=False)
        return jnp.dot(rows, out_weight, preferred_element_type=jnp.float32)

    def total(owner_bits, bit):
        if bit == 1:
            return partial(me ^ owner_bits)
        half = bit // 2
        sent = bf16(total(owner_bits | half, half))
        given = swapped(sent, "tp", half)
        return total(owner_bits, half) + f32(given)

    return total(0, parts)


def routing_table(expert_ids, group_share, pair_scores, own_rows, count):
    weights = group_share[:, None] * jax.nn.softmax(pair_scores, axis=-1)
    lanes = -(-2 * count // 128) * 128
    column = jnp.arange(lanes, dtype=jnp.int32)[None, :]
    coarse = lax.reduce_precision(weights, 8, 7)
    fine = weights - coarse
    table = jnp.zeros((own_rows, lanes), jnp.float32)
    for slot in range(expert_ids.shape[1]):
        at = expert_ids[:, slot : slot + 1]
        table = table + jnp.where(column == at, coarse[:, slot : slot + 1], 0.0)
        table = table + jnp.where(column == at + count, fine[:, slot : slot + 1], 0.0)
    return bf16(table)


def per_device(
    conv_outer,
    conv_inner,
    conv_input,
    conv_taps,
    out_weight,
    mix_gate,
    residual,
    mix_gain,
    expert_gain,
    expert_ids,
    group_share,
    pair_scores,
    gate_experts,
    up_experts,
    down_experts,
):
    count = lax.axis_size("sp")
    me = lax.axis_index("sp")
    own_rows = residual.shape[0]
    groups = count // 2
    place = me // 2
    side = lax.axis_index("tp") % 2
    half = gate_experts.shape[2] // 2

    def fetched(weight, axis):
        piece = lax.dynamic_slice_in_dim(weight[0], side * half, half, axis)
        first = swapped(piece, "sp", 1)
        second = swapped(first, "tp", 1)
        return jnp.concatenate([weight[0], first, second], axis)

    gate_both = fetched(gate_experts, 1)
    up_both = fetched(up_experts, 1)
    down_both = fetched(down_experts, 0)

    lanes = -(-2 * count // 128) * 128
    table = routing_table(expert_ids, group_share, pair_scores, own_rows, count)

    def spread(own):
        below, above = {0: own}, {0: own}
        for step in range(1, groups):
            below[step] = shifted(below[step - 1], 2, range(2 * (step - 1), count - 2))
            above[step] = shifted(above[step - 1], -2, range(2, count - 2 * (step - 1)))
        order = {0: own}
        for near in range(1, (groups - 1) // 2 + 1):
            far = groups - near
            early = jnp.where(place < near, above[near], below[near])
            _, over, under, away = lax.optimization_barrier(
                (early, above[near], below[far], above[far])
            )
            order[near] = early
            late = jnp.where(place < far, over, under)
            order[far] = jnp.where(place < near, away, late)
        if groups % 2 == 0:
            mid = groups // 2
            order[mid] = jnp.where(place < mid, above[mid], below[mid])
        return order

    mixed_rows = mixer_rows(conv_outer, conv_inner, conv_input, conv_taps)
    projected = project(mixed_rows, out_weight, own_rows)
    mixed = jax.nn.sigmoid(f32(mix_gate)) * projected
    hidden_state = bf16(f32(residual) + rms_scale(mixed, mix_gain))
    normed = bf16(rms_scale(f32(hidden_state), expert_gain))

    blocks = spread(jnp.concatenate([normed, table], 1))
    depth = normed.shape[1]

    def served(block):
        rows = block[:, :depth]
        chosen = jnp.arange(lanes, dtype=jnp.int32)[:, None] % count
        picks = bf16(chosen == jnp.stack([me, me ^ 1])[None, :])
        picks = jnp.where(jnp.arange(lanes)[:, None] < 2 * count, picks, 0)
        shares = jnp.dot(block[:, depth:], picks, preferred_element_type=jnp.float32)
        wide = 2 * half
        first = jnp.dot(rows, gate_both, preferred_element_type=jnp.float32)
        second = jnp.dot(rows, up_both, preferred_element_type=jnp.float32)
        mine = jnp.arange(2 * wide)[None, :] < wide
        share = jnp.where(mine, shares[:, :1], shares[:, 1:])
        hidden = lax.optimization_barrier(bf16(jax.nn.silu(first) * second * share))
        return lax.optimization_barrier(
            jnp.dot(hidden, down_both, preferred_element_type=jnp.float32)
        )

    results = {number: served(block) for number, block in blocks.items()}

    def for_upper(step):
        gone = groups - step
        if step == gone or step < gone:
            return results[gone]
        return jnp.where(place < gone, results[gone], results[step])

    down = up = None
    for step in range(1, groups):
        gone = groups - step
        lower, upper = results[gone], for_upper(step)
        if down is not None:
            lower, upper = lower + f32(down), upper + f32(up)
        down = shifted(bf16(lower), -2, range(2 * gone, count))
        up = shifted(bf16(upper), 2, range(0, count - 2 * gone))
    result = f32(hidden_state) + results[0]
    if down is not None:
        result = result + f32(down) + f32(up)
    return bf16(result)


MESH_ID = pl.DeviceIdType.MESH
OWN, OTHER, OUT, ARRIVE, FORWARD, LATER = (8 << i for i in range(6))
SPECIAL = 8 << 6
(DOWN_PASS, SEND_ACROSS, FIRST_PASS, GATE_PASS, UP_PASS, DOWN_READY, FAR_PASS, HIDDEN_READY, SEND_OUTWARD, LATE_RELAY, LATE_PASS, LATE_READY, FAR_READY,) = (SPECIAL << i for i in range(13))

OUTER_STEPS = (
    0 | FIRST_PASS,
    4 | OWN | ARRIVE,
    0 | OWN,
    0 | GATE_PASS | UP_PASS,
    4 | OTHER | OUT | DOWN_PASS | DOWN_READY | HIDDEN_READY,
    6 | OWN | OTHER | ARRIVE,
    6 | OUT | LATE_RELAY,
    7 | OWN | OTHER | OUT | ARRIVE,
    2 | OWN | ARRIVE,
    7 | OUT | LATER | LATE_PASS | LATE_READY,
    1 | OWN,
    2 | OTHER,
    6 | OUT | LATER,
    0 | OTHER,
    4 | OUT | LATER,
    5 | OWN | OTHER | OUT | ARRIVE,
    1 | OTHER | OUT,
    3 | OWN | ARRIVE,
    2 | OUT,
    0 | OUT,
    3 | OTHER | OUT,
    1 | OUT | LATER,
    0 | OUT | LATER,
)
INNER_STEPS = (
    4 | OWN | ARRIVE | FORWARD,
    0 | OWN | ARRIVE | FORWARD,
    1 | OWN | ARRIVE | FORWARD,
    6 | OWN | ARRIVE | FORWARD,
    0 | SEND_ACROSS | FIRST_PASS,
    0 | DOWN_PASS | GATE_PASS,
    7 | OWN | ARRIVE | FORWARD,
    3 | OWN | UP_PASS,
    0 | FAR_PASS | SEND_OUTWARD | LATE_RELAY,
    4 | OTHER | HIDDEN_READY,
    7 | OTHER | DOWN_READY,
    6 | OTHER,
    4 | OUT,
    0 | OTHER,
    5 | OWN | ARRIVE | FORWARD,
    6 | OUT,
    1 | OTHER | LATE_PASS,
    7 | OUT,
    5 | OTHER,
    2 | OWN,
    7 | OUT | LATER | LATE_READY,
    1 | OUT,
    0 | OUT,
    6 | OUT | LATER,
    2 | OTHER,
    3 | OTHER,
    4 | OUT | LATER,
    1 | OUT | LATER,
    0 | OUT | LATER,
    5 | OUT | FAR_READY,
    5 | OUT | LATER,
    2 | OUT,
    2 | OUT | LATER,
    3 | OUT,
    3 | OUT | LATER,
)


def mega_kernel(
    co_hbm, ci_hbm, cx_hbm, taps, ow_hbm, mg_hbm, res_hbm, mgain, egain, ids, scores, group,
    g_hbm, u_hbm, d_hbm, out_hbm,
    ci, cx, co, ow, mg, res, mix, acc, part_out, part_in, x_out, x_in,
    X, T, P, S, H, HR, stage, g1, u1, g2, u2, wd, wdo, picks,
    load_sem, halo_s, halo_r, tab_s, tab_r, core_s, core_r, xsw_s, xsw_r,
    w_s, w_r, rows_s, rows_r, sum_s, sum_r, hid_s, hid_r, do_s, do_r, out_sem,
):
    sp = lax.axis_index("sp")
    tp = lax.axis_index("tp")
    z = sp // 2
    y = sp % 2
    half = z // 2
    outer = z * (3 - z) == 0
    inner = jnp.logical_not(outer)
    own = jnp.where(outer, 0, 1)
    core_peer = tp + 1 - 2 * (tp % 2)
    x_peer = (tp + 2) % 4
    y_peer = sp + 1 - 2 * y
    rows, depth = res.shape
    piece = rows // 2
    width = g1.shape[1]
    count = T.shape[1] // 2
    channels = ow.shape[0]
    halo = ci.shape[0] - co.shape[0]

    def line(slot):
        where = jnp.where(slot == 0, 3 * half, jnp.where(slot == 1, 1 + half, jnp.where(slot == 2, 2 - half, 3 - 3 * half)))
        return 2 * where + y

    def remote(src, dst, s, r, device):
        return pltpu.make_async_remote_copy(
            src_ref=src, dst_ref=dst, send_sem=s, recv_sem=r, device_id=device, device_id_type=MESH_ID
        )

    barrier = pltpu.get_barrier_semaphore()

    def greet(device):
        pl.semaphore_signal(barrier, inc=1, device_id=device, device_id_type=MESH_ID)

    greet((sp, core_peer))
    greet((sp, x_peer))
    greet((y_peer, tp))
    greet((line(1 - own), tp))

    @pl.when(inner)
    def _():
        greet((line(2), tp))

    has_next = jnp.logical_and(y == 1, sp < count - 1)
    has_last = jnp.logical_and(y == 0, sp > 0)

    @pl.when(has_next)
    def _():
        greet((sp + 1, tp))

    @pl.when(has_last)
    def _():
        greet((sp - 1, tp))

    tokens = co.shape[0]
    loads = [
        pltpu.make_async_copy(ci_hbm, ci.at[pl.ds(halo, tokens)], load_sem.at[0]),
        pltpu.make_async_copy(cx_hbm, cx.at[pl.ds(halo, tokens)], load_sem.at[1]),
        pltpu.make_async_copy(co_hbm, co, load_sem.at[2]),
        pltpu.make_async_copy(ow_hbm, ow, load_sem.at[3]),
        pltpu.make_async_copy(mg_hbm, mg, load_sem.at[4]),
        pltpu.make_async_copy(res_hbm, res, load_sem.at[5]),
        pltpu.make_async_copy(g_hbm.at[0], g1, load_sem.at[6]),
        pltpu.make_async_copy(u_hbm.at[0], u1, load_sem.at[7]),
        pltpu.make_async_copy(d_hbm.at[0], wd.at[pl.ds(0, width)], load_sem.at[8]),
    ]
    for k in (0, 1, 3, 2):
        loads[k].start()

    raw = scores[...]
    top = jnp.maximum(raw[0:1], raw[1:2])
    up = jnp.exp(raw - top)
    weights = group[...] * (up / (up[0:1] + up[1:2]))
    coarse = f32(bf16(weights))
    fine = weights - coarse
    line_of = lax.broadcasted_iota(jnp.int32, (T.shape[1], rows), 0)
    entries = jnp.zeros((T.shape[1], rows), jnp.float32)
    for k in range(2):
        entries = entries + jnp.where(line_of == ids[k : k + 1], coarse[k : k + 1], 0.0)
        entries = entries + jnp.where(line_of == ids[k : k + 1] + count, fine[k : k + 1], 0.0)
    entries = bf16(entries)
    for p in range(2):
        T[2 * own + p] = entries[:, (1 - p) * piece : (2 - p) * piece]

    pl.semaphore_wait(barrier, 4 + jnp.where(inner, 1, 0) + jnp.where(has_next, 1, 0) + jnp.where(has_last, 1, 0))

    def halo_copy(k, device):
        src = (ci_hbm, cx_hbm)[k].at[pl.ds(tokens - halo, halo)]
        return remote(src, (ci, cx)[k].at[pl.ds(0, halo)], halo_s.at[k], halo_r.at[k], device)

    @pl.when(sp < count - 1)
    def _():
        for k in range(2):
            halo_copy(k, (sp + 1, tp)).start()

    eighth = depth // 8
    wide = width // 2
    side = tp % 2
    tile = min(512, depth)
    tiles = depth // tile
    quarter = width // 4
    first = jnp.where(tp // 2 == 0, side, 6 + side)
    lacking = jnp.where(tp // 2 == 0, 6 + side, side)

    def weight_copy(k, leg):
        block = (first, 2 + side, 4 + side, first, 2 + side, 4 + side, lacking, first)[leg]
        at = pl.ds(pl.multiple_of(block * eighth, eighth), eighth)
        buf = (g2, u2)[k]
        src = (g_hbm, u_hbm)[k].at[0, at] if leg < 3 else buf.at[at]
        device = (y_peer, tp) if leg < 3 else (sp, core_peer) if leg < 7 else (sp, x_peer)
        return remote(src, buf.at[at], w_s.at[8 * k + leg], w_r.at[8 * k + leg], device)

    def tile_copy(t, leg):
        row = (x_peer if leg == 3 else tp) * quarter
        cols = pl.ds(t * tile, tile)
        dst = wd.at[pl.ds(pl.multiple_of(width + row, quarter), quarter), cols]
        src = d_hbm.at[0, pl.ds(pl.multiple_of(row, quarter), quarter), cols] if leg == 0 else dst
        device = ((y_peer, tp), (sp, core_peer), (sp, x_peer), (sp, core_peer))[leg]
        return remote(src, dst, w_s.at[16 + 4 * t + leg], w_r.at[16 + 4 * t + leg], device)

    early = range(tiles // 2)
    late = range(tiles // 2, tiles)
    for k in range(2):
        weight_copy(k, 0).start()
    for t in early:
        tile_copy(t, 0).start()
    for k in range(2):
        weight_copy(k, 1).start()
        weight_copy(k, 2).start()
    for t in late:
        tile_copy(t, 0).start()

    part = wide // 2

    def down_copy(leg):
        if leg < 2:
            src = d_hbm.at[0, pl.ds(pl.multiple_of(side * wide + leg * part, part), part)]
            dst = wdo.at[pl.ds(pl.multiple_of(side * wide + leg * part, part), part)]
            device = (line(1), tp)
        else:
            near = wdo.at[pl.ds(pl.multiple_of(side * wide, wide), wide)]
            far = wdo.at[pl.ds(pl.multiple_of(width + side * wide, wide), wide)]
            src, dst = ((near, near), (near, far), (far, far))[leg - 2]
            device = (y_peer, tp) if leg == 3 else (sp, core_peer)
        return remote(src, dst, do_s.at[leg], do_r.at[leg], device)

    @pl.when(outer)
    def _():
        down_copy(0).start()

    def table_copy(slot, across):
        dst = 3 - slot if across else slot
        at = slot + (4 if across else 0)
        return remote(
            T.at[pl.ds(2 * slot, 2)],
            T.at[pl.ds(2 * dst, 2)],
            tab_s.at[at],
            tab_r.at[dst],
            (line(2) if across else line(1 - own), tp),
        )

    def table_came(slot):
        at = T.at[pl.ds(2 * slot, 2)]
        remote(at, at, tab_s.at[0], tab_r.at[slot], (sp, core_peer)).wait_recv()

    table_copy(own, False).start()

    @pl.when(inner)
    def _():
        table_copy(1, True).start()

    P[0] = jnp.zeros(P.shape[1:], P.dtype)
    lane = lax.broadcasted_iota(jnp.int32, (T.shape[1], width), 0)
    for k in range(2):
        picks[k] = jnp.where(lane % count == (sp, y_peer)[k], 1.0, 0.0).astype(picks.dtype)

    for k in range(3):
        loads[k].wait()
    for k in range(4, 9):
        loads[k].start()

    kept = taps.shape[0] - 1
    run = 32

    def conv(start):
        def some(i, c):
            at = pl.multiple_of(start + i * run, run)
            near = f32(ci[pl.ds(at, halo + run)]) * f32(cx[pl.ds(at, halo + run)])
            total = taps[0:1] * near[halo - kept : halo - kept + run]
            for j in range(1, kept + 1):
                total = total + taps[j : j + 1] * near[halo - kept + j : halo - kept + j + run]
            mix[pl.ds(at, run)] = bf16(f32(co[pl.ds(at, run)]) * total)
            return c

        lax.fori_loop(0, piece // run, some, 0)

    loads[3].wait()

    def core_copy(phase, p):
        at = 2 * phase + p
        return remote(part_out.at[at], part_in.at[at], core_s.at[at], core_r.at[at], (sp, core_peer))

    some_rows = piece // 2

    def x_copy(p, k):
        at = pl.ds(k * some_rows, some_rows)
        return remote(
            x_out.at[p, at], x_in.at[p, at], xsw_s.at[2 * p + k], xsw_r.at[2 * p + k], (sp, x_peer)
        )

    def projected(i, carry):
        phase = i // 4
        p = i // 2 % 2
        second = i % 2 == 1
        owner = jnp.where(
            phase == 0, jnp.where(second, x_peer, 3 - tp), jnp.where(second, tp, core_peer)
        )
        start = pl.multiple_of(owner * rows + (1 - p) * piece, piece)

        @pl.when(jnp.logical_and(i == 2, sp == 0))
        def _():
            ci[pl.ds(0, halo)] = jnp.zeros((halo, channels), ci.dtype)
            cx[pl.ds(0, halo)] = jnp.zeros((halo, channels), cx.dtype)

        @pl.when(jnp.logical_and(i == 2, sp > 0))
        def _():
            for k in range(2):
                halo_copy(k, (sp, core_peer)).wait_recv()

        conv(start)

        def some(n, c):
            cols = pl.ds(pl.multiple_of(n * tile, tile), tile)
            got = jnp.dot(mix[pl.ds(start, piece)], ow[:, cols], preferred_element_type=jnp.float32)

            @pl.when(second)
            def _():
                acc[p, :, cols] = got

            @pl.when(jnp.logical_not(second))
            def _():
                part_out[2 * phase + p, :, cols] = bf16(got)

            return c

        lax.fori_loop(0, depth // tile, some, 0)

        @pl.when(jnp.logical_not(second))
        def _():
            core_copy(phase, p).start()

        @pl.when(jnp.logical_and(second, phase == 0))
        def _():
            core_copy(0, p).wait_recv()

            def add(r, c):
                at = pl.ds(pl.multiple_of(r * 16, 16), 16)
                x_out[p, at] = bf16(acc[p, at] + f32(part_in[p, at]))
                return c

            steps = some_rows // 16
            for k in range(2):
                lax.fori_loop(k * steps, (k + 1) * steps, add, 0)
                x_copy(p, k).start()

        return carry

    lax.fori_loop(0, 8, projected, 0)
    loads[4].wait()
    loads[5].wait()

    def rows_copy(item, device, dst, at, k):
        some = pl.ds(k * some_rows, some_rows)
        return remote(X.at[item, some], X.at[dst, some], rows_s.at[at, k], rows_r.at[dst, k], device)

    def normalize(c, k):
        def some(r, carry):
            at = pl.ds(pl.multiple_of(r * 16, 16), 16)
            src = pl.ds(pl.multiple_of((1 - c) * piece + r * 16, 16), 16)
            total = acc[c, at] + f32(part_in[2 + c, at]) + f32(x_in[c, at])
            mixed = jax.nn.sigmoid(f32(mg[src])) * total
            state = bf16(f32(res[src]) + rms_scale(mixed, mgain[...]))
            P[1 + c, at] = state
            X[2 * own + c, at] = bf16(rms_scale(f32(state), egain[...]))
            return carry

        steps = some_rows // 16
        lax.fori_loop(k * steps, (k + 1) * steps, some, 0)

    def send_own(c, k, across):
        item = 2 * own + c
        if across:
            rows_copy(item, (line(2), tp), 4 + c, 8 + c, k).start()
        else:
            rows_copy(item, (line(1 - own), tp), item, item, k).start()

    def weight_on(k, came, *legs):
        weight_copy(k, came).wait_recv()
        for leg in legs:
            weight_copy(k, leg).start()

    def tile_on(t, came, *legs):
        tile_copy(t, came).wait_recv()
        for leg in legs:
            tile_copy(t, leg).start()

    @pl.when(inner)
    def _():
        table_came(0)
        table_copy(0, True).start()
        table_came(2)
        table_copy(2, False).start()

    weight_on(0, 0, 3, 7)
    core_copy(1, 0).wait_recv()
    for k in range(2):
        x_copy(0, k).wait_recv()
        normalize(0, k)
        send_own(0, k, False)

        @pl.when(inner)
        def _():
            send_own(0, k, True)

    @pl.when(inner)
    def _():
        table_came(3)
        table_copy(3, False).start()

    weight_on(1, 0, 3, 7)
    core_copy(1, 1).wait_recv()
    for k in range(2):
        x_copy(1, k).wait_recv()
        normalize(1, k)

        @pl.when(outer)
        def _():
            send_own(1, k, False)

    @pl.when(outer)
    def _():
        down_copy(1).start()

    for t in early:
        tile_on(t, 0, 1, 2)
    for k in range(6, 9):
        loads[k].wait()

    @pl.when(outer)
    def _():
        for slot in range(1, 4):
            table_came(slot)

    def hidden(item, k):
        gate, up = ((g1, u1), (g2, u2))[k]
        x = X[item]
        first = jnp.dot(x, gate[...], preferred_element_type=jnp.float32)
        second = jnp.dot(x, up[...], preferred_element_type=jnp.float32)
        share = lax.dot_general(
            T[item], picks[k], (((0,), (0,)), ((), ())), preferred_element_type=jnp.float32
        )
        H[item, :, k * width : (k + 1) * width] = bf16(jax.nn.silu(first) * second * share)

    def sum_copy(item, m):
        slot = item // 2
        c = item % 2
        to = jnp.where(outer, 1, jnp.where(slot == 0, 0, 2))
        dst = jnp.where(outer, jnp.where(slot == 2, 9 + c, 3 + c), jnp.where(slot == 2, 7 + c, 5 + c))
        cols = pl.ds(pl.multiple_of(m * tile, tile), tile)
        return remote(S.at[item, :, cols], P.at[dst, :, cols], sum_s.at[item, m], sum_r.at[dst, m], (line(to), tp))

    def held(item):
        return jnp.where(item == 5, 2, item - 2)

    def hidden_copy(item):
        at = held(item)
        return remote(H.at[item], HR.at[at], hid_s.at[at], hid_r.at[at], (line(1), tp))

    def out_copy(c, m):
        cols = pl.ds(pl.multiple_of(m * tile, tile), tile)
        return pltpu.make_async_copy(
            S.at[2 * own + c, :, cols],
            out_hbm.at[pl.ds(pl.multiple_of((1 - c) * piece, piece), piece), cols],
            out_sem.at[c, m],
        )

    def came(at, m):
        cols = pl.ds(pl.multiple_of(m * tile, tile), tile)
        ref = P.at[at, :, cols]
        remote(ref, ref, sum_s.at[0, m], sum_r.at[at, m], (sp, core_peer)).wait_recv()

    def run_steps(steps, outer, own):
        def step(n, carry):
            code = 0
            for i, value in enumerate(steps):
                code = jnp.where(n == i, value, code)
            item = code % 8

            def has(flag):
                return code // flag % 2 == 1

            slot = item // 2
            c = item % 2

            @pl.when(has(ARRIVE))
            def _():
                forwards = has(FORWARD)
                across = slot == 0
                for k in range(2):
                    rows_copy(item, (sp, core_peer), item, item, k).wait_recv()

                    @pl.when(forwards)
                    def _():
                        rows_copy(
                            item,
                            (line(jnp.where(across, 2, 0)), tp),
                            jnp.where(across, 6 + c, item),
                            jnp.where(across, 10 + c, item),
                            k,
                        ).start()

            def specials():
                @pl.when(has(DOWN_PASS))
                def _():
                    for t in early:
                        tile_on(t, 2, 3)

                @pl.when(has(SEND_ACROSS))
                def _():
                    for k in range(2):
                        send_own(1, k, True)

                @pl.when(has(FIRST_PASS))
                def _():
                    weight_on(0, 7, 6)
                    weight_on(1, 7, 6)

                for k in range(2):

                    @pl.when(has((GATE_PASS, UP_PASS)[k]))
                    def _():
                        weight_on(k, 1, 4)
                        weight_on(k, 2, 5)

                @pl.when(has(DOWN_READY))
                def _():
                    for t in early:
                        tile_copy(t, 1).wait_recv()
                        tile_copy(t, 3).wait_recv()

                @pl.when(has(FAR_PASS))
                def _():
                    down_copy(0).wait_recv()
                    down_copy(1).wait_recv()
                    down_copy(2).start()
                    down_copy(3).start()

                @pl.when(has(HIDDEN_READY))
                def _():
                    for k in range(2):
                        for leg in range(3, 7):
                            weight_copy(k, leg).wait_recv()

                @pl.when(has(SEND_OUTWARD))
                def _():
                    for k in range(2):
                        send_own(1, k, False)

                @pl.when(has(LATE_RELAY))
                def _():
                    for t in late:
                        tile_on(t, 0, 1, 2)

                @pl.when(has(LATE_PASS))
                def _():
                    for t in late:
                        tile_on(t, 2, 3)

                @pl.when(has(LATE_READY))
                def _():
                    for t in late:
                        tile_copy(t, 1).wait_recv()
                        tile_copy(t, 3).wait_recv()

                @pl.when(has(FAR_READY))
                def _():
                    down_copy(3).wait_recv()
                    down_copy(4).start()
                    down_copy(2).wait_recv()
                    down_copy(4).wait_recv()

            pl.when(code >= SPECIAL)(specials)

            @pl.when(has(OWN))
            def _():
                hidden(item, 0)

            @pl.when(has(OTHER))
            def _():
                hidden(item, 1)

            middle = jnp.logical_or(slot == 1, item == 5)
            begins = code // LATER % 2 == 0

            short = jnp.logical_and(outer, middle)

            @pl.when(jnp.logical_and(has(OUT), short))
            def _():
                hidden_copy(item).start()

            @pl.when(jnp.logical_and(has(OUT), jnp.logical_not(short)))
            def _():
                inner_at = jnp.where(slot == 1, 7 + c, jnp.where(slot == 2, jnp.where(c == 0, 9, 0), 3 + c))
                a = jnp.where(slot == 0, 5 + c, jnp.where(outer, 0, inner_at))
                d = jnp.where(slot == own, 1 + c, 0)

                @pl.when(jnp.logical_and(middle, begins))
                def _():
                    ref = HR.at[held(item)]
                    remote(ref, ref, hid_s.at[0], hid_r.at[held(item)], (sp, core_peer)).wait_recv()

                def some(m, carry):
                    cols = pl.ds(pl.multiple_of(m * tile, tile), tile)

                    stage[...] = jnp.dot(H[item], wd[:, cols], preferred_element_type=jnp.float32)

                    @pl.when(middle)
                    def _():
                        stage[...] += jnp.dot(HR[held(item)], wdo[:, cols], preferred_element_type=jnp.float32)

                    @pl.when(a > 0)
                    def _():
                        came(a, m)

                    S[item, :, cols] = bf16(stage[...] + f32(P[d, :, cols]) + f32(P[a, :, cols]))

                    @pl.when(slot == own)
                    def _():
                        out_copy(c, m).start()

                    @pl.when(slot != own)
                    def _():
                        sum_copy(item, m).start()

                    return carry

                begin = jnp.where(begins, 0, tiles // 2)
                lax.fori_loop(begin, begin + tiles // 2, some, 0)

            return carry

        lax.fori_loop(0, len(steps), step, 0)

    @pl.when(outer)
    def _():
        run_steps(OUTER_STEPS, True, 0)

    @pl.when(inner)
    def _():
        run_steps(INNER_STEPS, False, 1)

    for c in range(2):
        for m in range(depth // tile):
            out_copy(c, m).wait()
        core_copy(0, c).wait_send()
        core_copy(1, c).wait_send()
        x_copy(c, 0).wait_send()
        x_copy(c, 1).wait_send()

    @pl.when(sp < count - 1)
    def _():
        for k in range(2):
            halo_copy(k, (sp + 1, tp)).wait_send()

    for k in range(2):
        for leg in range(8):
            weight_copy(k, leg).wait_send()
    for t in range(tiles):
        for leg in range(4):
            tile_copy(t, leg).wait_send()
    table_copy(own, False).wait_send()

    @pl.when(inner)
    def _():
        table_copy(1, True).wait_send()
        table_copy(0, True).wait_send()
        table_copy(2, False).wait_send()
        table_copy(3, False).wait_send()


    def gone(at):
        for k in range(2):
            rows_copy(at % 8, (sp, core_peer), at % 8, at, k).wait_send()

    def summed(item):
        for m in range(depth // tile):
            sum_copy(item, m).wait_send()

    for c in range(2):
        gone(2 * own + c)

    @pl.when(outer)
    def _():
        summed(4)
        hidden_copy(5).wait_send()
        for c in range(2):
            down_copy(c).wait_send()
            summed(6 + c)
            hidden_copy(2 + c).wait_send()

    @pl.when(inner)
    def _():
        for leg in range(2, 5):
            down_copy(leg).wait_send()
        for c in range(2):
            for at in (4 + c, 6 + c, 8 + c, 10 + c):
                gone(at)
            for slot in (0, 2, 3):
                summed(2 * slot + c)


def mega(
    conv_outer, conv_inner, conv_input, conv_taps, out_weight, mix_gate, residual, mix_gain, expert_gain,
    expert_ids, group_share, pair_scores, gate_experts, up_experts, down_experts,
):
    count = lax.axis_size("sp")
    rows, depth = residual.shape
    tokens, channels = conv_inner.shape
    width = gate_experts.shape[2]
    piece = rows // 2
    halo = 16
    tiles = depth // min(512, depth)
    half_type, full = jnp.bfloat16, jnp.float32
    hbm = pl.BlockSpec(memory_space=pl.ANY)
    vmem = pl.BlockSpec(memory_space=pltpu.VMEM)
    dma = pltpu.SemaphoreType.DMA
    return pl.pallas_call(
        mega_kernel,
        out_shape=jax.ShapeDtypeStruct((rows, depth), half_type),
        in_specs=[hbm, hbm, hbm, vmem, hbm, hbm, hbm, vmem, vmem, vmem, vmem, vmem, hbm, hbm, hbm],
        out_specs=hbm,
        scratch_shapes=[
            pltpu.VMEM((halo + tokens, channels), half_type),
            pltpu.VMEM((halo + tokens, channels), half_type),
            pltpu.VMEM((tokens, channels), half_type),
            pltpu.VMEM((channels, depth), half_type),
            pltpu.VMEM((rows, depth), half_type),
            pltpu.VMEM((rows, depth), half_type),
            pltpu.VMEM((tokens, channels), half_type),
            pltpu.VMEM((2, piece, depth), full),
            pltpu.VMEM((4, piece, depth), half_type),
            pltpu.VMEM((4, piece, depth), half_type),
            pltpu.VMEM((2, piece, depth), half_type),
            pltpu.VMEM((2, piece, depth), half_type),
            pltpu.VMEM((8, piece, depth), half_type),
            pltpu.VMEM((8, 2 * count, piece), half_type),
            pltpu.VMEM((11, piece, depth), half_type),
            pltpu.VMEM((8, piece, depth), half_type),
            pltpu.VMEM((8, piece, 2 * width), half_type),
            pltpu.VMEM((3, piece, 2 * width), half_type),
            pltpu.VMEM((piece, min(512, depth)), full),
            pltpu.VMEM((depth, width), half_type),
            pltpu.VMEM((depth, width), half_type),
            pltpu.VMEM((depth, width), half_type),
            pltpu.VMEM((depth, width), half_type),
            pltpu.VMEM((2 * width, depth), half_type),
            pltpu.VMEM((2 * width, depth), half_type),
            pltpu.VMEM((2, 2 * count, width), half_type),
            dma((9,)),
            dma((2,)),
            dma((2,)),
            dma((8,)),
            dma((4,)),
            dma((4,)),
            dma((4,)),
            dma((4,)),
            dma((4,)),
            dma((16 + 4 * tiles,)),
            dma((16 + 4 * tiles,)),
            dma((16, 2)),
            dma((8, 2)),
            dma((8, tiles)),
            dma((11, tiles)),
            dma((3,)),
            dma((3,)),
            dma((5,)),
            dma((5,)),
            dma((2, tiles)),
        ],
        compiler_params=pltpu.CompilerParams(
            collective_id=0, has_side_effects=True, vmem_limit_bytes=60 * 1024 * 1024
        ),
        name="layer",
    )(
        conv_outer, conv_inner, conv_input, conv_taps, out_weight, mix_gate, residual,
        mix_gain[None, :], expert_gain[None, :], expert_ids.T, pair_scores.T, group_share[None, :], gate_experts, up_experts, down_experts,
    )


def solution(mesh):
    placed = (
        P("sp", "tp"),
        P("sp", "tp"),
        P("sp", "tp"),
        P(None, "tp"),
        P("tp", None),
        P(("sp", "tp"), None),
        P(("sp", "tp"), None),
        P(),
        P(),
        P(("sp", "tp"), None),
        P(("sp", "tp")),
        P(("sp", "tp"), None),
        P("sp", None, None),
        P("sp", None, None),
        P("sp", None, None),
    )

    square = mesh.shape["tp"] == 4 and mesh.shape["sp"] == 8

    def layer(*arrays):
        return (mega if square else per_device)(*arrays)

    return jax.shard_map(
        layer, mesh=mesh, in_specs=placed, out_specs=P(("sp", "tp"), None), check_vma=False
    )
```
